32 devices in a mesh: sp: 8 (over z, y), tp: 4 (over x, core).
Axes of the slice: x: 2, y: 2, z: 4, core: 2. Of those that a mesh axis runs over, the one named last changes fastest.
Arguments:
- grouped_head_inputs: bfloat16 [8192, 2, 1024], P('sp', None, 'tp'), may hold values from -6 to 6
- head_gate_inputs: bfloat16 [8192, 2, 1024], P('sp', None, 'tp'), may hold values from -6 to 6
- unsmoothed_step: float32 [8192, 2, 16], P('sp', None, 'tp'), may hold values from -3.8 to 3.8
- head_decay_rate: float32 [2, 16], P(None, 'tp'), may hold values from 1.2207031e-05 to 0.04761905
- extra_log_decay: float32 [8192, 2, 16], P('sp', None, 'tp'), may hold values from -1.4 to 0
- first_group_keys: bfloat16 [8192, 128], P('sp'), may hold values from -6 to 6
- first_group_queries: bfloat16 [8192, 128], P('sp'), may hold values from -6 to 6
- second_group_keys: bfloat16 [8192, 64], P('sp'), may hold values from -6 to 6
- second_group_queries: bfloat16 [8192, 64], P('sp'), may hold values from -6 to 6
- head_input_filter: float32 [4, 2, 1024], P(None, None, 'tp'), may hold values from -3 to 3
- first_group_filter: float32 [4, 2, 128], replicated, may hold values from -3 to 3
- second_group_filter: float32 [4, 2, 64], replicated, may hold values from -3 to 3
- head_norm_gain: float32 [2, 1024], P(None, 'tp'), may hold values from 0.1 to 1.9
- output_weight: bfloat16 [2, 1024, 2048], P(None, None, 'tp'), may hold values from -0.125 to 0.125
- residual: bfloat16 [8192, 2048], P('sp', 'tp'), may hold values from -37 to 37
- channel_norm_gain: float32 [2048], replicated, may hold values from 0.1 to 1.9
- channel_gate_weight: bfloat16 [2048, 5120], P('sp', 'tp'), may hold values from -0.125 to 0.125
- channel_up_weight: bfloat16 [2048, 5120], P('sp', 'tp'), may hold values from -0.125 to 0.125
- channel_down_weight: bfloat16 [2048, 5120], P('sp', 'tp'), may hold values from -0.078125 to 0.078125
Outputs:
- layer_output: bfloat16 [8192, 2048], P('sp', 'tp')
The draws below stay inside these ranges and needn't reach their ends.
All inputs are finite; a program needn't handle non-finite values.
Results may differ from the reference program's by a relative error of at most 0.007.
Values may be sent and summed in bfloat16 or wider, within the bound.
A program may use at most 128 MiB of HBM per device.

```python
import math
import jax
import jax.numpy as jnp
from jax import lax

D = 2048
GROUP_HEADS = 16
HEAD = 64
STATE_ONE = 128
STATE_TWO = 64
FF = 5120
CONV = 4
BLOCK = 128
TOKENS = 8192
CHANNELS = 1024
N_TP = 4


def draw_unsmoothed_step(key, part):
    noise_key = jax.random.fold_in(key, 11)
    block_key = jax.random.fold_in(key, 12)
    block_total = TOKENS // BLOCK
    offsets = jax.random.uniform(block_key, (block_total, 1, 1, 1), jnp.float32, -1.0, 1.0)
    noise = 0.7 * jax.random.truncated_normal(noise_key, -4.0, 4.0, (block_total, BLOCK, 2, GROUP_HEADS), jnp.float32)
    return (noise + offsets).reshape(TOKENS, 2, GROUP_HEADS)


def draw_head_decay_rate(key, part):
    choose_key = jax.random.fold_in(key, 21)
    fast_key = jax.random.fold_in(key, 22)
    slow_key = jax.random.fold_in(key, 23)
    share = 0.5
    quick = jax.random.uniform(choose_key, (2, GROUP_HEADS), jnp.float32) < share
    fast = jnp.exp(jax.random.uniform(fast_key, (2, GROUP_HEADS), jnp.float32, math.log(1.0 / 70.0), math.log(1.0 / 21.0)))
    slow = jnp.exp(jax.random.uniform(slow_key, (2, GROUP_HEADS), jnp.float32, math.log(0.1), math.log(0.6))) / TOKENS
    return jnp.where(quick, fast, slow)


def draw_extra_log_decay(key, part):
    place_key = jax.random.fold_in(key, 31)
    loss_key = jax.random.fold_in(key, 32)
    places = jax.random.randint(place_key, (2, 2, GROUP_HEADS), 0, TOKENS)
    losses = jax.random.uniform(loss_key, (2, 2, GROUP_HEADS), jnp.float32, 0.2, 0.5)
    positions = jnp.arange(TOKENS, dtype=jnp.int32)[:, None, None, None]
    struck = positions == places[None]
    return jnp.sum(jnp.where(struck, jnp.log(1.0 - losses)[None], 0.0), axis=1)


def draw_residual(key, part):
    row_key = jax.random.fold_in(key, 41)
    column_key = jax.random.fold_in(key, 42)
    noise_key = jax.random.fold_in(key, 43)
    row_scale = jnp.exp(jax.random.uniform(row_key, (TOKENS, 1), jnp.float32, math.log(0.3), math.log(3.0)))
    column_scale = jnp.exp(jax.random.uniform(column_key, (1, D), jnp.float32, math.log(0.3), math.log(3.0)))
    noise = jax.random.truncated_normal(noise_key, -4.0, 4.0, (TOKENS, D), jnp.float32)
    return (noise * row_scale * column_scale).astype(jnp.bfloat16)


def level_of(own_key, dims, cuts, least, high):
    def one(axis_at, parts):
        heights = jax.random.uniform(jax.random.fold_in(jax.random.fold_in(own_key, 6), axis_at), (parts,), jnp.float32, least / len(cuts), high / len(cuts))
        return jnp.repeat(jnp.exp(heights), dims[axis_at] // parts).reshape((-1,) + (1,) * (len(dims) - axis_at - 1))

    gain = one(*cuts[0])
    for cut in cuts[1:]:
        gain = gain * one(*cut)
    return gain


def normal_values(own_key, dims, width, bound, cuts=(), kind=jnp.bfloat16):
    level = level_of(own_key, dims, cuts, -0.22, 0.18) if cuts else 1.0
    entries = jax.random.normal(own_key, dims, jnp.float32) * width * level
    return jnp.minimum(jnp.maximum(entries, -bound), bound).astype(kind)


def setup_inputs(seed: int = 0) -> dict:
    key_list = jax.random.split(jax.random.key(seed), 20)
    grouped_head_inputs = normal_values(key_list[0], (TOKENS, 2, CHANNELS), 1.0, 6.0, ((0, 8), (2, 4)))
    head_gate_inputs = normal_values(key_list[1], (TOKENS, 2, CHANNELS), 1.0, 6.0, ((0, 8), (2, 4)))
    unsmoothed_step = draw_unsmoothed_step(jax.random.fold_in(key_list[19], 71), 0)
    head_decay_rate = draw_head_decay_rate(jax.random.fold_in(key_list[19], 71), 0)
    extra_log_decay = draw_extra_log_decay(jax.random.fold_in(key_list[19], 71), 0)
    first_group_keys = normal_values(key_list[5], (TOKENS, STATE_ONE), 1.0, 6.0, ((0, 8),))
    first_group_queries = normal_values(key_list[6], (TOKENS, STATE_ONE), 1.0, 6.0, ((0, 8),))
    second_group_keys = normal_values(key_list[7], (TOKENS, STATE_TWO), 1.0, 6.0, ((0, 8),))
    second_group_queries = normal_values(key_list[8], (TOKENS, STATE_TWO), 1.0, 6.0, ((0, 8),))
    head_input_filter = normal_values(key_list[9], (CONV, 2, CHANNELS), 0.5, 3.0, ((2, 4),), jnp.float32)
    first_group_filter = normal_values(key_list[10], (CONV, 2, STATE_ONE), 0.5, 3.0, (), jnp.float32)
    second_group_filter = normal_values(key_list[11], (CONV, 2, STATE_TWO), 0.5, 3.0, (), jnp.float32)
    head_norm_gain = jnp.clip(1.0 + 0.18 * jax.random.normal(key_list[12], (2, CHANNELS), jnp.float32), 0.1, 1.9)
    output_weight = normal_values(key_list[13], (2, CHANNELS, D), (2 * CHANNELS) ** -0.5, 0.125, ((2, 4),))
    residual = draw_residual(jax.random.fold_in(key_list[19], 71), 0)
    channel_norm_gain = jnp.clip(1.0 + 0.18 * jax.random.normal(key_list[15], (D,), jnp.float32), 0.1, 1.9)
    channel_gate_weight = normal_values(key_list[16], (D, FF), D ** -0.5, 0.125, ((0, 8), (1, 4)))
    channel_up_weight = normal_values(key_list[17], (D, FF), D ** -0.5, 0.125, ((0, 8), (1, 4)))
    channel_down_weight = normal_values(key_list[18], (D, FF), FF ** -0.5, 0.078125, ((0, 8), (1, 4)))
    return dict(grouped_head_inputs=grouped_head_inputs, head_gate_inputs=head_gate_inputs, unsmoothed_step=unsmoothed_step, head_decay_rate=head_decay_rate, extra_log_decay=extra_log_decay, first_group_keys=first_group_keys, first_group_queries=first_group_queries, second_group_keys=second_group_keys, second_group_queries=second_group_queries, head_input_filter=head_input_filter, first_group_filter=first_group_filter, second_group_filter=second_group_filter, head_norm_gain=head_norm_gain, output_weight=output_weight, residual=residual, channel_norm_gain=channel_norm_gain, channel_gate_weight=channel_gate_weight, channel_up_weight=channel_up_weight, channel_down_weight=channel_down_weight)


EPSILON = 1e-06
PRECISE = lax.Precision.HIGHEST

def causal_taps(values, taps):
    length = values.shape[0]
    zeros_rows = jnp.zeros((CONV - 1,) + values.shape[1:], jnp.float32)
    padded = jnp.concatenate([zeros_rows, values.astype(jnp.float32)], axis=0)
    running = jnp.zeros(values.shape, jnp.float32)
    for offset in range(CONV):
        running = running + taps[offset].astype(jnp.float32) * padded[offset:offset + length]
    return jax.nn.silu(running)

def block_pass(current, value_rows, log_rows, key_rows, query_rows):
    cumulative = jnp.cumsum(log_rows, axis=0)
    length = value_rows.shape[0]
    causal = jnp.arange(length)[:, None] >= jnp.arange(length)[None, :]
    scores = jnp.dot(query_rows, key_rows.T, precision=PRECISE)
    span_logs = jnp.where(causal[:, :, None], cumulative[:, None, :] - cumulative[None, :, :], -jnp.inf)
    weights = jnp.exp(span_logs) * scores[:, :, None]
    inside = jnp.einsum('lsh,shp->lhp', weights, value_rows, precision=PRECISE)
    carried = jnp.einsum('ls,hps->lhp', query_rows, current, precision=PRECISE) * jnp.exp(cumulative)[:, :, None]
    to_end = jnp.exp(cumulative[-1][None, :] - cumulative)
    update = jnp.einsum('lhp,ls->hps', value_rows * to_end[:, :, None], key_rows, precision=PRECISE)
    new_state = current * jnp.exp(cumulative[-1])[:, None, None] + update
    return (new_state, inside + carried)

def scan_group(value_rows, log_rows, key_rows, query_rows):
    length, head_count, head_width = value_rows.shape
    block_count = length // BLOCK
    initial = jnp.zeros((head_count, head_width, key_rows.shape[1]), jnp.float32)
    blocks = (value_rows.reshape(block_count, BLOCK, head_count, head_width), log_rows.reshape(block_count, BLOCK, head_count), key_rows.reshape(block_count, BLOCK, -1), query_rows.reshape(block_count, BLOCK, -1))

    def advance(current, pieces):
        return block_pass(current, pieces[0], pieces[1], pieces[2], pieces[3])
    final_state, outputs = lax.scan(advance, initial, blocks)
    return outputs.reshape(length, head_count, head_width)

def reference(grouped_head_inputs, head_gate_inputs, unsmoothed_step, head_decay_rate, extra_log_decay, first_group_keys, first_group_queries, second_group_keys, second_group_queries, head_input_filter, first_group_filter, second_group_filter, head_norm_gain, output_weight, residual, channel_norm_gain, channel_gate_weight, channel_up_weight, channel_down_weight):
    length = grouped_head_inputs.shape[0]
    conv_heads = causal_taps(grouped_head_inputs, head_input_filter)
    keys_one = causal_taps(first_group_keys, first_group_filter[:, 0])
    queries_one = causal_taps(first_group_queries, first_group_filter[:, 1])
    keys_two = causal_taps(second_group_keys, second_group_filter[:, 0])
    queries_two = causal_taps(second_group_queries, second_group_filter[:, 1])
    head_step_size = jax.nn.softplus(unsmoothed_step.astype(jnp.float32))
    decay_logarithm = extra_log_decay.astype(jnp.float32) - head_step_size * head_decay_rate.astype(jnp.float32)[None]
    values = conv_heads.reshape(length, 2, GROUP_HEADS, HEAD) * head_step_size[:, :, :, None]
    first = scan_group(values[:, 0], decay_logarithm[:, 0], keys_one, queries_one)
    second = scan_group(values[:, 1], decay_logarithm[:, 1], keys_two, queries_two)
    mixer = jnp.stack([first, second], axis=1)
    gated = mixer * jax.nn.silu(head_gate_inputs.astype(jnp.float32)).reshape(length, 2, GROUP_HEADS, HEAD)
    scaled = gated * lax.rsqrt(lax.optimization_barrier(jnp.mean(gated * gated, axis=3, keepdims=True)) + EPSILON)
    mixed = (scaled.reshape(length, 2, CHANNELS) * head_norm_gain.astype(jnp.float32)[None]).astype(jnp.bfloat16)
    projected = jnp.dot(mixed.reshape(length, 2 * CHANNELS), output_weight.reshape(2 * CHANNELS, D), preferred_element_type=jnp.float32)
    stream = (residual.astype(jnp.float32) + projected).astype(jnp.bfloat16)
    stream_wide = stream.astype(jnp.float32)
    normed = (stream_wide * lax.rsqrt(lax.optimization_barrier(jnp.mean(stream_wide * stream_wide, axis=1, keepdims=True)) + EPSILON) * channel_norm_gain.astype(jnp.float32)[None]).astype(jnp.bfloat16)
    gate = jnp.dot(normed, channel_gate_weight, preferred_element_type=jnp.float32)
    upward = jnp.dot(normed, channel_up_weight, preferred_element_type=jnp.float32)
    hidden = (jax.nn.silu(gate) * upward).astype(jnp.bfloat16)
    block_width = FF // N_TP
    summed = jnp.zeros((length, D), jnp.float32)
    for index in range(N_TP):
        piece = hidden[:, index * block_width:(index + 1) * block_width]
        columns = channel_down_weight[:, index * block_width:(index + 1) * block_width]
        partial_value = lax.dot_general(piece, columns, (((1,), (1,)), ((), ())), preferred_element_type=jnp.float32)
        rounded = lax.optimization_barrier(partial_value.astype(jnp.bfloat16))
        summed = summed + rounded.astype(jnp.float32)
    return (stream_wide + 0.5 * summed).astype(jnp.bfloat16)
```

```python
import functools

import jax
import jax.numpy as jnp
from jax import lax
from jax.experimental import pallas as pl
from jax.experimental.pallas import tpu as pltpu
from jax.sharding import PartitionSpec as P

HEAD = 64
CONV = 4
BLOCK = 128
RIM = 16
EPSILON = 1e-06
LANES = 128
VMEM_LIMIT = 63 << 20
MESH = pl.DeviceIdType.MESH


def rows_of(b):
    return pl.ds(pl.multiple_of(b * BLOCK, BLOCK), BLOCK)


def spread(columns, first, count):
    parts = [
        jnp.broadcast_to(columns[:, h : h + 1], (columns.shape[0], HEAD))
        for h in range(first, first + count)
    ]
    return jnp.concatenate(parts, axis=1)


def sigmoid(x):
    return 1.0 / (1.0 + jnp.exp(-x))


def layer_kernel(
    n, tp, heads, s1, s2, split,
    x_ref, gate_ref, log_ref, step_ref, taps_ref, hgain_ref, wout_ref, res_ref, cgain_ref,
    wg_ref, wu_ref, wd_ref,
    out_ref,
    xs, rim, vals, kq, cums, st, stsend, strecv, mix, stream, normed, weights, hidden,
    give, give_recv, sums, sums_recv,
    rim_sems, st_send, st_recv, m_send, m_fwd, m_recv, r_send, r_fwd, r_recv,
    p_send, p_fwd, p_recv, w_local, w_pair, w_send, w_recv, g_send, g_recv, s_send, s_recv,
):
    me = lax.axis_index("sp")
    t = lax.axis_index("tp")
    half = heads * HEAD
    wide = 2 * half
    nb = x_ref.shape[0] // BLOCK
    nx = tp // 2
    core = lax.rem(t, 2)
    my_x = t // 2
    partner = my_x * 2 + (1 - core)

    m = n // 2
    q = me // 2
    y = lax.rem(me, 2)
    pair = q * 2 + (1 - y)
    shard = wg_ref.shape[-2]
    tokens = x_ref.shape[0]
    sources = (wg_ref, wu_ref, wd_ref)
    part = weights.shape[2]

    def half_of(w, which):
        if split:
            return sources[w].at[which]
        return sources[w].at[:, pl.ds(pl.multiple_of(which * part, part), part)]

    def unit(w, s):
        return weights.at[w, pl.ds(pl.multiple_of(s * shard, shard), shard)]

    def keep_own(w):
        return pltpu.make_async_copy(half_of(w, y), unit(w, me), w_local.at[w])

    def give_pair(w):
        return pltpu.make_async_remote_copy(
            src_ref=half_of(w, 1 - y),
            dst_ref=unit(w, me),
            send_sem=w_pair.at[w],
            recv_sem=w_recv.at[w, me],
            device_id={"sp": pair},
            device_id_type=MESH,
        )

    def along(w, s, up, own=False):
        return pltpu.make_async_remote_copy(
            src_ref=half_of(w, y) if own else unit(w, s),
            dst_ref=unit(w, s),
            send_sem=w_send.at[int(up), w, s],
            recv_sem=w_recv.at[w, s],
            device_id={"sp": lax.rem(me + 2, n) if up else lax.rem(me + n - 2, n)},
            device_id_type=MESH,
        )

    def send_along(w, s, up, own=False):
        @pl.when(q < m - 1 if up else q > 0)
        def _():
            along(w, s, up, own).start()

    def take_unit(w, s):
        along(w, s, True).wait_recv()

    def start_weights():
        for w in range(2):
            give_pair(w).start()
            send_along(w, me, False, own=True)
            send_along(w, me, True, own=True)
        give_pair(2).start()
        for w in range(3):
            keep_own(w).start()

    def relay(w, d, sel):
        other = lax.rem(y + sel, 2)

        @pl.when(q + d < m)
        def _():
            s = (q + d) * 2 + other
            take_unit(w, s)
            send_along(w, s, False)

            @pl.when(d == 0)
            def _():
                send_along(w, s, True)

        @pl.when((d > 0) & (q - d >= 0))
        def _():
            s = (q - d) * 2 + other
            take_unit(w, s)
            send_along(w, s, True)

    def relay_step(k):
        relay(lax.rem(k, 2), k // 4, lax.rem(k // 2, 2))

    early = 4 * (m - 1)
    points = nb // 2 + (nb + 4) // 2
    per_point = pl.cdiv(max(early - 2, 0), points)

    def relay_point(p):
        for i in range(per_point):
            k = 2 + p * per_point + i

            @pl.when(k < early)
            def _():
                relay_step(k)

    rim_copy = pltpu.make_async_remote_copy(
        src_ref=x_ref.at[pl.ds(x_ref.shape[0] - RIM, RIM)],
        dst_ref=rim,
        send_sem=rim_sems.at[0],
        recv_sem=rim_sems.at[1],
        device_id={"sp": lax.rem(me + 1, n)},
        device_id_type=MESH,
    )

    @pl.when(me < n - 1)
    def _():
        rim_copy.start()

    start_weights()

    @pl.when(me > 0)
    def _():
        rim_copy.wait_recv()
        xs[...] = rim[...].astype(jnp.float32)[RIM - 8 :]

    @pl.when(me == 0)
    def _():
        xs[...] = jnp.zeros_like(xs)

    st[...] = jnp.zeros_like(st)
    row_i = lax.broadcasted_iota(jnp.int32, (BLOCK, BLOCK), 0)
    col_i = lax.broadcasted_iota(jnp.int32, (BLOCK, BLOCK), 1)
    causal = row_i >= col_i
    tri = jnp.where(causal, 1.0, 0.0).astype(jnp.float32)

    def state_update(b, cum):
        last = cum[BLOCK - 1 : BLOCK]
        to_end = jnp.exp(last - cum)
        decay = jnp.exp(last)
        r = rows_of(b)
        for g in range(2):
            k0, size = (wide, s1) if g == 0 else (wide + 2 * s1, s2)
            base = 0 if g == 0 else s1
            keys = kq[r, k0 - wide : k0 - wide + size]
            v = vals[r, g * half : (g + 1) * half].astype(jnp.float32)
            v = (v * spread(to_end, g * heads, heads)).astype(jnp.bfloat16)
            add = lax.dot_general(
                keys, v, (((0,), (0,)), ((), ())), preferred_element_type=jnp.float32
            )
            st[base : base + size] = (
                st[base : base + size] * spread(decay, g * heads, heads) + add
            )

    def first_pass(b, total):
        r = rows_of(b)
        current = x_ref[r].astype(jnp.float32)
        taps = taps_ref[...]
        extended = jnp.concatenate([xs[...], current], axis=0)
        acc = taps[CONV - 1 : CONV] * current
        for k in range(CONV - 1):
            acc = acc + taps[k : k + 1] * pltpu.roll(extended, CONV - 1 - k, 0)[8:]
        xs[...] = current[BLOCK - 8 :]
        acc = acc * sigmoid(acc)
        vals[r] = (acc[:, :wide] * spread(step_ref[r], 0, 2 * heads)).astype(jnp.bfloat16)
        kq[r] = acc[:, wide:].astype(jnp.bfloat16)
        cum = jnp.dot(
            tri, log_ref[r], precision=lax.Precision.HIGHEST, preferred_element_type=jnp.float32
        )
        cums[r] = cum
        state_update(b, cum)

        @pl.when(lax.rem(b, 2) == 1)
        def _():
            relay_point(b // 2)

        return total + cum[BLOCK - 1 : BLOCK]

    total = lax.fori_loop(0, nb, first_pass, jnp.zeros((1, log_ref.shape[1]), jnp.float32))

    states = s1 + s2
    stsend[0:states] = st[...].astype(jnp.bfloat16)
    which = lax.broadcasted_iota(jnp.int32, (RIM, half), 0)
    extra = jnp.zeros((RIM, half), jnp.float32)
    for g in range(2):
        logs = spread(total, g * heads, heads)
        high = logs.astype(jnp.bfloat16).astype(jnp.float32)
        low = logs - high
        extra = jnp.where(which == g, high, extra)
        extra = jnp.where(which == 2 + g, low, extra)
    stsend[states : states + RIM] = extra.astype(jnp.bfloat16)

    def state_copy(to, source):
        return pltpu.make_async_remote_copy(
            src_ref=stsend,
            dst_ref=strecv.at[source],
            send_sem=st_send.at[to],
            recv_sem=st_recv.at[source],
            device_id={"sp": to},
            device_id_type=MESH,
        )

    def send_state(to, carry):
        state_copy(to, me).start()
        return carry

    lax.fori_loop(me + 1, n, send_state, 0)
    st[...] = jnp.zeros_like(st)

    def take_state(source, carry):
        state_copy(n - 1, source).wait_recv()
        got = strecv[source].astype(jnp.float32)
        for g in range(2):
            base, size = (0, s1) if g == 0 else (s1, s2)
            logs = got[states + g : states + g + 1] + got[states + 2 + g : states + 3 + g]
            st[base : base + size] = st[base : base + size] * jnp.exp(logs) + got[base : base + size]
        return carry

    lax.fori_loop(0, me, take_state, 0)

    def share(buf, yy, source, b, sp, to, send, recv):
        piece = buf.at[yy, source, rows_of(b)]
        return pltpu.make_async_remote_copy(
            src_ref=piece,
            dst_ref=piece,
            send_sem=send,
            recv_sem=recv.at[source, b],
            device_id={"sp": sp, "tp": to},
            device_id_type=MESH,
        )

    def across(d):
        return lax.rem(my_x + d, nx) * 2

    def send_own(buf, yy, b, send, recv):
        for d in range(1, nx):
            to = across(d) + core
            share(buf, yy, t, b, me, to, send.at[d, b], recv).start()
        share(buf, yy, t, b, me, partner, send.at[0, b], recv).start()

    def forward(buf, yy, b, fwd, recv):
        for d in range(1, nx):
            source = across(d) + core
            move = share(buf, yy, source, b, me, partner, fwd.at[d, b], recv)
            move.wait_recv()
            move.start()

    def wait_rest(buf, yy, b, send, recv):
        share(buf, yy, partner, b, me, partner, send.at[0, b], recv).wait_recv()
        for d in range(1, nx):
            source = across(d) + (1 - core)
            share(buf, yy, source, b, me, partner, send.at[0, b], recv).wait_recv()

    def send_pair(b):
        for d in range(nx):
            to = across(d) + core
            share(stream, y, t, b, pair, to, p_send.at[d, b], p_recv).start()

    def forward_pair(b):
        for d in range(nx):
            source = across(d) + core
            move = share(stream, 1 - y, source, b, me, partner, p_fwd.at[d, b], p_recv)
            move.wait_recv()
            move.start()

    def wait_pair(b):
        for d in range(nx):
            source = across(d) + (1 - core)
            share(stream, 1 - y, source, b, me, partner, p_fwd.at[d, b], p_recv).wait_recv()

    def second_pass(b):
        r = rows_of(b)
        cum = cums[r]
        cum_t = cum.T
        grown = jnp.exp(cum)
        for g in range(2):
            off, size = (0, s1) if g == 0 else (2 * s1, s2)
            base = 0 if g == 0 else s1
            keys = kq[r, off : off + size]
            queries = kq[r, off + size : off + 2 * size]
            scores = lax.dot_general(
                queries, keys, (((1,), (1,)), ((), ())), preferred_element_type=jnp.float32
            )
            carried = jnp.dot(
                queries,
                st[base : base + size].astype(jnp.bfloat16),
                preferred_element_type=jnp.float32,
            )
            carried = carried * spread(grown, g * heads, heads)
            v = vals[r, g * half : (g + 1) * half]
            outs = []
            for h in range(heads):
                c = g * heads + h
                span = jnp.where(causal, cum[:, c : c + 1] - cum_t[c : c + 1, :], -jnp.inf)
                w = (jnp.exp(span) * scores).astype(jnp.bfloat16)
                lanes = slice(h * HEAD, (h + 1) * HEAD)
                y = jnp.dot(w, v[:, lanes], preferred_element_type=jnp.float32)
                y = y + carried[:, lanes]
                z = gate_ref[r, g * half + h * HEAD : g * half + (h + 1) * HEAD].astype(jnp.float32)
                y = y * (z * sigmoid(z))
                y = y * lax.rsqrt(jnp.mean(y * y, axis=1, keepdims=True) + EPSILON)
                outs.append(y)
            out = jnp.concatenate(outs, axis=1) * hgain_ref[:, g * half : (g + 1) * half]
            mix[0, t, r, g * half : (g + 1) * half] = out.astype(jnp.bfloat16)
        state_update(b, cum)
        send_own(mix, 0, b, m_send, m_recv)

    def project(b):
        r = rows_of(b)
        wait_rest(mix, 0, b, m_send, m_recv)
        acc = res_ref[r].astype(jnp.float32)
        for source in range(tp):
            acc = acc + jnp.dot(
                mix[0, source, r], wout_ref[source], preferred_element_type=jnp.float32
            )
        stream[y, t, r] = acc.astype(jnp.bfloat16)
        send_own(stream, y, b, r_send, r_recv)
        send_pair(b)

    cols = res_ref.shape[1]

    def normalise(yy, b):
        r = rows_of(b)
        parts = [stream[yy, source, r].astype(jnp.float32) for source in range(tp)]
        square = sum(jnp.sum(p * p, axis=1, keepdims=True) for p in parts)
        scale = lax.rsqrt(square / (tp * cols) + EPSILON)
        for source in range(tp):
            lanes = slice(source * cols, (source + 1) * cols)
            normed[yy, r, lanes] = (parts[source] * scale * cgain_ref[:, lanes]).astype(
                jnp.bfloat16
            )

    def stage(b, carry):
        @pl.when(b < nb)
        def _():
            second_pass(b)

        @pl.when(lax.rem(b, 2) == 0)
        def _():
            relay_point(nb // 2 + b // 2)

        @pl.when((b >= 1) & (b < nb + 1))
        def _():
            forward(mix, 0, b - 1, m_fwd, m_recv)

        @pl.when((b >= 2) & (b < nb + 2))
        def _():
            project(b - 2)

        @pl.when((b >= 3) & (b < nb + 3))
        def _():
            forward(stream, y, b - 3, r_fwd, r_recv)
            forward_pair(b - 3)

        @pl.when(b >= 4)
        def _():
            wait_rest(stream, y, b - 4, r_send, r_recv)
            normalise(y, b - 4)
            wait_pair(b - 4)
            normalise(1 - y, b - 4)

        return carry

    lax.fori_loop(0, nb + 4, stage, 0)

    down = 2
    send_along(down, me, False, own=True)
    send_along(down, me, True, own=True)
    take_unit(down, pair)
    send_along(down, pair, False)
    send_along(down, pair, True)

    def late(k, carry):
        relay_step(k)
        return carry

    lax.fori_loop(early, 4 * m, late, 0)
    for w in range(3):
        keep_own(w).wait()

    tall = 2 * BLOCK
    pieces = tokens // tall

    def mix_channels(i, carry):
        yy = i // pieces
        r = pl.ds(pl.multiple_of(lax.rem(i, pieces) * tall, tall), tall)
        rows = normed[yy, r]
        g = jnp.dot(rows, weights[0], preferred_element_type=jnp.float32)
        u = jnp.dot(rows, weights[1], preferred_element_type=jnp.float32)
        hidden[yy, r] = (g * sigmoid(g) * u).astype(jnp.bfloat16)
        return carry

    lax.fori_loop(0, 2 * pieces, mix_channels, 0)

    near = jnp.minimum(q, m - 1 - q)

    def block_at(i):
        d = (i + 1) // 2
        side = jnp.where(lax.rem(i, 2) == 1, q + d, q - d)
        beyond = jnp.where(q < m - 1 - q, i, m - 1 - i)
        return jnp.where(i <= 2 * near, side, beyond)

    width = sums.shape[2]
    units = width // shard
    chunks = tp * cols // width
    per_owner = cols // width

    def shard_at(i):
        return block_at(i // 2) * 2 + lax.rem(y + lax.rem(i, 2), 2)

    def take_down(i):
        s = shard_at(i)

        @pl.when(i >= 2)
        def _():
            take_unit(down, s)

            @pl.when(s > me)
            def _():
                send_along(down, s, False)

            @pl.when(s < me)
            def _():
                send_along(down, s, True)

    def chunk_at(i):
        return shard_at(i) if units == 1 else i

    def product(yy, k, p):
        r = pl.ds(pl.multiple_of(p * tall, tall), tall)
        block = weights[down, pl.ds(pl.multiple_of(k * width, width), width)]
        return lax.dot_general(
            hidden[yy, r], block, (((1,), (1,)), ((), ())), preferred_element_type=jnp.float32
        )

    def give_copy(i, k):
        return pltpu.make_async_remote_copy(
            src_ref=give.at[lax.rem(i, 2)],
            dst_ref=give_recv.at[k],
            send_sem=g_send.at[lax.rem(i, 2)],
            recv_sem=g_recv.at[k],
            device_id={"tp": partner},
            device_id_type=MESH,
        )

    mine = my_x * 2 + y

    def sum_copy(i, k, source):
        return pltpu.make_async_remote_copy(
            src_ref=sums.at[lax.rem(i, 2)],
            dst_ref=sums_recv.at[source, lax.rem(k, per_owner)],
            send_sem=s_send.at[lax.rem(i, 2)],
            recv_sem=s_recv.at[source, lax.rem(k, per_owner)],
            device_id={"sp": q * 2 + core, "tp": k // per_owner},
            device_id_type=MESH,
        )

    def to_self(k):
        return (k // per_owner == t) & (y == core)

    def give_half(i):
        k = chunk_at(i)

        @pl.when(i >= 2)
        def _():
            give_copy(i, k).wait_send()

        def one(p, carry):
            r = pl.ds(pl.multiple_of(p * tall, tall), tall)
            give[lax.rem(i, 2), r] = product(1 - core, k, p).astype(jnp.bfloat16)
            return carry

        lax.fori_loop(0, pieces, one, 0)
        give_copy(i, k).start()

    def sum_half(i):
        k = chunk_at(i)

        @pl.when(i >= 2)
        def _():
            before = chunk_at(i - 2)

            @pl.when(jnp.logical_not(to_self(before)))
            def _():
                sum_copy(i, before, mine).wait_send()

        give_copy(i, k).wait_recv()

        def one(p, carry):
            r = pl.ds(pl.multiple_of(p * tall, tall), tall)
            both = product(core, k, p) + give_recv[k, r].astype(jnp.float32)
            sums[lax.rem(i, 2), r] = both.astype(jnp.bfloat16)
            return carry

        lax.fori_loop(0, pieces, one, 0)

        @pl.when(to_self(k))
        def _():
            sums_recv[mine, lax.rem(k, per_owner)] = sums[lax.rem(i, 2)]

        @pl.when(jnp.logical_not(to_self(k)))
        def _():
            sum_copy(i, k, mine).start()

    if units > 1:

        def take_all(i, carry):
            take_down(i)
            return carry

        lax.fori_loop(0, n, take_all, 0)

    def chunk_step(i, carry):
        @pl.when(i < chunks)
        def _():
            if units == 1:
                take_down(i)
            give_half(i)

        @pl.when(i >= 1)
        def _():
            sum_half(i - 1)

        return carry

    lax.fori_loop(0, chunks + 1, chunk_step, 0)

    group = sums_recv.shape[0]
    for source in range(group):
        for c in range(per_owner):

            @pl.when((source != mine) | (y != core))
            def _():
                sum_copy(0, c, source).wait_recv()

    def finish(p, carry):
        r = pl.ds(pl.multiple_of(p * tall, tall), tall)
        for c in range(per_owner):
            lanes = slice(c * width, (c + 1) * width)
            total = sums_recv[0, c, r].astype(jnp.float32)
            for source in range(1, group):
                total = total + sums_recv[source, c, r].astype(jnp.float32)
            own = stream[y, t, r, lanes].astype(jnp.float32)
            out_ref[r, lanes] = (own + 0.5 * total).astype(jnp.bfloat16)
        return carry

    lax.fori_loop(0, pieces, finish, 0)

    for i in range(max(chunks - 2, 0), chunks):
        last = chunk_at(i)
        give_copy(i, last).wait_send()

        @pl.when(jnp.logical_not(to_self(last)))
        def _():
            sum_copy(i, last, mine).wait_send()

    @pl.when(me < n - 1)
    def _():
        rim_copy.wait_send()

    def end_state(to, carry):
        state_copy(to, me).wait_send()
        return carry

    lax.fori_loop(me + 1, n, end_state, 0)

    def end_shares(b, carry):
        for buf, yy, send, fwd, recv in (
            (mix, 0, m_send, m_fwd, m_recv),
            (stream, y, r_send, r_fwd, r_recv),
        ):
            for d in range(nx):
                share(buf, yy, t, b, me, partner, send.at[d, b], recv).wait_send()
            for d in range(1, nx):
                share(buf, yy, t, b, me, partner, fwd.at[d, b], recv).wait_send()
        for d in range(nx):
            share(stream, y, t, b, me, partner, p_send.at[d, b], p_recv).wait_send()
            share(stream, y, t, b, me, partner, p_fwd.at[d, b], p_recv).wait_send()
        return carry

    lax.fori_loop(0, nb, end_shares, 0)

    def end_weights(s, carry):
        for w in range(3):
            @pl.when((s // 2 >= q) & (q > 0))
            def _():
                along(w, s, False).wait_send()

            @pl.when((s // 2 <= q) & (q < m - 1))
            def _():
                along(w, s, True).wait_send()

        return carry

    lax.fori_loop(0, n, end_weights, 0)
    for w in range(3):
        give_pair(w).wait_send()


def layer(x, gate, logs, step, taps, hgain, wout, residual, cgain, wg, wu, wd, heads, s1, s2):
    n, tp = lax.axis_size("sp"), lax.axis_size("tp")
    tokens, lanes = x.shape
    half = heads * HEAD
    cols = residual.shape[1]
    nb = tokens // BLOCK
    shard, units = wg.shape
    part = units // 2
    split = part % LANES != 0
    if split:
        wg, wu, wd = (w.reshape(shard, 2, part).swapaxes(0, 1) for w in (wg, wu, wd))
    width = max(shard, min(cols, 2 * LANES))
    chunks = tp * cols // width
    vmem = pl.BlockSpec(memory_space=pltpu.VMEM)
    hbm = pl.BlockSpec(memory_space=pl.ANY)
    dma = pltpu.SemaphoreType.DMA
    return pl.pallas_call(
        functools.partial(layer_kernel, n, tp, heads, s1, s2, split),
        out_shape=jax.ShapeDtypeStruct((tokens, cols), jnp.bfloat16),
        in_specs=[vmem] * 9 + [hbm] * 3,
        out_specs=vmem,
        scratch_shapes=[
            pltpu.VMEM((8, lanes), jnp.float32),
            pltpu.VMEM((RIM, lanes), jnp.bfloat16),
            pltpu.VMEM((tokens, 2 * half), jnp.bfloat16),
            pltpu.VMEM((tokens, 2 * (s1 + s2)), jnp.bfloat16),
            pltpu.VMEM((tokens, logs.shape[1]), jnp.float32),
            pltpu.VMEM((s1 + s2, half), jnp.float32),
            pltpu.VMEM((s1 + s2 + RIM, half), jnp.bfloat16),
            pltpu.VMEM((n, s1 + s2 + RIM, half), jnp.bfloat16),
            pltpu.VMEM((1, tp, tokens, 2 * half), jnp.bfloat16),
            pltpu.VMEM((2, tp, tokens, cols), jnp.bfloat16),
            pltpu.VMEM((2, tokens, tp * cols), jnp.bfloat16),
            pltpu.VMEM((3, n * shard, part), jnp.bfloat16),
            pltpu.VMEM((2, tokens, part), jnp.bfloat16),
            pltpu.VMEM((2, tokens, width), jnp.bfloat16),
            pltpu.VMEM((chunks, tokens, width), jnp.bfloat16),
            pltpu.VMEM((2, tokens, width), jnp.bfloat16),
            pltpu.VMEM((tp, cols // width, tokens, width), jnp.bfloat16),
            dma((2,)),
            dma((n,)),
            dma((n,)),
            dma((tp, nb)),
            dma((tp, nb)),
            dma((tp, nb)),
            dma((tp, nb)),
            dma((tp, nb)),
            dma((tp, nb)),
            dma((tp, nb)),
            dma((tp, nb)),
            dma((tp, nb)),
            dma((3,)),
            dma((3,)),
            dma((2, 3, n)),
            dma((3, n)),
            dma((2,)),
            dma((chunks,)),
            dma((2,)),
            dma((tp, cols // width)),
        ],
        compiler_params=pltpu.CompilerParams(
            has_side_effects=True, vmem_limit_bytes=VMEM_LIMIT
        ),
        name="layer",
    )(x, gate, logs, step, taps, hgain, wout, residual, cgain, wg, wu, wd)


def shards(
    grouped_head_inputs,
    head_gate_inputs,
    unsmoothed_step,
    head_decay_rate,
    extra_log_decay,
    first_group_keys,
    first_group_queries,
    second_group_keys,
    second_group_queries,
    head_input_filter,
    first_group_filter,
    second_group_filter,
    head_norm_gain,
    output_weight,
    residual,
    channel_norm_gain,
    channel_gate_weight,
    channel_up_weight,
    channel_down_weight,
):
    tp = lax.axis_size("tp")
    tokens = grouped_head_inputs.shape[0]
    heads = head_decay_rate.shape[1]
    half = heads * HEAD
    s1, s2 = first_group_keys.shape[1], second_group_keys.shape[1]
    x = jnp.concatenate(
        [
            grouped_head_inputs.reshape(tokens, 2 * half),
            first_group_keys,
            first_group_queries,
            second_group_keys,
            second_group_queries,
        ],
        axis=1,
    )
    taps = jnp.concatenate(
        [
            head_input_filter.reshape(CONV, 2 * half),
            first_group_filter.reshape(CONV, 2 * s1),
            second_group_filter.reshape(CONV, 2 * s2),
        ],
        axis=1,
    )
    step = jax.nn.softplus(unsmoothed_step.reshape(tokens, 2 * heads))
    logs = extra_log_decay.reshape(tokens, 2 * heads) - step * head_decay_rate.reshape(1, -1)
    pad = ((0, 0), (0, BLOCK - 2 * heads))
    wout = output_weight.reshape(2, tp, half, -1).swapaxes(0, 1).reshape(tp, 2 * half, -1)
    return layer(
        x,
        head_gate_inputs.reshape(tokens, 2 * half),
        jnp.pad(logs, pad),
        jnp.pad(step, pad),
        taps,
        head_norm_gain.reshape(1, 2 * half),
        wout,
        residual,
        channel_norm_gain.reshape(1, -1),
        channel_gate_weight,
        channel_up_weight,
        channel_down_weight,
        heads,
        s1,
        s2,
    )


def solution(mesh):
    return jax.shard_map(
        shards,
        mesh=mesh,
        in_specs=(
            P("sp", None, "tp"),
            P("sp", None, "tp"),
            P("sp", None, "tp"),
            P(None, "tp"),
            P("sp", None, "tp"),
            P("sp", None),
            P("sp", None),
            P("sp", None),
            P("sp", None),
            P(None, None, "tp"),
            P(),
            P(),
            P(None, "tp"),
            P(None, None, "tp"),
            P("sp", "tp"),
            P(),
            P("sp", "tp"),
            P("sp", "tp"),
            P("sp", "tp"),
        ),
        out_specs=P("sp", "tp"),
        check_vma=False,
    )
```

```python
import functools

import jax
import jax.numpy as jnp
from jax import lax
from jax.experimental import pallas as pl
from jax.experimental.pallas import tpu as pltpu
from jax.sharding import PartitionSpec as P

HEAD = 64
CONV = 4
BLOCK = 128
RIM = 16
EPSILON = 1e-06
LANES = 128
VMEM_LIMIT = 63 << 20
MESH = pl.DeviceIdType.MESH


def rows_of(b):
    return pl.ds(pl.multiple_of(b * BLOCK, BLOCK), BLOCK)


def spread(columns, first, count):
    parts = [
        jnp.broadcast_to(columns[:, h : h + 1], (columns.shape[0], HEAD))
        for h in range(first, first + count)
    ]
    return jnp.concatenate(parts, axis=1)


def sigmoid(x):
    return 1.0 / (1.0 + jnp.exp(-x))


def layer_kernel(
    n, tp, heads, s1, s2, split,
    x_ref, keys1_ref, queries1_ref, keys2_ref, queries2_ref, unsmoothed_ref, extra_ref, rate_ref,
    head_taps_ref, taps1_ref, taps2_ref, hgain_ref, cgain_ref,
    gate_in, wout_in, res_in, wg_ref, wu_ref, wd_ref,
    out_ref,
    gate_ref, wout_ref, res_ref, in_sems, taps_ref, step_rows, log_rows, rim_out, xs, rim, vals, kq, cums, st, stsend, strecv, mix, stream, normed, weights, hidden,
    give, give_recv, sums, across_recv, ready, sums_recv,
    rim_sems, st_send, st_recv, m_send, m_fwd, m_recv, r_send, r_fwd, r_recv,
    p_send, p_fwd, p_recv, w_local, w_pair, w_send, w_recv,
    g_send, g_recv, a_send, a_recv, s_send, s_recv,
):
    me = lax.axis_index("sp")
    t = lax.axis_index("tp")
    half = heads * HEAD
    wide = 2 * half
    nb = x_ref.shape[0] // BLOCK
    nx = tp // 2
    core = lax.rem(t, 2)
    my_x = t // 2
    partner = my_x * 2 + (1 - core)

    m = n // 2
    q = me // 2
    y = lax.rem(me, 2)
    pair = q * 2 + (1 - y)
    shard = wg_ref.shape[-2]
    tokens = x_ref.shape[0]
    sources = (wg_ref, wu_ref, wd_ref)
    part = weights.shape[2]

    def half_of(w, which):
        if split:
            return sources[w].at[which]
        return sources[w].at[:, pl.ds(pl.multiple_of(which * part, part), part)]

    def unit(w, s):
        return weights.at[w, pl.ds(pl.multiple_of(s * shard, shard), shard)]

    def keep_own(w):
        return pltpu.make_async_copy(half_of(w, y), unit(w, me), w_local.at[w])

    def give_pair(w):
        return pltpu.make_async_remote_copy(
            src_ref=half_of(w, 1 - y),
            dst_ref=unit(w, me),
            send_sem=w_pair.at[w],
            recv_sem=w_recv.at[w, me],
            device_id={"sp": pair},
            device_id_type=MESH,
        )

    def along(w, s, up, own=False):
        return pltpu.make_async_remote_copy(
            src_ref=half_of(w, y) if own else unit(w, s),
            dst_ref=unit(w, s),
            send_sem=w_send.at[int(up), w, s],
            recv_sem=w_recv.at[w, s],
            device_id={"sp": lax.rem(me + 2, n) if up else lax.rem(me + n - 2, n)},
            device_id_type=MESH,
        )

    def send_along(w, s, up, own=False):
        @pl.when(q < m - 1 if up else q > 0)
        def _():
            along(w, s, up, own).start()

    def take_unit(w, s):
        along(w, s, True).wait_recv()

    def start_weights():
        for w in range(2):
            give_pair(w).start()
            send_along(w, me, False, own=True)
        send_along(0, me, True, own=True)
        for w in range(3):
            keep_own(w).start()

    def relay_down(k):
        w, d, sel = lax.rem(k, 2), k // 4, lax.rem(k // 2, 2)

        @pl.when(q + d < m)
        def _():
            s = (q + d) * 2 + lax.rem(y + sel, 2)
            take_unit(w, s)
            send_along(w, s, False)

    def relay_up(k):
        w, d, sel = lax.rem(k, 2), k // 4, lax.rem(k // 2, 2)

        @pl.when(q - d >= 0)
        def _():
            s = (q - d) * 2 + lax.rem(y + sel, 2)
            take_unit(w, s)
            send_along(w, s, True)

    early = 4 * (m - 1)
    stride = max(m - 3, 0)

    def relay_points(b, first, go):
        for j, at in enumerate((0, 1, 3, 4)):

            @pl.when(b == first + at)
            def _():
                if m > 2:
                    go(4 + j)

        for j in range(4):

            @pl.when(b == first + nb - 2 + j)
            def _():
                for i in range(stride):
                    go(8 + j * stride + i)

    later = [
        pltpu.make_async_copy(source, place, in_sems.at[i])
        for i, (source, place) in enumerate(
            ((gate_in, gate_ref), (wout_in, wout_ref), (res_in, res_ref))
        )
    ]

    def tokens_of(b):
        r = rows_of(b)
        second = jnp.concatenate([keys2_ref[:, r], queries2_ref[:, r]], axis=0)
        return jnp.concatenate(
            [
                x_ref[r].astype(jnp.float32),
                keys1_ref[r].astype(jnp.float32),
                queries1_ref[r].astype(jnp.float32),
                second.astype(jnp.float32).T,
            ],
            axis=1,
        )

    rim_copy = pltpu.make_async_remote_copy(
        src_ref=rim_out,
        dst_ref=rim,
        send_sem=rim_sems.at[0],
        recv_sem=rim_sems.at[1],
        device_id={"sp": lax.rem(me + 1, n)},
        device_id_type=MESH,
    )

    start_weights()

    @pl.when(me < n - 1)
    def _():
        rim_out[...] = tokens_of(nb - 1)[BLOCK - RIM :].astype(jnp.bfloat16)
        rim_copy.start()

    for copy in later:
        copy.start()

    for g in range(2):
        taps_ref[:, g * half : (g + 1) * half] = head_taps_ref[:, g, :]
        taps_ref[:, wide + g * s1 : wide + (g + 1) * s1] = taps1_ref[:, g, :]
    taps_ref[:, wide + 2 * s1 :] = jnp.concatenate([taps2_ref[:, 0, :], taps2_ref[:, 1, :]], axis=1)

    unsmoothed = unsmoothed_ref[...]
    steps = jnp.maximum(unsmoothed, 0.0) + jnp.log1p(jnp.exp(-jnp.abs(unsmoothed)))
    step_rows[...] = jnp.zeros_like(step_rows)
    log_rows[...] = jnp.zeros_like(log_rows)
    for g in range(2):
        for h in range(heads):
            c = g * heads + h
            row = steps[g, h : h + 1]
            step_rows[c : c + 1] = row
            log_rows[c : c + 1] = extra_ref[g, h : h + 1] - row * rate_ref[g, h]

    @pl.when(me > 0)
    def _():
        rim_copy.wait_recv()
        xs[...] = rim[...].astype(jnp.float32)[RIM - 8 :]

    @pl.when(me == 0)
    def _():
        xs[...] = jnp.zeros_like(xs)

    st[...] = jnp.zeros_like(st)
    row_i = lax.broadcasted_iota(jnp.int32, (BLOCK, BLOCK), 0)
    col_i = lax.broadcasted_iota(jnp.int32, (BLOCK, BLOCK), 1)
    causal = row_i >= col_i
    tri = jnp.where(row_i <= col_i, 1.0, 0.0).astype(jnp.float32)
    rows8 = log_rows.shape[0]

    def state_update(b, cum):
        last = cum[BLOCK - 1 : BLOCK]
        to_end = jnp.exp(last - cum)
        decay = jnp.exp(last)
        r = rows_of(b)
        for g in range(2):
            k0, size = (wide, s1) if g == 0 else (wide + 2 * s1, s2)
            base = 0 if g == 0 else s1
            keys = kq[r, k0 - wide : k0 - wide + size]
            v = vals[r, g * half : (g + 1) * half].astype(jnp.float32)
            v = (v * spread(to_end, g * heads, heads)).astype(jnp.bfloat16)
            add = lax.dot_general(
                keys, v, (((0,), (0,)), ((), ())), preferred_element_type=jnp.float32
            )
            st[base : base + size] = (
                st[base : base + size] * spread(decay, g * heads, heads) + add
            )

    def first_pass(b, total):
        r = rows_of(b)
        current = tokens_of(b)
        taps = taps_ref[...]
        extended = jnp.concatenate([xs[...], current], axis=0)
        acc = taps[CONV - 1 : CONV] * current
        for k in range(CONV - 1):
            acc = acc + taps[k : k + 1] * pltpu.roll(extended, CONV - 1 - k, 0)[8:]
        xs[...] = current[BLOCK - 8 :]
        acc = acc * sigmoid(acc)
        cum_rows = jnp.dot(
            log_rows[:, r], tri, precision=lax.Precision.HIGHEST, preferred_element_type=jnp.float32
        )
        fill = jnp.zeros((BLOCK - 2 * rows8, BLOCK), jnp.float32)
        cum = jnp.concatenate([cum_rows, step_rows[:, r], fill], axis=0).T
        cums[r] = cum
        vals[r] = (acc[:, :wide] * spread(cum, rows8, 2 * heads)).astype(jnp.bfloat16)
        kq[r] = acc[:, wide:].astype(jnp.bfloat16)
        state_update(b, cum)

        return total + cum[BLOCK - 1 : BLOCK]

    total = lax.fori_loop(0, nb, first_pass, jnp.zeros((1, BLOCK), jnp.float32))

    states = s1 + s2

    def pack_state(total):
        stsend[0:states] = st[...].astype(jnp.bfloat16)
        which = lax.broadcasted_iota(jnp.int32, (RIM, half), 0)
        extra = jnp.zeros((RIM, half), jnp.float32)
        for g in range(2):
            logs = total[g]
            high = logs.astype(jnp.bfloat16).astype(jnp.float32)
            low = logs - high
            extra = jnp.where(which == g, high, extra)
            extra = jnp.where(which == 2 + g, low, extra)
        stsend[states : states + RIM] = extra.astype(jnp.bfloat16)

    def logs_of(got):
        return [
            got[states + g : states + g + 1] + got[states + 2 + g : states + 3 + g]
            for g in range(2)
        ]

    def state_copy(to, source):
        return pltpu.make_async_remote_copy(
            src_ref=stsend,
            dst_ref=strecv.at[source],
            send_sem=st_send.at[to],
            recv_sem=st_recv.at[source],
            device_id={"sp": to},
            device_id_type=MESH,
        )

    def send_state(to, carry):
        state_copy(to, me).start()
        return carry

    own_logs = [spread(total, g * heads, heads) for g in range(2)]

    @pl.when(y == 0)
    def _():
        pack_state(own_logs)
        state_copy(pair, me).start()

    @pl.when(y == 1)
    def _():
        state_copy(me, pair).wait_recv()
        got = strecv[pair].astype(jnp.float32)
        for g in range(2):
            base, size = (0, s1) if g == 0 else (s1, s2)
            st[base : base + size] = (
                st[base : base + size] + got[base : base + size] * jnp.exp(own_logs[g])
            )
        both = [a + b for a, b in zip(logs_of(got), own_logs)]
        pack_state(both)
        lax.fori_loop(me + 1, n, send_state, 0)

    send_along(1, me, True, own=True)
    for w in range(2):
        take_unit(w, pair)
        send_along(w, pair, False)
        send_along(w, pair, True)
    st[...] = jnp.zeros_like(st)

    def add_state(source):
        got = strecv[source].astype(jnp.float32)
        logs = logs_of(got)
        for g in range(2):
            base, size = (0, s1) if g == 0 else (s1, s2)
            st[base : base + size] = (
                st[base : base + size] * jnp.exp(logs[g]) + got[base : base + size]
            )

    def take_state(before, carry):
        source = before * 2 + 1
        state_copy(n - 1, source).wait_recv()
        add_state(source)
        return carry

    lax.fori_loop(0, q, take_state, 0)

    @pl.when(y == 1)
    def _():
        add_state(pair)

    def share(buf, yy, source, b, sp, to, send, recv):
        piece = buf.at[yy, source, rows_of(b)]
        return pltpu.make_async_remote_copy(
            src_ref=piece,
            dst_ref=piece,
            send_sem=send,
            recv_sem=recv.at[source, b],
            device_id={"sp": sp, "tp": to},
            device_id_type=MESH,
        )

    def across(d):
        return lax.rem(my_x + d, nx) * 2

    def send_own(buf, yy, b, send, recv):
        for d in range(1, nx):
            to = across(d) + core
            share(buf, yy, t, b, me, to, send.at[d, b], recv).start()
        share(buf, yy, t, b, me, partner, send.at[0, b], recv).start()

    def forward(buf, yy, b, fwd, recv):
        for d in range(1, nx):
            source = across(d) + core
            move = share(buf, yy, source, b, me, partner, fwd.at[d, b], recv)
            move.wait_recv()
            move.start()

    def wait_rest(buf, yy, b, send, recv):
        share(buf, yy, partner, b, me, partner, send.at[0, b], recv).wait_recv()
        for d in range(1, nx):
            source = across(d) + (1 - core)
            share(buf, yy, source, b, me, partner, send.at[0, b], recv).wait_recv()

    def send_pair(b):
        share(stream, y, t, b, pair, t, p_send.at[0, b], p_recv).start()

    def forward_pair(b):
        for d in range(nx):
            source = across(d) + core
            move = share(stream, 1 - y, source, b, me, partner, p_fwd.at[d, b], p_recv)
            move.wait_recv()
            move.start()

    def wait_pair(b):
        for d in range(nx):
            source = across(d) + (1 - core)
            share(stream, 1 - y, source, b, me, partner, p_fwd.at[d, b], p_recv).wait_recv()

    def second_pass(b):
        r = rows_of(b)
        cum = cums[r]
        cum_t = cum.T
        grown = jnp.exp(cum)
        for g in range(2):
            off, size = (0, s1) if g == 0 else (2 * s1, s2)
            base = 0 if g == 0 else s1
            keys = kq[r, off : off + size]
            queries = kq[r, off + size : off + 2 * size]
            scores = lax.dot_general(
                queries, keys, (((1,), (1,)), ((), ())), preferred_element_type=jnp.float32
            )
            carried = jnp.dot(
                queries,
                st[base : base + size].astype(jnp.bfloat16),
                preferred_element_type=jnp.float32,
            )
            carried = carried * spread(grown, g * heads, heads)
            v = vals[r, g * half : (g + 1) * half]
            outs = []
            for h in range(heads):
                c = g * heads + h
                span = jnp.where(causal, cum[:, c : c + 1] - cum_t[c : c + 1, :], -jnp.inf)
                w = (jnp.exp(span) * scores).astype(jnp.bfloat16)
                lanes = slice(h * HEAD, (h + 1) * HEAD)
                y = jnp.dot(w, v[:, lanes], preferred_element_type=jnp.float32)
                y = y + carried[:, lanes]
                z = gate_ref[r, g * half + h * HEAD : g * half + (h + 1) * HEAD].astype(jnp.float32)
                y = y * (z * sigmoid(z))
                y = y * lax.rsqrt(jnp.mean(y * y, axis=1, keepdims=True) + EPSILON)
                outs.append(y)
            out = jnp.concatenate(outs, axis=1) * hgain_ref[g : g + 1]
            mix[0, t, r, g * half : (g + 1) * half] = out.astype(jnp.bfloat16)
        state_update(b, cum)
        send_own(mix, 0, b, m_send, m_recv)

    def project(b):
        r = rows_of(b)
        wait_rest(mix, 0, b, m_send, m_recv)
        acc = res_ref[r].astype(jnp.float32)
        for source in range(tp):
            for g in range(2):
                acc = acc + jnp.dot(
                    mix[0, source, r, g * half : (g + 1) * half],
                    wout_ref[g, source * half : (source + 1) * half],
                    preferred_element_type=jnp.float32,
                )
        stream[y, t, r] = acc.astype(jnp.bfloat16)
        send_own(stream, y, b, r_send, r_recv)
        send_pair(b)

    cols = res_ref.shape[1]

    def normalise(yy, b):
        r = rows_of(b)
        parts = [stream[yy, source, r].astype(jnp.float32) for source in range(tp)]
        square = sum(jnp.sum(p * p, axis=1, keepdims=True) for p in parts)
        scale = lax.rsqrt(square / (tp * cols) + EPSILON)
        for source in range(tp):
            lanes = slice(source * cols, (source + 1) * cols)
            normed[yy, r, lanes] = (parts[source] * scale * cgain_ref[:, lanes]).astype(
                jnp.bfloat16
            )

    down = 2

    def stage(b, carry):
        @pl.when(b < nb)
        def _():
            second_pass(b)

        relay_points(b, 0, relay_down)
        relay_points(b, 1, relay_up)

        @pl.when((b >= 1) & (b < nb + 1))
        def _():
            forward(mix, 0, b - 1, m_fwd, m_recv)

        @pl.when((b >= 2) & (b < nb + 2))
        def _():
            project(b - 2)

        @pl.when(b == nb)
        def _():
            give_pair(2).start()

        @pl.when(b == nb + 3)
        def _():
            send_along(down, me, False, own=True)
            send_along(down, me, True, own=True)

        @pl.when((b >= 3) & (b < nb + 3))
        def _():
            forward(stream, y, b - 3, r_fwd, r_recv)
            for d in range(1, nx):
                source = across(d) + core
                share(stream, y, source, b - 3, pair, t, p_send.at[d, b - 3], p_recv).start()

        @pl.when((b >= 4) & (b < nb + 4))
        def _():
            wait_rest(stream, y, b - 4, r_send, r_recv)
            normalise(y, b - 4)

        @pl.when((b >= 6) & (b < nb + 6))
        def _():
            forward_pair(b - 6)

        @pl.when(b >= 7)
        def _():
            wait_pair(b - 7)
            normalise(1 - y, b - 7)

        return carry

    for copy in later:
        copy.wait()
    lax.fori_loop(0, nb + 7, stage, 0)

    between = (q > 0) & (q < m - 1)

    def relay_far(d):
        for sel in range(2):

            @pl.when(between & (q + d < m))
            def _():
                s = (q + d) * 2 + sel
                take_unit(down, s)
                send_along(down, s, False)

            @pl.when(between & (q - d >= 0))
            def _():
                s = (q - d) * 2 + sel
                take_unit(down, s)
                send_along(down, s, True)

    keep_own(down).wait()
    take_unit(down, pair)
    send_along(down, pair, False)
    send_along(down, pair, True)
    relay_far(1)

    def late(k, carry):
        relay_down(k)
        relay_up(k)
        return carry

    lax.fori_loop(max(early, 4), 4 * m, late, 0)
    for w in range(2):
        keep_own(w).wait()

    tall = 2 * BLOCK
    pieces = tokens // tall

    def mix_channels(i, carry):
        yy = i // pieces
        r = pl.ds(pl.multiple_of(lax.rem(i, pieces) * tall, tall), tall)
        rows = normed[yy, r]
        g = jnp.dot(rows, weights[0], preferred_element_type=jnp.float32)
        u = jnp.dot(rows, weights[1], preferred_element_type=jnp.float32)
        hidden[yy, r] = (g * sigmoid(g) * u).astype(jnp.bfloat16)
        return carry

    lax.fori_loop(0, 2 * pieces, mix_channels, 0)

    def pass_on(d, carry):
        relay_far(d)
        return carry

    lax.fori_loop(2, m, pass_on, 0)

    near = jnp.minimum(q, m - 1 - q)

    def block_at(i):
        d = (i + 1) // 2
        side = jnp.where(lax.rem(i, 2) == 1, q + d, q - d)
        beyond = jnp.where(q < m - 1 - q, i, m - 1 - i)
        return jnp.where(i <= 2 * near, side, beyond)

    width = sums.shape[2]
    units = width // shard
    chunks = tp * cols // width
    per_owner = cols // width

    def shard_at(i):
        return block_at(i // 2) * 2 + lax.rem(i, 2)

    def take_down(i):
        @pl.when((i >= 2) & jnp.logical_not(between))
        def _():
            take_unit(down, shard_at(i))

    def chunk_at(i):
        return shard_at(i) if units == 1 else i

    def product(yy, k, p):
        r = pl.ds(pl.multiple_of(p * tall, tall), tall)
        block = weights[down, pl.ds(pl.multiple_of(k * width, width), width)]
        return lax.dot_general(
            hidden[yy, r], block, (((1,), (1,)), ((), ())), preferred_element_type=jnp.float32
        )

    def rows_at(p):
        return pl.ds(pl.multiple_of(p * tall, tall), tall)

    def give_copy(i, k, p):
        return pltpu.make_async_remote_copy(
            src_ref=give.at[lax.rem(i, 2), rows_at(p)],
            dst_ref=give_recv.at[k, rows_at(p)],
            send_sem=g_send.at[lax.rem(i, 2), p],
            recv_sem=g_recv.at[k, p],
            device_id={"tp": partner},
            device_id_type=MESH,
        )

    def pair_copy(i, k, p):
        return pltpu.make_async_remote_copy(
            src_ref=sums.at[lax.rem(i, 2), rows_at(p)],
            dst_ref=across_recv.at[k, rows_at(p)],
            send_sem=a_send.at[lax.rem(i, 2), p],
            recv_sem=a_recv.at[k, p],
            device_id={"sp": pair},
            device_id_type=MESH,
        )

    def owner_copy(i, k, p, source):
        return pltpu.make_async_remote_copy(
            src_ref=ready.at[lax.rem(i, 2), rows_at(p)],
            dst_ref=sums_recv.at[source, lax.rem(k, per_owner), rows_at(p)],
            send_sem=s_send.at[lax.rem(i, 2), p],
            recv_sem=s_recv.at[source, lax.rem(k, per_owner), p],
            device_id={"tp": k // per_owner},
            device_id_type=MESH,
        )

    keeps = core == y

    def give_half(i):
        k = chunk_at(i)

        def one(p, carry):
            @pl.when(i >= 2)
            def _():
                give_copy(i, k, p).wait_send()

            give[lax.rem(i, 2), rows_at(p)] = product(1 - core, k, p).astype(jnp.bfloat16)
            give_copy(i, k, p).start()
            return carry

        lax.fori_loop(0, pieces, one, 0)

    def sum_half(i):
        k = chunk_at(i)

        def one(p, carry):
            @pl.when(jnp.logical_not(keeps) & (i >= 2))
            def _():
                pair_copy(i, k, p).wait_send()

            give_copy(i, k, p).wait_recv()
            both = product(core, k, p) + give_recv[k, rows_at(p)].astype(jnp.float32)
            sums[lax.rem(i, 2), rows_at(p)] = both.astype(jnp.bfloat16)

            @pl.when(jnp.logical_not(keeps))
            def _():
                pair_copy(i, k, p).start()

            return carry

        lax.fori_loop(0, pieces, one, 0)

    def sum_pair(i):
        k = chunk_at(i)
        away = k // per_owner != t
        before = chunk_at(jnp.maximum(i - 2, 0))

        def one(p, carry):
            @pl.when((i >= 2) & (before // per_owner != t))
            def _():
                owner_copy(i, before, p, my_x).wait_send()

            pair_copy(i, k, p).wait_recv()
            r = rows_at(p)
            both = sums[lax.rem(i, 2), r].astype(jnp.float32) + across_recv[k, r].astype(
                jnp.float32
            )
            both = both.astype(jnp.bfloat16)

            @pl.when(away)
            def _():
                ready[lax.rem(i, 2), r] = both
                owner_copy(i, k, p, my_x).start()

            @pl.when(jnp.logical_not(away))
            def _():
                sums_recv[my_x, lax.rem(k, per_owner), r] = both

            return carry

        lax.fori_loop(0, pieces, one, 0)

    if units > 1:

        def take_all(i, carry):
            take_down(i)
            return carry

        lax.fori_loop(0, n, take_all, 0)

    def chunk_step(i, carry):
        @pl.when(i < chunks)
        def _():
            if units == 1:
                take_down(i)
            give_half(i)

        @pl.when((i >= 1) & (i < chunks + 1))
        def _():
            sum_half(i - 1)

        @pl.when(keeps & (i >= 2))
        def _():
            sum_pair(i - 2)

        return carry

    lax.fori_loop(0, chunks + 2, chunk_step, 0)

    def finish(p, carry):
        r = rows_at(p)
        for c in range(per_owner):
            for source in range(nx):

                @pl.when((source != my_x) | jnp.logical_not(keeps))
                def _():
                    owner_copy(0, c, p, source).wait_recv()

            lanes = slice(c * width, (c + 1) * width)
            total = sums_recv[0, c, r].astype(jnp.float32)
            for source in range(1, nx):
                total = total + sums_recv[source, c, r].astype(jnp.float32)
            own = stream[y, t, r, lanes].astype(jnp.float32)
            out_ref[r, lanes] = (own + 0.5 * total).astype(jnp.bfloat16)
        return carry

    lax.fori_loop(0, pieces, finish, 0)

    def end_sums(p, carry):
        for i in range(max(chunks - 2, 0), chunks):
            last = chunk_at(i)
            give_copy(i, last, p).wait_send()

            @pl.when(jnp.logical_not(keeps))
            def _():
                pair_copy(i, last, p).wait_send()

            @pl.when(keeps & (last // per_owner != t))
            def _():
                owner_copy(i, last, p, my_x).wait_send()

        return carry

    lax.fori_loop(0, pieces, end_sums, 0)

    @pl.when(me < n - 1)
    def _():
        rim_copy.wait_send()

    def end_state(to, carry):
        state_copy(to, me).wait_send()
        return carry

    lax.fori_loop(me + 1, jnp.where(y == 0, me + 2, n), end_state, 0)

    def end_shares(b, carry):
        for buf, yy, send, fwd, recv in (
            (mix, 0, m_send, m_fwd, m_recv),
            (stream, y, r_send, r_fwd, r_recv),
        ):
            for d in range(nx):
                share(buf, yy, t, b, me, partner, send.at[d, b], recv).wait_send()
            for d in range(1, nx):
                share(buf, yy, t, b, me, partner, fwd.at[d, b], recv).wait_send()
        for d in range(nx):
            share(stream, y, t, b, me, partner, p_send.at[d, b], p_recv).wait_send()
            share(stream, y, t, b, me, partner, p_fwd.at[d, b], p_recv).wait_send()
        return carry

    lax.fori_loop(0, nb, end_shares, 0)

    def end_weights(s, carry):
        for w in range(3):
            @pl.when((s // 2 >= q) & (q > 0))
            def _():
                along(w, s, False).wait_send()

            @pl.when((s // 2 <= q) & (q < m - 1))
            def _():
                along(w, s, True).wait_send()

        return carry

    lax.fori_loop(0, n, end_weights, 0)
    for w in range(3):
        give_pair(w).wait_send()


def layer(front, later, wg, wu, wd, heads, s1, s2):
    n, tp = lax.axis_size("sp"), lax.axis_size("tp")
    gate, wout, residual = later
    tokens = gate.shape[0]
    half = heads * HEAD
    lanes = 2 * (half + s1 + s2)
    rows8 = -(-2 * heads // 8) * 8
    cols = residual.shape[1]
    nb = tokens // BLOCK
    shard, units = wg.shape
    part = units // 2
    split = part % LANES != 0
    if split:
        wg, wu, wd = (w.reshape(shard, 2, part).swapaxes(0, 1) for w in (wg, wu, wd))
    width = max(shard, min(cols, 2 * LANES))
    chunks = tp * cols // width
    pieces = tokens // (2 * BLOCK)
    vmem = pl.BlockSpec(memory_space=pltpu.VMEM)
    hbm = pl.BlockSpec(memory_space=pl.ANY)
    dma = pltpu.SemaphoreType.DMA
    return pl.pallas_call(
        functools.partial(layer_kernel, n, tp, heads, s1, s2, split),
        out_shape=jax.ShapeDtypeStruct((tokens, cols), jnp.bfloat16),
        in_specs=[vmem] * 7
        + [pl.BlockSpec(memory_space=pltpu.SMEM)]
        + [vmem] * 5
        + [hbm] * 6,
        out_specs=vmem,
        scratch_shapes=[
            pltpu.VMEM(gate.shape, gate.dtype),
            pltpu.VMEM(wout.shape, wout.dtype),
            pltpu.VMEM(residual.shape, residual.dtype),
            dma((3,)),
            pltpu.VMEM((CONV, lanes), jnp.float32),
            pltpu.VMEM((rows8, tokens), jnp.float32),
            pltpu.VMEM((rows8, tokens), jnp.float32),
            pltpu.VMEM((RIM, lanes), jnp.bfloat16),
            pltpu.VMEM((8, lanes), jnp.float32),
            pltpu.VMEM((RIM, lanes), jnp.bfloat16),
            pltpu.VMEM((tokens, 2 * half), jnp.bfloat16),
            pltpu.VMEM((tokens, 2 * (s1 + s2)), jnp.bfloat16),
            pltpu.VMEM((tokens, BLOCK), jnp.float32),
            pltpu.VMEM((s1 + s2, half), jnp.float32),
            pltpu.VMEM((s1 + s2 + RIM, half), jnp.bfloat16),
            pltpu.VMEM((n, s1 + s2 + RIM, half), jnp.bfloat16),
            pltpu.VMEM((1, tp, tokens, 2 * half), jnp.bfloat16),
            pltpu.VMEM((2, tp, tokens, cols), jnp.bfloat16),
            pltpu.VMEM((2, tokens, tp * cols), jnp.bfloat16),
            pltpu.VMEM((3, n * shard, part), jnp.bfloat16),
            pltpu.VMEM((2, tokens, part), jnp.bfloat16),
            pltpu.VMEM((2, tokens, width), jnp.bfloat16),
            pltpu.VMEM((chunks, tokens, width), jnp.bfloat16),
            pltpu.VMEM((2, tokens, width), jnp.bfloat16),
            pltpu.VMEM((chunks, tokens, width), jnp.bfloat16),
            pltpu.VMEM((2, tokens, width), jnp.bfloat16),
            pltpu.VMEM((tp // 2, cols // width, tokens, width), jnp.bfloat16),
            dma((2,)),
            dma((n,)),
            dma((n,)),
            dma((tp, nb)),
            dma((tp, nb)),
            dma((tp, nb)),
            dma((tp, nb)),
            dma((tp, nb)),
            dma((tp, nb)),
            dma((tp, nb)),
            dma((tp, nb)),
            dma((tp, nb)),
            dma((3,)),
            dma((3,)),
            dma((2, 3, n)),
            dma((3, n)),
            dma((2, pieces)),
            dma((chunks, pieces)),
            dma((2, pieces)),
            dma((chunks, pieces)),
            dma((2, pieces)),
            dma((tp // 2, cols // width, pieces)),
        ],
        compiler_params=pltpu.CompilerParams(
            has_side_effects=True, vmem_limit_bytes=VMEM_LIMIT
        ),
        name="layer",
    )(*front, gate, wout, residual, wg, wu, wd)


def shards(
    grouped_head_inputs,
    head_gate_inputs,
    unsmoothed_step,
    head_decay_rate,
    extra_log_decay,
    first_group_keys,
    first_group_queries,
    second_group_keys,
    second_group_queries,
    head_input_filter,
    first_group_filter,
    second_group_filter,
    head_norm_gain,
    output_weight,
    residual,
    channel_norm_gain,
    channel_gate_weight,
    channel_up_weight,
    channel_down_weight,
):
    tokens = grouped_head_inputs.shape[0]
    heads = head_decay_rate.shape[1]
    half = heads * HEAD
    s1, s2 = first_group_keys.shape[1], second_group_keys.shape[1]
    return layer(
        (
            grouped_head_inputs.reshape(tokens, 2 * half),
            first_group_keys,
            first_group_queries,
            second_group_keys.T,
            second_group_queries.T,
            unsmoothed_step.transpose(1, 2, 0),
            extra_log_decay.transpose(1, 2, 0),
            head_decay_rate,
            head_input_filter,
            first_group_filter,
            second_group_filter,
            head_norm_gain,
            channel_norm_gain.reshape(1, -1),
        ),
        (head_gate_inputs.reshape(tokens, 2 * half), output_weight, residual),
        channel_gate_weight,
        channel_up_weight,
        channel_down_weight,
        heads,
        s1,
        s2,
    )


def solution(mesh):
    return jax.shard_map(
        shards,
        mesh=mesh,
        in_specs=(
            P("sp", None, "tp"),
            P("sp", None, "tp"),
            P("sp", None, "tp"),
            P(None, "tp"),
            P("sp", None, "tp"),
            P("sp", None),
            P("sp", None),
            P("sp", None),
            P("sp", None),
            P(None, None, "tp"),
            P(),
            P(),
            P(None, "tp"),
            P(None, None, "tp"),
            P("sp", "tp"),
            P(),
            P("sp", "tp"),
            P("sp", "tp"),
            P("sp", "tp"),
        ),
        out_specs=P("sp", "tp"),
        check_vma=False,
    )
```

```python
import functools

import jax
import jax.numpy as jnp
from jax import lax
from jax.experimental import pallas as pl
from jax.experimental.pallas import tpu as pltpu
from jax.sharding import PartitionSpec as P

HEAD = 64
CONV = 4
BLOCK = 128
RIM = 16
EPSILON = 1e-06
LANES = 128
VMEM_LIMIT = 63 << 20
MESH = pl.DeviceIdType.MESH


def rows_of(b):
    return pl.ds(pl.multiple_of(b * BLOCK, BLOCK), BLOCK)


def spread(columns, first, count):
    parts = [
        jnp.broadcast_to(columns[:, h : h + 1], (columns.shape[0], HEAD))
        for h in range(first, first + count)
    ]
    return jnp.concatenate(parts, axis=1)


def sigmoid(x):
    return 1.0 / (1.0 + jnp.exp(-x))


def layer_kernel(
    n, tp, heads, s1, s2, split,
    x_ref, keys1_ref, queries1_ref, keys2_ref, queries2_ref, unsmoothed_ref, extra_ref, rate_ref,
    head_taps_ref, taps1_ref, taps2_ref, hgain_ref, cgain_ref,
    gate_in, wout_in, res_in, wg_ref, wu_ref, wd_ref,
    out_ref,
    gate_ref, wout_ref, res_ref, in_sems, taps_ref, step_rows, log_rows, rim_out, xs, rim, vals, kq, cums, st, stsend, entering, strecv, mix, stream, normed, weights, hidden,
    give, give_recv, sums, across_recv, ready, sums_recv,
    rim_sems, st_send, st_recv, m_send, m_fwd, m_recv, r_send, r_fwd, r_recv,
    p_send, p_fwd, p_recv, w_local, w_pair, w_send, w_recv,
    g_send, g_recv, a_send, a_recv, s_send, s_recv,
):
    me = lax.axis_index("sp")
    t = lax.axis_index("tp")
    half = heads * HEAD
    wide = 2 * half
    nb = x_ref.shape[0] // BLOCK
    nx = tp // 2
    core = lax.rem(t, 2)
    my_x = t // 2
    partner = my_x * 2 + (1 - core)

    m = n // 2
    q = me // 2
    y = lax.rem(me, 2)
    pair = q * 2 + (1 - y)
    shard = wg_ref.shape[-2]
    tokens = x_ref.shape[0]
    sources = (wg_ref, wu_ref, wd_ref)
    part = weights.shape[2]

    def half_of(w, which):
        if split:
            return sources[w].at[which]
        return sources[w].at[:, pl.ds(pl.multiple_of(which * part, part), part)]

    def unit(w, s):
        return weights.at[w, pl.ds(pl.multiple_of(s * shard, shard), shard)]

    def keep_own(w):
        return pltpu.make_async_copy(half_of(w, y), unit(w, me), w_local.at[w])

    def give_pair(w):
        return pltpu.make_async_remote_copy(
            src_ref=half_of(w, 1 - y),
            dst_ref=unit(w, me),
            send_sem=w_pair.at[w],
            recv_sem=w_recv.at[w, me],
            device_id={"sp": pair},
            device_id_type=MESH,
        )

    def along(w, s, up, own=False):
        return pltpu.make_async_remote_copy(
            src_ref=half_of(w, y) if own else unit(w, s),
            dst_ref=unit(w, s),
            send_sem=w_send.at[int(up), w, s],
            recv_sem=w_recv.at[w, s],
            device_id={"sp": lax.rem(me + 2, n) if up else lax.rem(me + n - 2, n)},
            device_id_type=MESH,
        )

    def send_along(w, s, up, own=False):
        @pl.when(q < m - 1 if up else q > 0)
        def _():
            along(w, s, up, own).start()

    def take_unit(w, s):
        along(w, s, True).wait_recv()

    def start_weights():
        give_pair(0).start()

        @pl.when(y == 1)
        def _():
            give_pair(1).start()

        for w in range(2):
            send_along(w, me, False, own=True)
        send_along(0, me, True, own=True)
        for w in range(3):
            keep_own(w).start()

    def relay_down(k):
        w, d, sel = lax.rem(k, 2), k // 4, lax.rem(k // 2, 2)

        @pl.when(q + d < m)
        def _():
            s = (q + d) * 2 + lax.rem(y + sel, 2)
            take_unit(w, s)
            send_along(w, s, False)

    def relay_up(k):
        w, d, sel = lax.rem(k, 2), k // 4, lax.rem(k // 2, 2)

        @pl.when(q - d >= 0)
        def _():
            s = (q - d) * 2 + lax.rem(y + sel, 2)
            take_unit(w, s)
            send_along(w, s, True)

    early = 4 * (m - 1)
    stride = max(m - 3, 0)

    def relay_points(b, first, go):
        for j, at in enumerate((0, 1, 3, 4)):

            @pl.when(b == first + at)
            def _():
                if m > 2:
                    go(4 + j)

        for j in range(4):

            @pl.when(b == first + nb - 2 + j)
            def _():
                for i in range(stride):
                    go(8 + j * stride + i)

    later = [
        pltpu.make_async_copy(source, place, in_sems.at[i])
        for i, (source, place) in enumerate(
            ((gate_in, gate_ref), (wout_in, wout_ref), (res_in, res_ref))
        )
    ]

    def tokens_of(b):
        r = rows_of(b)
        second = jnp.concatenate([keys2_ref[:, r], queries2_ref[:, r]], axis=0)
        return jnp.concatenate(
            [
                x_ref[r].astype(jnp.float32),
                keys1_ref[r].astype(jnp.float32),
                queries1_ref[r].astype(jnp.float32),
                second.astype(jnp.float32).T,
            ],
            axis=1,
        )

    rim_copy = pltpu.make_async_remote_copy(
        src_ref=rim_out,
        dst_ref=rim,
        send_sem=rim_sems.at[0],
        recv_sem=rim_sems.at[1],
        device_id={"sp": lax.rem(me + 1, n)},
        device_id_type=MESH,
    )

    @pl.when(me < n - 1)
    def _():
        rim_out[...] = tokens_of(nb - 1)[BLOCK - RIM :].astype(jnp.bfloat16)
        rim_copy.start()

    start_weights()

    for copy in later:
        copy.start()

    for g in range(2):
        taps_ref[:, g * half : (g + 1) * half] = head_taps_ref[:, g, :]
        taps_ref[:, wide + g * s1 : wide + (g + 1) * s1] = taps1_ref[:, g, :]
    taps_ref[:, wide + 2 * s1 :] = jnp.concatenate([taps2_ref[:, 0, :], taps2_ref[:, 1, :]], axis=1)

    unsmoothed = unsmoothed_ref[...]
    steps = jnp.maximum(unsmoothed, 0.0) + jnp.log1p(jnp.exp(-jnp.abs(unsmoothed)))
    step_rows[...] = jnp.zeros_like(step_rows)
    log_rows[...] = jnp.zeros_like(log_rows)
    for g in range(2):
        for h in range(heads):
            c = g * heads + h
            row = steps[g, h : h + 1]
            step_rows[c : c + 1] = row
            log_rows[c : c + 1] = extra_ref[g, h : h + 1] - row * rate_ref[g, h]

    @pl.when(me > 0)
    def _():
        rim_copy.wait_recv()
        xs[...] = rim[...].astype(jnp.float32)[RIM - 8 :]

    @pl.when(me == 0)
    def _():
        xs[...] = jnp.zeros_like(xs)

    st[...] = jnp.zeros_like(st)
    row_i = lax.broadcasted_iota(jnp.int32, (BLOCK, BLOCK), 0)
    col_i = lax.broadcasted_iota(jnp.int32, (BLOCK, BLOCK), 1)
    causal = row_i >= col_i
    tri = jnp.where(row_i <= col_i, 1.0, 0.0).astype(jnp.float32)
    rows8 = log_rows.shape[0]

    def state_update(b, cum):
        last = cum[BLOCK - 1 : BLOCK]
        to_end = jnp.exp(last - cum)
        decay = jnp.exp(last)
        r = rows_of(b)
        for g in range(2):
            k0, size = (wide, s1) if g == 0 else (wide + 2 * s1, s2)
            base = 0 if g == 0 else s1
            keys = kq[r, k0 - wide : k0 - wide + size]
            v = vals[r, g * half : (g + 1) * half].astype(jnp.float32)
            v = (v * spread(to_end, g * heads, heads)).astype(jnp.bfloat16)
            add = lax.dot_general(
                keys, v, (((0,), (0,)), ((), ())), preferred_element_type=jnp.float32
            )
            st[base : base + size] = (
                st[base : base + size] * spread(decay, g * heads, heads) + add
            )

    def first_pass(b, total):
        r = rows_of(b)
        current = tokens_of(b)
        taps = taps_ref[...]
        extended = jnp.concatenate([xs[...], current], axis=0)
        acc = taps[CONV - 1 : CONV] * current
        for k in range(CONV - 1):
            acc = acc + taps[k : k + 1] * pltpu.roll(extended, CONV - 1 - k, 0)[8:]
        xs[...] = current[BLOCK - 8 :]
        acc = acc * sigmoid(acc)
        cum_rows = jnp.dot(
            log_rows[:, r], tri, precision=lax.Precision.HIGHEST, preferred_element_type=jnp.float32
        )
        fill = jnp.zeros((BLOCK - 2 * rows8, BLOCK), jnp.float32)
        cum = jnp.concatenate([cum_rows, step_rows[:, r], fill], axis=0).T
        cums[r] = cum
        vals[r] = (acc[:, :wide] * spread(cum, rows8, 2 * heads)).astype(jnp.bfloat16)
        kq[r] = acc[:, wide:].astype(jnp.bfloat16)
        state_update(b, cum)

        return total + cum[BLOCK - 1 : BLOCK]

    total = lax.fori_loop(0, nb, first_pass, jnp.zeros((1, BLOCK), jnp.float32))

    states = s1 + s2

    def pack_state(total):
        stsend[0:states] = st[...].astype(jnp.bfloat16)
        which = lax.broadcasted_iota(jnp.int32, (RIM, half), 0)
        extra = jnp.zeros((RIM, half), jnp.float32)
        for g in range(2):
            logs = total[g]
            high = logs.astype(jnp.bfloat16).astype(jnp.float32)
            low = logs - high
            extra = jnp.where(which == g, high, extra)
            extra = jnp.where(which == 2 + g, low, extra)
        stsend[states : states + RIM] = extra.astype(jnp.bfloat16)

    def logs_of(got):
        return [
            got[states + g : states + g + 1] + got[states + 2 + g : states + 3 + g]
            for g in range(2)
        ]

    def state_copy(to, source, packed):
        return pltpu.make_async_remote_copy(
            src_ref=packed,
            dst_ref=strecv.at[source, pl.ds(0, packed.shape[0])],
            send_sem=st_send.at[to],
            recv_sem=st_recv.at[source],
            device_id={"sp": to},
            device_id_type=MESH,
        )

    def send_state(i, carry):
        state_copy(n - 1 - 2 * i, me, stsend).start()
        return carry

    own_logs = [spread(total, g * heads, heads) for g in range(2)]

    @pl.when(y == 0)
    def _():
        pack_state(own_logs)
        state_copy(pair, me, stsend).start()
        give_pair(1).start()
        give_pair(2).start()

    @pl.when(y == 1)
    def _():
        state_copy(me, pair, stsend).wait_recv()
        got = strecv[pair].astype(jnp.float32)
        for g in range(2):
            base, size = (0, s1) if g == 0 else (s1, s2)
            st[base : base + size] = (
                st[base : base + size] + got[base : base + size] * jnp.exp(own_logs[g])
            )
        both = [a + b for a, b in zip(logs_of(got), own_logs)]
        pack_state(both)
        lax.fori_loop(0, m - 1 - q, send_state, 0)

    def relay_pair(w):
        take_unit(w, pair)
        send_along(w, pair, False)
        send_along(w, pair, True)

    send_along(1, me, True, own=True)
    relay_pair(0)

    @pl.when(y == 0)
    def _():
        relay_pair(1)

    st[...] = jnp.zeros_like(st)

    def add_state(source):
        got = strecv[source].astype(jnp.float32)
        logs = logs_of(got)
        for g in range(2):
            base, size = (0, s1) if g == 0 else (s1, s2)
            st[base : base + size] = (
                st[base : base + size] * jnp.exp(logs[g]) + got[base : base + size]
            )

    def take_state(before, carry):
        source = before * 2 + 1
        state_copy(n - 1, source, stsend).wait_recv()
        add_state(source)
        return carry

    @pl.when(y == 1)
    def _():
        lax.fori_loop(0, q, take_state, 0)

        @pl.when(q > 0)
        def _():
            entering[...] = st[...].astype(jnp.bfloat16)
            state_copy(pair, me, entering).start()

        give_pair(2).start()
        add_state(pair)
        relay_pair(1)

    @pl.when((y == 0) & (q > 0))
    def _():
        state_copy(me, pair, entering).wait_recv()
        st[...] = strecv[pair, 0:states].astype(jnp.float32)

    def share(buf, yy, source, b, sp, to, send, recv):
        piece = buf.at[yy, source, rows_of(b)]
        return pltpu.make_async_remote_copy(
            src_ref=piece,
            dst_ref=piece,
            send_sem=send,
            recv_sem=recv.at[source, b],
            device_id={"sp": sp, "tp": to},
            device_id_type=MESH,
        )

    def across(d):
        return lax.rem(my_x + d, nx) * 2

    def send_own(buf, yy, b, send, recv):
        for d in range(1, nx):
            to = across(d) + core
            share(buf, yy, t, b, me, to, send.at[d, b], recv).start()
        share(buf, yy, t, b, me, partner, send.at[0, b], recv).start()

    def forward(buf, yy, b, fwd, recv):
        for d in range(1, nx):
            source = across(d) + core
            move = share(buf, yy, source, b, me, partner, fwd.at[d, b], recv)
            move.wait_recv()
            move.start()

    def wait_rest(buf, yy, b, send, recv):
        share(buf, yy, partner, b, me, partner, send.at[0, b], recv).wait_recv()
        for d in range(1, nx):
            source = across(d) + (1 - core)
            share(buf, yy, source, b, me, partner, send.at[0, b], recv).wait_recv()

    def send_pair(b):
        share(stream, y, t, b, pair, t, p_send.at[0, b], p_recv).start()

    def forward_pair(b):
        for d in range(nx):
            source = across(d) + core
            move = share(stream, 1 - y, source, b, me, partner, p_fwd.at[d, b], p_recv)
            move.wait_recv()
            move.start()

    def wait_pair(b):
        for d in range(nx):
            source = across(d) + (1 - core)
            share(stream, 1 - y, source, b, me, partner, p_fwd.at[d, b], p_recv).wait_recv()

    def second_pass(b):
        r = rows_of(b)
        cum = cums[r]
        cum_t = cum.T
        grown = jnp.exp(cum)
        for g in range(2):
            off, size = (0, s1) if g == 0 else (2 * s1, s2)
            base = 0 if g == 0 else s1
            keys = kq[r, off : off + size]
            queries = kq[r, off + size : off + 2 * size]
            scores = lax.dot_general(
                queries, keys, (((1,), (1,)), ((), ())), preferred_element_type=jnp.float32
            )
            carried = jnp.dot(
                queries,
                st[base : base + size].astype(jnp.bfloat16),
                preferred_element_type=jnp.float32,
            )
            carried = carried * spread(grown, g * heads, heads)
            v = vals[r, g * half : (g + 1) * half]
            outs = []
            for h in range(heads):
                c = g * heads + h
                span = jnp.where(causal, cum[:, c : c + 1] - cum_t[c : c + 1, :], -jnp.inf)
                w = (jnp.exp(span) * scores).astype(jnp.bfloat16)
                lanes = slice(h * HEAD, (h + 1) * HEAD)
                y = jnp.dot(w, v[:, lanes], preferred_element_type=jnp.float32)
                y = y + carried[:, lanes]
                z = gate_ref[r, g * half + h * HEAD : g * half + (h + 1) * HEAD].astype(jnp.float32)
                y = y * (z * sigmoid(z))
                y = y * lax.rsqrt(jnp.mean(y * y, axis=1, keepdims=True) + EPSILON)
                outs.append(y)
            out = jnp.concatenate(outs, axis=1) * hgain_ref[g : g + 1]
            mix[0, t, r, g * half : (g + 1) * half] = out.astype(jnp.bfloat16)
        state_update(b, cum)
        send_own(mix, 0, b, m_send, m_recv)

    def project(b):
        r = rows_of(b)
        wait_rest(mix, 0, b, m_send, m_recv)
        acc = res_ref[r].astype(jnp.float32)
        for source in range(tp):
            for g in range(2):
                acc = acc + jnp.dot(
                    mix[0, source, r, g * half : (g + 1) * half],
                    wout_ref[g, source * half : (source + 1) * half],
                    preferred_element_type=jnp.float32,
                )
        stream[y, t, r] = acc.astype(jnp.bfloat16)
        send_own(stream, y, b, r_send, r_recv)
        send_pair(b)

    cols = res_ref.shape[1]

    def normalise(yy, b):
        r = rows_of(b)
        parts = [stream[yy, source, r].astype(jnp.float32) for source in range(tp)]
        square = sum(jnp.sum(p * p, axis=1, keepdims=True) for p in parts)
        scale = lax.rsqrt(square / (tp * cols) + EPSILON)
        for source in range(tp):
            lanes = slice(source * cols, (source + 1) * cols)
            normed[yy, r, lanes] = (parts[source] * scale * cgain_ref[:, lanes]).astype(
                jnp.bfloat16
            )

    down = 2

    def stage(b, carry):
        @pl.when(b < nb)
        def _():
            second_pass(b)

        relay_points(b, 0, relay_down)
        relay_points(b, 1, relay_up)

        @pl.when((b >= 1) & (b < nb + 1))
        def _():
            forward(mix, 0, b - 1, m_fwd, m_recv)

        @pl.when((b >= 2) & (b < nb + 2))
        def _():
            project(b - 2)

        @pl.when(b == nb + 3)
        def _():
            send_along(down, me, False, own=True)
            send_along(down, me, True, own=True)

        @pl.when((b >= 3) & (b < nb + 3))
        def _():
            forward(stream, y, b - 3, r_fwd, r_recv)
            for d in range(1, nx):
                source = across(d) + core
                share(stream, y, source, b - 3, pair, t, p_send.at[d, b - 3], p_recv).start()

        @pl.when((b >= 4) & (b < nb + 4))
        def _():
            wait_rest(stream, y, b - 4, r_send, r_recv)
            normalise(y, b - 4)

        @pl.when((b >= 6) & (b < nb + 6))
        def _():
            forward_pair(b - 6)

        @pl.when(b >= 7)
        def _():
            wait_pair(b - 7)
            normalise(1 - y, b - 7)

        return carry

    for copy in later:
        copy.wait()
    lax.fori_loop(0, nb + 7, stage, 0)

    between = (q > 0) & (q < m - 1)

    def relay_far(d):
        for sel in range(2):

            @pl.when(between & (q + d < m))
            def _():
                s = (q + d) * 2 + sel
                take_unit(down, s)
                send_along(down, s, False)

            @pl.when(between & (q - d >= 0))
            def _():
                s = (q - d) * 2 + sel
                take_unit(down, s)
                send_along(down, s, True)

    keep_own(down).wait()
    take_unit(down, pair)
    send_along(down, pair, False)
    send_along(down, pair, True)
    relay_far(1)

    def late(k, carry):
        relay_down(k)
        relay_up(k)
        return carry

    lax.fori_loop(max(early, 4), 4 * m, late, 0)
    for w in range(2):
        keep_own(w).wait()

    tall = 2 * BLOCK
    pieces = tokens // tall

    def pass_on(d, carry):
        relay_far(d)
        return carry

    near = jnp.minimum(q, m - 1 - q)

    def block_at(i):
        d = (i + 1) // 2
        side = jnp.where(lax.rem(i, 2) == 1, q + d, q - d)
        beyond = jnp.where(q < m - 1 - q, i, m - 1 - i)
        return jnp.where(i <= 2 * near, side, beyond)

    width = sums.shape[2]
    units = width // shard
    chunks = tp * cols // width
    per_owner = cols // width

    def shard_at(i):
        return block_at(i // 2) * 2 + lax.rem(i, 2)

    def take_down(i):
        @pl.when((i >= 2) & jnp.logical_not(between))
        def _():
            take_unit(down, shard_at(i))

    def chunk_at(i):
        return shard_at(i) if units == 1 else i

    def product(yy, k, p):
        r = pl.ds(pl.multiple_of(p * tall, tall), tall)
        block = weights[down, pl.ds(pl.multiple_of(k * width, width), width)]
        return lax.dot_general(
            hidden[yy, r], block, (((1,), (1,)), ((), ())), preferred_element_type=jnp.float32
        )

    def rows_at(p):
        return pl.ds(pl.multiple_of(p * tall, tall), tall)

    def give_copy(i, k, p):
        return pltpu.make_async_remote_copy(
            src_ref=give.at[lax.rem(i, 2), rows_at(p)],
            dst_ref=give_recv.at[k, rows_at(p)],
            send_sem=g_send.at[lax.rem(i, 2), p],
            recv_sem=g_recv.at[k, p],
            device_id={"tp": partner},
            device_id_type=MESH,
        )

    def pair_copy(i, k, p):
        return pltpu.make_async_remote_copy(
            src_ref=sums.at[lax.rem(i, 2), rows_at(p)],
            dst_ref=across_recv.at[k, rows_at(p)],
            send_sem=a_send.at[lax.rem(i, 2), p],
            recv_sem=a_recv.at[k, p],
            device_id={"sp": pair},
            device_id_type=MESH,
        )

    def owner_copy(i, k, p, source):
        return pltpu.make_async_remote_copy(
            src_ref=ready.at[lax.rem(i, 2), rows_at(p)],
            dst_ref=sums_recv.at[source, lax.rem(k, per_owner), rows_at(p)],
            send_sem=s_send.at[lax.rem(i, 2), p],
            recv_sem=s_recv.at[source, lax.rem(k, per_owner), p],
            device_id={"tp": k // per_owner},
            device_id_type=MESH,
        )

    keeps = core == y

    def give_piece(i, p):
        k = chunk_at(i)

        @pl.when(i >= 2)
        def _():
            give_copy(i, k, p).wait_send()

        give[lax.rem(i, 2), rows_at(p)] = product(1 - core, k, p).astype(jnp.bfloat16)
        give_copy(i, k, p).start()

    def sum_piece(i, p):
        k = chunk_at(i)

        @pl.when(jnp.logical_not(keeps) & (i >= 2))
        def _():
            pair_copy(i, k, p).wait_send()

        give_copy(i, k, p).wait_recv()
        both = product(core, k, p) + give_recv[k, rows_at(p)].astype(jnp.float32)
        sums[lax.rem(i, 2), rows_at(p)] = both.astype(jnp.bfloat16)

        @pl.when(jnp.logical_not(keeps))
        def _():
            pair_copy(i, k, p).start()

    def give_half(i):
        def one(p, carry):
            give_piece(i, p)
            return carry

        lax.fori_loop(0, pieces, one, 0)

    def sum_half(i):
        def one(p, carry):
            sum_piece(i, p)
            return carry

        lax.fori_loop(0, pieces, one, 0)

    def sum_pair(i):
        k = chunk_at(i)
        away = k // per_owner != t
        before = chunk_at(jnp.maximum(i - 2, 0))

        def one(p, carry):
            @pl.when((i >= 2) & (before // per_owner != t))
            def _():
                owner_copy(i, before, p, my_x).wait_send()

            pair_copy(i, k, p).wait_recv()
            r = rows_at(p)
            both = sums[lax.rem(i, 2), r].astype(jnp.float32) + across_recv[k, r].astype(
                jnp.float32
            )
            both = both.astype(jnp.bfloat16)

            @pl.when(away)
            def _():
                ready[lax.rem(i, 2), r] = both
                owner_copy(i, k, p, my_x).start()

            @pl.when(jnp.logical_not(away))
            def _():
                sums_recv[my_x, lax.rem(k, per_owner), r] = both

            return carry

        lax.fori_loop(0, pieces, one, 0)

    def take_all(i, carry):
        take_down(i)
        return carry

    def first_part(i):
        @pl.when(keeps)
        def _():
            give_half(i)

        @pl.when(jnp.logical_not(keeps))
        def _():
            sum_half(i)

    def second_part(i):
        @pl.when(keeps)
        def _():
            sum_half(i)

        @pl.when(jnp.logical_not(keeps))
        def _():
            give_half(i)

    if units > 1:
        lax.fori_loop(2, m, pass_on, 0)
        lax.fori_loop(0, n, take_all, 0)

    def mix_channels(yy, p):
        rows = normed[yy, rows_at(p)]
        g = jnp.dot(rows, weights[0], preferred_element_type=jnp.float32)
        u = jnp.dot(rows, weights[1], preferred_element_type=jnp.float32)
        hidden[yy, rows_at(p)] = (g * sigmoid(g) * u).astype(jnp.bfloat16)

    ahead = min(2, chunks)

    def mix_step(j, carry):
        p = lax.rem(j, pieces)
        theirs = j < pieces
        mix_channels(jnp.where(theirs, 1 - y, y), p)

        @pl.when(theirs & keeps)
        def _():
            give_piece(0, p)

        @pl.when(theirs & jnp.logical_not(keeps))
        def _():
            sum_piece(0, p)

        @pl.when(j == pieces - 1)
        def _():
            if ahead > 1:
                first_part(1)

        return carry

    lax.fori_loop(0, 2 * pieces, mix_step, 0)
    if units == 1:
        lax.fori_loop(2, m, pass_on, 0)

    def chunk_step(i, carry):
        @pl.when((i >= ahead) & (i < chunks))
        def _():
            if units == 1:
                take_down(i)
            first_part(i)

        @pl.when(i < chunks)
        def _():
            second_part(i)

        @pl.when(keeps & (i >= 1))
        def _():
            sum_pair(i - 1)

        return carry

    lax.fori_loop(0, chunks + 1, chunk_step, 0)

    def finish(p, carry):
        r = rows_at(p)
        for c in range(per_owner):
            for source in range(nx):

                @pl.when((source != my_x) | jnp.logical_not(keeps))
                def _():
                    owner_copy(0, c, p, source).wait_recv()

            lanes = slice(c * width, (c + 1) * width)
            total = sums_recv[0, c, r].astype(jnp.float32)
            for source in range(1, nx):
                total = total + sums_recv[source, c, r].astype(jnp.float32)
            own = stream[y, t, r, lanes].astype(jnp.float32)
            out_ref[r, lanes] = (own + 0.5 * total).astype(jnp.bfloat16)
        return carry

    lax.fori_loop(0, pieces, finish, 0)

    def end_sums(p, carry):
        for i in range(max(chunks - 2, 0), chunks):
            last = chunk_at(i)
            give_copy(i, last, p).wait_send()

            @pl.when(jnp.logical_not(keeps))
            def _():
                pair_copy(i, last, p).wait_send()

            @pl.when(keeps & (last // per_owner != t))
            def _():
                owner_copy(i, last, p, my_x).wait_send()

        return carry

    lax.fori_loop(0, pieces, end_sums, 0)

    @pl.when(me < n - 1)
    def _():
        rim_copy.wait_send()

    def end_state(i, carry):
        state_copy(n - 1 - 2 * i, me, stsend).wait_send()
        return carry

    @pl.when(y == 0)
    def _():
        state_copy(pair, me, stsend).wait_send()

    @pl.when(y == 1)
    def _():
        lax.fori_loop(0, m - 1 - q, end_state, 0)

        @pl.when(q > 0)
        def _():
            state_copy(pair, me, entering).wait_send()

    def end_shares(b, carry):
        for buf, yy, send, fwd, recv in (
            (mix, 0, m_send, m_fwd, m_recv),
            (stream, y, r_send, r_fwd, r_recv),
        ):
            for d in range(nx):
                share(buf, yy, t, b, me, partner, send.at[d, b], recv).wait_send()
            for d in range(1, nx):
                share(buf, yy, t, b, me, partner, fwd.at[d, b], recv).wait_send()
        for d in range(nx):
            share(stream, y, t, b, me, partner, p_send.at[d, b], p_recv).wait_send()
            share(stream, y, t, b, me, partner, p_fwd.at[d, b], p_recv).wait_send()
        return carry

    lax.fori_loop(0, nb, end_shares, 0)

    def end_weights(s, carry):
        for w in range(3):
            @pl.when((s // 2 >= q) & (q > 0))
            def _():
                along(w, s, False).wait_send()

            @pl.when((s // 2 <= q) & (q < m - 1))
            def _():
                along(w, s, True).wait_send()

        return carry

    lax.fori_loop(0, n, end_weights, 0)
    for w in range(3):
        give_pair(w).wait_send()


def layer(front, later, wg, wu, wd, heads, s1, s2):
    n, tp = lax.axis_size("sp"), lax.axis_size("tp")
    gate, wout, residual = later
    tokens = gate.shape[0]
    half = heads * HEAD
    lanes = 2 * (half + s1 + s2)
    rows8 = -(-2 * heads // 8) * 8
    cols = residual.shape[1]
    nb = tokens // BLOCK
    shard, units = wg.shape
    part = units // 2
    split = part % LANES != 0
    if split:
        wg, wu, wd = (w.reshape(shard, 2, part).swapaxes(0, 1) for w in (wg, wu, wd))
    width = max(shard, min(cols, 2 * LANES))
    chunks = tp * cols // width
    pieces = tokens // (2 * BLOCK)
    vmem = pl.BlockSpec(memory_space=pltpu.VMEM)
    hbm = pl.BlockSpec(memory_space=pl.ANY)
    dma = pltpu.SemaphoreType.DMA
    return pl.pallas_call(
        functools.partial(layer_kernel, n, tp, heads, s1, s2, split),
        out_shape=jax.ShapeDtypeStruct((tokens, cols), jnp.bfloat16),
        in_specs=[vmem] * 7
        + [pl.BlockSpec(memory_space=pltpu.SMEM)]
        + [vmem] * 5
        + [hbm] * 6,
        out_specs=vmem,
        scratch_shapes=[
            pltpu.VMEM(gate.shape, gate.dtype),
            pltpu.VMEM(wout.shape, wout.dtype),
            pltpu.VMEM(residual.shape, residual.dtype),
            dma((3,)),
            pltpu.VMEM((CONV, lanes), jnp.float32),
            pltpu.VMEM((rows8, tokens), jnp.float32),
            pltpu.VMEM((rows8, tokens), jnp.float32),
            pltpu.VMEM((RIM, lanes), jnp.bfloat16),
            pltpu.VMEM((8, lanes), jnp.float32),
            pltpu.VMEM((RIM, lanes), jnp.bfloat16),
            pltpu.VMEM((tokens, 2 * half), jnp.bfloat16),
            pltpu.VMEM((tokens, 2 * (s1 + s2)), jnp.bfloat16),
            pltpu.VMEM((tokens, BLOCK), jnp.float32),
            pltpu.VMEM((s1 + s2, half), jnp.float32),
            pltpu.VMEM((s1 + s2 + RIM, half), jnp.bfloat16),
            pltpu.VMEM((s1 + s2, half), jnp.bfloat16),
            pltpu.VMEM((n, s1 + s2 + RIM, half), jnp.bfloat16),
            pltpu.VMEM((1, tp, tokens, 2 * half), jnp.bfloat16),
            pltpu.VMEM((2, tp, tokens, cols), jnp.bfloat16),
            pltpu.VMEM((2, tokens, tp * cols), jnp.bfloat16),
            pltpu.VMEM((3, n * shard, part), jnp.bfloat16),
            pltpu.VMEM((2, tokens, part), jnp.bfloat16),
            pltpu.VMEM((2, tokens, width), jnp.bfloat16),
            pltpu.VMEM((chunks, tokens, width), jnp.bfloat16),
            pltpu.VMEM((2, tokens, width), jnp.bfloat16),
            pltpu.VMEM((chunks, tokens, width), jnp.bfloat16),
            pltpu.VMEM((2, tokens, width), jnp.bfloat16),
            pltpu.VMEM((tp // 2, cols // width, tokens, width), jnp.bfloat16),
            dma((2,)),
            dma((n,)),
            dma((n,)),
            dma((tp, nb)),
            dma((tp, nb)),
            dma((tp, nb)),
            dma((tp, nb)),
            dma((tp, nb)),
            dma((tp, nb)),
            dma((tp, nb)),
            dma((tp, nb)),
            dma((tp, nb)),
            dma((3,)),
            dma((3,)),
            dma((2, 3, n)),
            dma((3, n)),
            dma((2, pieces)),
            dma((chunks, pieces)),
            dma((2, pieces)),
            dma((chunks, pieces)),
            dma((2, pieces)),
            dma((tp // 2, cols // width, pieces)),
        ],
        compiler_params=pltpu.CompilerParams(
            has_side_effects=True, vmem_limit_bytes=VMEM_LIMIT
        ),
        name="layer",
    )(*front, gate, wout, residual, wg, wu, wd)


def shards(
    grouped_head_inputs,
    head_gate_inputs,
    unsmoothed_step,
    head_decay_rate,
    extra_log_decay,
    first_group_keys,
    first_group_queries,
    second_group_keys,
    second_group_queries,
    head_input_filter,
    first_group_filter,
    second_group_filter,
    head_norm_gain,
    output_weight,
    residual,
    channel_norm_gain,
    channel_gate_weight,
    channel_up_weight,
    channel_down_weight,
):
    tokens = grouped_head_inputs.shape[0]
    heads = head_decay_rate.shape[1]
    half = heads * HEAD
    s1, s2 = first_group_keys.shape[1], second_group_keys.shape[1]
    return layer(
        (
            grouped_head_inputs.reshape(tokens, 2 * half),
            first_group_keys,
            first_group_queries,
            second_group_keys.T,
            second_group_queries.T,
            unsmoothed_step.transpose(1, 2, 0),
            extra_log_decay.transpose(1, 2, 0),
            head_decay_rate,
            head_input_filter,
            first_group_filter,
            second_group_filter,
            head_norm_gain,
            channel_norm_gain.reshape(1, -1),
        ),
        (head_gate_inputs.reshape(tokens, 2 * half), output_weight, residual),
        channel_gate_weight,
        channel_up_weight,
        channel_down_weight,
        heads,
        s1,
        s2,
    )


def solution(mesh):
    return jax.shard_map(
        shards,
        mesh=mesh,
        in_specs=(
            P("sp", None, "tp"),
            P("sp", None, "tp"),
            P("sp", None, "tp"),
            P(None, "tp"),
            P("sp", None, "tp"),
            P("sp", None),
            P("sp", None),
            P("sp", None),
            P("sp", None),
            P(None, None, "tp"),
            P(),
            P(),
            P(None, "tp"),
            P(None, None, "tp"),
            P("sp", "tp"),
            P(),
            P("sp", "tp"),
            P("sp", "tp"),
            P("sp", "tp"),
        ),
        out_specs=P("sp", "tp"),
        check_vma=False,
    )
```

```python
import functools

import jax
import jax.numpy as jnp
from jax import lax
from jax.experimental import pallas as pl
from jax.experimental.pallas import tpu as pltpu
from jax.sharding import PartitionSpec as P

HEAD = 64
CONV = 4
BLOCK = 128
RIM = 16
EPSILON = 1e-06
LANES = 128
SLOTS = 4
VMEM_LIMIT = 63 << 20
MESH = pl.DeviceIdType.MESH


def rows_of(b):
    return pl.ds(pl.multiple_of(b * BLOCK, BLOCK), BLOCK)


def spread(columns, first, count):
    parts = [
        jnp.broadcast_to(columns[:, h : h + 1], (columns.shape[0], HEAD))
        for h in range(first, first + count)
    ]
    return jnp.concatenate(parts, axis=1)


def sigmoid(x):
    return 1.0 / (1.0 + jnp.exp(-x))


def layer_kernel(
    n, tp, heads, s1, s2, split,
    x_ref, keys1_ref, queries1_ref, keys2_ref, queries2_ref, unsmoothed_ref, extra_ref, rate_ref,
    head_taps_ref, taps1_ref, taps2_ref, hgain_ref, cgain_ref,
    gate_in, wout_in, res_in, wg_ref, wu_ref, wd_ref,
    out_ref,
    gate_ref, wout_ref, res_ref, in_sems, taps_ref, step_rows, log_rows, rim_out, xs, rim, vals, kq, cums, st, stsend, entering, strecv, mix, stream, normed, weights, hidden,
    give, give_recv, sums, across_recv, ready, sums_recv,
    rim_sems, st_send, st_recv, m_send, m_fwd, m_recv, r_send, r_fwd, r_recv,
    p_send, p_fwd, p_recv, w_local, w_pair, w_send, w_recv,
    g_send, g_recv, a_send, a_recv, s_send, s_recv,
):
    me = lax.axis_index("sp")
    t = lax.axis_index("tp")
    half = heads * HEAD
    wide = 2 * half
    nb = x_ref.shape[0] // BLOCK
    nx = tp // 2
    core = lax.rem(t, 2)
    my_x = t // 2
    partner = my_x * 2 + (1 - core)

    m = n // 2
    q = me // 2
    y = lax.rem(me, 2)
    pair = q * 2 + (1 - y)
    shard = wg_ref.shape[-2]
    tokens = x_ref.shape[0]
    sources = (wg_ref, wu_ref, wd_ref)
    part = weights.shape[2]

    def half_of(w, which):
        if split:
            return sources[w].at[which]
        return sources[w].at[:, pl.ds(pl.multiple_of(which * part, part), part)]

    def unit(w, s):
        return weights.at[w, pl.ds(pl.multiple_of(s * shard, shard), shard)]

    def keep_own(w):
        return pltpu.make_async_copy(half_of(w, y), unit(w, me), w_local.at[w])

    def give_pair(w):
        return pltpu.make_async_remote_copy(
            src_ref=half_of(w, 1 - y),
            dst_ref=unit(w, me),
            send_sem=w_pair.at[w],
            recv_sem=w_recv.at[w, me],
            device_id={"sp": pair},
            device_id_type=MESH,
        )

    def along(w, s, up, own=False):
        return pltpu.make_async_remote_copy(
            src_ref=half_of(w, y) if own else unit(w, s),
            dst_ref=unit(w, s),
            send_sem=w_send.at[int(up), w, s],
            recv_sem=w_recv.at[w, s],
            device_id={"sp": lax.rem(me + 2, n) if up else lax.rem(me + n - 2, n)},
            device_id_type=MESH,
        )

    def send_along(w, s, up, own=False):
        @pl.when(q < m - 1 if up else q > 0)
        def _():
            along(w, s, up, own).start()

    def take_unit(w, s):
        along(w, s, True).wait_recv()

    def start_weights():
        give_pair(0).start()

        @pl.when(y == 1)
        def _():
            give_pair(1).start()

        for w in range(2):
            send_along(w, me, False, own=True)
            send_along(w, me, True, own=True)
        for w in range(3):
            keep_own(w).start()

    def relay_down(k):
        w, d, sel = lax.rem(k, 2), k // 4, lax.rem(k // 2, 2)

        @pl.when(q + d < m)
        def _():
            s = (q + d) * 2 + lax.rem(y + sel, 2)
            take_unit(w, s)
            send_along(w, s, False)

    def relay_up(k):
        w, d, sel = lax.rem(k, 2), k // 4, lax.rem(k // 2, 2)

        @pl.when(q - d >= 0)
        def _():
            s = (q - d) * 2 + lax.rem(y + sel, 2)
            take_unit(w, s)
            send_along(w, s, True)

    early = 4 * (m - 1)
    stride = max(m - 3, 0)

    def relay_points(b):
        for j, at in ((6, 1), (7, 3)):

            @pl.when(b == at)
            def _():
                if m > 2:
                    relay_down(j)
                    relay_up(j)

        for j in range(4):

            @pl.when(b == nb - 3 + j)
            def _():
                for i in range(stride):
                    relay_down(8 + j * stride + i)
                    relay_up(8 + j * stride + i)

    later = [
        pltpu.make_async_copy(source, place, in_sems.at[i])
        for i, (source, place) in enumerate(
            ((gate_in, gate_ref), (wout_in, wout_ref), (res_in, res_ref))
        )
    ]

    def tokens_of(b):
        r = rows_of(b)
        second = jnp.concatenate([keys2_ref[:, r], queries2_ref[:, r]], axis=0)
        return jnp.concatenate(
            [
                x_ref[r].astype(jnp.float32),
                keys1_ref[r].astype(jnp.float32),
                queries1_ref[r].astype(jnp.float32),
                second.astype(jnp.float32).T,
            ],
            axis=1,
        )

    rim_copy = pltpu.make_async_remote_copy(
        src_ref=rim_out,
        dst_ref=rim,
        send_sem=rim_sems.at[0],
        recv_sem=rim_sems.at[1],
        device_id={"sp": lax.rem(me + 1, n)},
        device_id_type=MESH,
    )

    @pl.when(me < n - 1)
    def _():
        rim_out[...] = tokens_of(nb - 1)[BLOCK - RIM :].astype(jnp.bfloat16)
        rim_copy.start()

    start_weights()

    for copy in later:
        copy.start()

    for g in range(2):
        taps_ref[:, g * half : (g + 1) * half] = head_taps_ref[:, g, :]
        taps_ref[:, wide + g * s1 : wide + (g + 1) * s1] = taps1_ref[:, g, :]
    taps_ref[:, wide + 2 * s1 :] = jnp.concatenate([taps2_ref[:, 0, :], taps2_ref[:, 1, :]], axis=1)

    unsmoothed = unsmoothed_ref[...]
    steps = jnp.maximum(unsmoothed, 0.0) + jnp.log1p(jnp.exp(-jnp.abs(unsmoothed)))
    step_rows[...] = jnp.zeros_like(step_rows)
    log_rows[...] = jnp.zeros_like(log_rows)
    for g in range(2):
        for h in range(heads):
            c = g * heads + h
            row = steps[g, h : h + 1]
            step_rows[c : c + 1] = row
            log_rows[c : c + 1] = extra_ref[g, h : h + 1] - row * rate_ref[g, h]

    @pl.when(me > 0)
    def _():
        rim_copy.wait_recv()
        xs[...] = rim[...].astype(jnp.float32)[RIM - 8 :]

    @pl.when(me == 0)
    def _():
        xs[...] = jnp.zeros_like(xs)

    st[...] = jnp.zeros_like(st)
    row_i = lax.broadcasted_iota(jnp.int32, (BLOCK, BLOCK), 0)
    col_i = lax.broadcasted_iota(jnp.int32, (BLOCK, BLOCK), 1)
    causal = row_i >= col_i
    tri = jnp.where(row_i <= col_i, 1.0, 0.0).astype(jnp.float32)
    rows8 = log_rows.shape[0]

    def state_update(b, cum):
        last = cum[BLOCK - 1 : BLOCK]
        to_end = jnp.exp(last - cum)
        decay = jnp.exp(last)
        r = rows_of(b)
        for g in range(2):
            k0, size = (wide, s1) if g == 0 else (wide + 2 * s1, s2)
            base = 0 if g == 0 else s1
            keys = kq[r, k0 - wide : k0 - wide + size]
            v = vals[r, g * half : (g + 1) * half].astype(jnp.float32)
            v = (v * spread(to_end, g * heads, heads)).astype(jnp.bfloat16)
            add = lax.dot_general(
                keys, v, (((0,), (0,)), ((), ())), preferred_element_type=jnp.float32
            )
            st[base : base + size] = (
                st[base : base + size] * spread(decay, g * heads, heads) + add
            )

    def first_pass(b, total):
        r = rows_of(b)
        current = tokens_of(b)
        taps = taps_ref[...]
        extended = jnp.concatenate([xs[...], current], axis=0)
        acc = taps[CONV - 1 : CONV] * current
        for k in range(CONV - 1):
            acc = acc + taps[k : k + 1] * pltpu.roll(extended, CONV - 1 - k, 0)[8:]
        xs[...] = current[BLOCK - 8 :]
        acc = acc * sigmoid(acc)
        cum_rows = jnp.dot(
            log_rows[:, r], tri, precision=lax.Precision.HIGHEST, preferred_element_type=jnp.float32
        )
        fill = jnp.zeros((BLOCK - 2 * rows8, BLOCK), jnp.float32)
        cum = jnp.concatenate([cum_rows, step_rows[:, r], fill], axis=0).T
        cums[r] = cum
        vals[r] = (acc[:, :wide] * spread(cum, rows8, 2 * heads)).astype(jnp.bfloat16)
        kq[r] = acc[:, wide:].astype(jnp.bfloat16)
        state_update(b, cum)

        return total + cum[BLOCK - 1 : BLOCK]

    total = lax.fori_loop(0, nb, first_pass, jnp.zeros((1, BLOCK), jnp.float32))

    states = s1 + s2

    def pack_state(total):
        stsend[0:states] = st[...].astype(jnp.bfloat16)
        which = lax.broadcasted_iota(jnp.int32, (RIM, half), 0)
        extra = jnp.zeros((RIM, half), jnp.float32)
        for g in range(2):
            logs = total[g]
            high = logs.astype(jnp.bfloat16).astype(jnp.float32)
            low = logs - high
            extra = jnp.where(which == g, high, extra)
            extra = jnp.where(which == 2 + g, low, extra)
        stsend[states : states + RIM] = extra.astype(jnp.bfloat16)

    def logs_of(got):
        return [
            got[states + g : states + g + 1] + got[states + 2 + g : states + 3 + g]
            for g in range(2)
        ]

    def state_copy(to, source, packed):
        return pltpu.make_async_remote_copy(
            src_ref=packed,
            dst_ref=strecv.at[source, pl.ds(0, packed.shape[0])],
            send_sem=st_send.at[to],
            recv_sem=st_recv.at[source],
            device_id={"sp": to},
            device_id_type=MESH,
        )

    def send_state(i, carry):
        state_copy(n - 1 - 2 * i, me, stsend).start()
        return carry

    own_logs = [spread(total, g * heads, heads) for g in range(2)]

    @pl.when(y == 0)
    def _():
        pack_state(own_logs)
        state_copy(pair, me, stsend).start()
        give_pair(1).start()
        give_pair(2).start()

    @pl.when(y == 1)
    def _():
        state_copy(me, pair, stsend).wait_recv()
        got = strecv[pair].astype(jnp.float32)
        for g in range(2):
            base, size = (0, s1) if g == 0 else (s1, s2)
            st[base : base + size] = (
                st[base : base + size] + got[base : base + size] * jnp.exp(own_logs[g])
            )
        both = [a + b for a, b in zip(logs_of(got), own_logs)]
        pack_state(both)
        lax.fori_loop(0, m - 1 - q, send_state, 0)

    def relay_pair(w):
        take_unit(w, pair)
        send_along(w, pair, False)
        send_along(w, pair, True)

    relay_pair(0)

    @pl.when(y == 0)
    def _():
        relay_pair(1)

    st[...] = jnp.zeros_like(st)

    def add_state(source):
        got = strecv[source].astype(jnp.float32)
        logs = logs_of(got)
        for g in range(2):
            base, size = (0, s1) if g == 0 else (s1, s2)
            st[base : base + size] = (
                st[base : base + size] * jnp.exp(logs[g]) + got[base : base + size]
            )

    def take_state(before, carry):
        source = before * 2 + 1
        state_copy(n - 1, source, stsend).wait_recv()
        add_state(source)
        return carry

    @pl.when(y == 1)
    def _():
        lax.fori_loop(0, q, take_state, 0)

        @pl.when(q > 0)
        def _():
            entering[...] = st[...].astype(jnp.bfloat16)
            state_copy(pair, me, entering).start()

        give_pair(2).start()
        add_state(pair)
        relay_pair(1)

    @pl.when((y == 0) & (q > 0))
    def _():
        state_copy(me, pair, entering).wait_recv()
        st[...] = strecv[pair, 0:states].astype(jnp.float32)

    def share(buf, yy, source, b, sp, to, send, recv):
        piece = buf.at[yy, source, rows_of(b)]
        return pltpu.make_async_remote_copy(
            src_ref=piece,
            dst_ref=piece,
            send_sem=send,
            recv_sem=recv.at[source, b],
            device_id={"sp": sp, "tp": to},
            device_id_type=MESH,
        )

    def across(d):
        return lax.rem(my_x + d, nx) * 2

    def send_own(buf, yy, b, send, recv):
        for d in range(1, nx):
            to = across(d) + core
            share(buf, yy, t, b, me, to, send.at[d, b], recv).start()
        share(buf, yy, t, b, me, partner, send.at[0, b], recv).start()

    def forward(buf, yy, b, fwd, recv):
        for d in range(1, nx):
            source = across(d) + core
            move = share(buf, yy, source, b, me, partner, fwd.at[d, b], recv)
            move.wait_recv()
            move.start()

    def wait_rest(buf, yy, b, send, recv):
        share(buf, yy, partner, b, me, partner, send.at[0, b], recv).wait_recv()
        for d in range(1, nx):
            source = across(d) + (1 - core)
            share(buf, yy, source, b, me, partner, send.at[0, b], recv).wait_recv()

    def send_pair(b):
        share(stream, y, t, b, pair, t, p_send.at[0, b], p_recv).start()

    def forward_pair(b):
        for d in range(nx):
            source = across(d) + core
            move = share(stream, 1 - y, source, b, me, partner, p_fwd.at[d, b], p_recv)
            move.wait_recv()
            move.start()

    def wait_pair(b):
        for d in range(nx):
            source = across(d) + (1 - core)
            share(stream, 1 - y, source, b, me, partner, p_fwd.at[d, b], p_recv).wait_recv()

    def second_pass(b):
        r = rows_of(b)
        cum = cums[r]
        cum_t = cum.T
        grown = jnp.exp(cum)
        for g in range(2):
            off, size = (0, s1) if g == 0 else (2 * s1, s2)
            base = 0 if g == 0 else s1
            keys = kq[r, off : off + size]
            queries = kq[r, off + size : off + 2 * size]
            scores = lax.dot_general(
                queries, keys, (((1,), (1,)), ((), ())), preferred_element_type=jnp.float32
            )
            carried = jnp.dot(
                queries,
                st[base : base + size].astype(jnp.bfloat16),
                preferred_element_type=jnp.float32,
            )
            carried = carried * spread(grown, g * heads, heads)
            v = vals[r, g * half : (g + 1) * half]
            outs = []
            for h in range(heads):
                c = g * heads + h
                span = jnp.where(causal, cum[:, c : c + 1] - cum_t[c : c + 1, :], -jnp.inf)
                w = (jnp.exp(span) * scores).astype(jnp.bfloat16)
                lanes = slice(h * HEAD, (h + 1) * HEAD)
                y = jnp.dot(w, v[:, lanes], preferred_element_type=jnp.float32)
                y = y + carried[:, lanes]
                z = gate_ref[r, g * half + h * HEAD : g * half + (h + 1) * HEAD].astype(jnp.float32)
                y = y * (z * sigmoid(z))
                y = y * lax.rsqrt(jnp.mean(y * y, axis=1, keepdims=True) + EPSILON)
                outs.append(y)
            out = jnp.concatenate(outs, axis=1) * hgain_ref[g : g + 1]
            mix[0, t, r, g * half : (g + 1) * half] = out.astype(jnp.bfloat16)
        state_update(b, cum)
        send_own(mix, 0, b, m_send, m_recv)

    def project(b):
        r = rows_of(b)
        wait_rest(mix, 0, b, m_send, m_recv)
        acc = res_ref[r].astype(jnp.float32)
        for source in range(tp):
            for g in range(2):
                acc = acc + jnp.dot(
                    mix[0, source, r, g * half : (g + 1) * half],
                    wout_ref[g, source * half : (source + 1) * half],
                    preferred_element_type=jnp.float32,
                )
        stream[y, t, r] = acc.astype(jnp.bfloat16)
        send_own(stream, y, b, r_send, r_recv)
        send_pair(b)

    cols = res_ref.shape[1]

    def normalise(yy, b):
        r = rows_of(b)
        parts = [stream[yy, source, r].astype(jnp.float32) for source in range(tp)]
        square = sum(jnp.sum(p * p, axis=1, keepdims=True) for p in parts)
        scale = lax.rsqrt(square / (tp * cols) + EPSILON)
        for source in range(tp):
            lanes = slice(source * cols, (source + 1) * cols)
            normed[yy, r, lanes] = (parts[source] * scale * cgain_ref[:, lanes]).astype(
                jnp.bfloat16
            )

    down = 2

    def stage(b, carry):
        @pl.when(b < nb)
        def _():
            second_pass(b)

        relay_points(b)

        @pl.when((b >= 1) & (b < nb + 1))
        def _():
            forward(mix, 0, b - 1, m_fwd, m_recv)

        @pl.when((b >= 2) & (b < nb + 2))
        def _():
            project(b - 2)

        for turn in range(2):

            @pl.when((b == nb + 1 + turn) & (y == turn))
            def _():
                send_along(down, me, False, own=True)
                send_along(down, me, True, own=True)

            @pl.when((b == nb + 1 + turn) & (y != turn))
            def _():
                relay_pair(down)

        @pl.when((b >= 3) & (b < nb + 3))
        def _():
            forward(stream, y, b - 3, r_fwd, r_recv)
            for d in range(1, nx):
                source = across(d) + core
                share(stream, y, source, b - 3, pair, t, p_send.at[d, b - 3], p_recv).start()

        @pl.when((b >= 4) & (b < nb + 4))
        def _():
            wait_rest(stream, y, b - 4, r_send, r_recv)
            normalise(y, b - 4)

        @pl.when((b >= 6) & (b < nb + 6))
        def _():
            forward_pair(b - 6)

        @pl.when(b >= 7)
        def _():
            wait_pair(b - 7)
            normalise(1 - y, b - 7)

        return carry

    for copy in later:
        copy.wait()
    if m > 2:
        for k in (4, 5):
            relay_down(k)
            relay_up(k)
    lax.fori_loop(0, nb + 7, stage, 0)

    units = sums.shape[2] // shard
    between = (q > 0) & (q < m - 1)

    def relay_far(d):
        for sel in range(2):

            @pl.when(between & (q + d < m))
            def _():
                s = (q + d) * 2 + sel
                take_unit(down, s)
                send_along(down, s, False)

            @pl.when(between & (q - d >= 0))
            def _():
                s = (q - d) * 2 + sel
                take_unit(down, s)
                send_along(down, s, True)

    keep_own(down).wait()
    if units > 1:
        relay_far(1)

    def late(k, carry):
        relay_down(k)
        relay_up(k)
        return carry

    lax.fori_loop(max(early, 4), 4 * m, late, 0)
    for w in range(2):
        keep_own(w).wait()

    tall = 2 * BLOCK
    pieces = tokens // tall

    def pass_on(d, carry):
        relay_far(d)
        return carry

    near = jnp.minimum(q, m - 1 - q)

    def block_at(i):
        d = (i + 1) // 2
        side = jnp.where(lax.rem(i, 2) == 1, q + d, q - d)
        beyond = jnp.where(q < m - 1 - q, i, m - 1 - i)
        return jnp.where(i <= 2 * near, side, beyond)

    width = sums.shape[2]
    chunks = tp * cols // width
    per_owner = cols // width

    def shard_at(i):
        return block_at(i // 2) * 2 + lax.rem(i, 2)

    def take_down(i):
        @pl.when((i >= 2) & jnp.logical_not(between))
        def _():
            take_unit(down, shard_at(i))

    def chunk_at(i):
        return shard_at(i) if units == 1 else i

    def product(yy, k, p, count):
        r = pl.ds(pl.multiple_of(p * tall, tall), count * tall)
        block = weights[down, pl.ds(pl.multiple_of(k * width, width), width)]
        return lax.dot_general(
            hidden[yy, r], block, (((1,), (1,)), ((), ())), preferred_element_type=jnp.float32
        )

    def rows_at(p):
        return pl.ds(pl.multiple_of(p * tall, tall), tall)

    def give_copy(i, k, p):
        return pltpu.make_async_remote_copy(
            src_ref=give.at[lax.rem(i, 2), rows_at(p)],
            dst_ref=give_recv.at[k, rows_at(p)],
            send_sem=g_send.at[lax.rem(i, 2), p],
            recv_sem=g_recv.at[k, p],
            device_id={"tp": partner},
            device_id_type=MESH,
        )

    def pair_copy(i, k, p):
        return pltpu.make_async_remote_copy(
            src_ref=sums.at[lax.rem(i, slots), rows_at(p)],
            dst_ref=across_recv.at[k, rows_at(p)],
            send_sem=a_send.at[lax.rem(i, slots), p],
            recv_sem=a_recv.at[k, p],
            device_id={"sp": pair},
            device_id_type=MESH,
        )

    def owner_copy(i, k, p, source):
        return pltpu.make_async_remote_copy(
            src_ref=ready.at[lax.rem(i, slots), rows_at(p)],
            dst_ref=sums_recv.at[source, lax.rem(k, per_owner), rows_at(p)],
            send_sem=s_send.at[lax.rem(i, slots), p],
            recv_sem=s_recv.at[source, lax.rem(k, per_owner), p],
            device_id={"tp": k // per_owner},
            device_id_type=MESH,
        )

    keeps = core == y
    slots = sums.shape[0]

    def give_piece(i, p, count=1):
        k = chunk_at(i)
        for c in range(count):

            @pl.when(i >= 2)
            def _():
                give_copy(i, k, p + c).wait_send()

        r = pl.ds(pl.multiple_of(p * tall, tall), count * tall)
        give[lax.rem(i, 2), r] = product(1 - core, k, p, count).astype(jnp.bfloat16)
        for c in range(count):
            give_copy(i, k, p + c).start()

    def sum_piece(i, p, count=1):
        k = chunk_at(i)
        for c in range(count):

            @pl.when(jnp.logical_not(keeps) & (i >= slots))
            def _():
                pair_copy(i, k, p + c).wait_send()

            give_copy(i, k, p + c).wait_recv()
        r = pl.ds(pl.multiple_of(p * tall, tall), count * tall)
        both = product(core, k, p, count) + give_recv[k, r].astype(jnp.float32)
        sums[lax.rem(i, slots), r] = both.astype(jnp.bfloat16)

        @pl.when(jnp.logical_not(keeps))
        def _():
            for c in range(count):
                pair_copy(i, k, p + c).start()

    many = 2 if pieces % 2 == 0 else 1

    def give_half(i):
        def one(p, carry):
            give_piece(i, p * many, many)
            return carry

        lax.fori_loop(0, pieces // many, one, 0)

    def sum_half(i):
        def one(p, carry):
            sum_piece(i, p * many, many)
            return carry

        lax.fori_loop(0, pieces // many, one, 0)

    def sum_pair(i):
        k = chunk_at(i)
        away = k // per_owner != t
        before = chunk_at(jnp.maximum(i - slots, 0))

        def one(p, carry):
            @pl.when((i >= slots) & (before // per_owner != t))
            def _():
                owner_copy(i, before, p, my_x).wait_send()

            pair_copy(i, k, p).wait_recv()
            r = rows_at(p)
            both = sums[lax.rem(i, slots), r].astype(jnp.float32) + across_recv[k, r].astype(
                jnp.float32
            )
            both = both.astype(jnp.bfloat16)

            @pl.when(away)
            def _():
                ready[lax.rem(i, slots), r] = both
                owner_copy(i, k, p, my_x).start()

            @pl.when(jnp.logical_not(away))
            def _():
                sums_recv[my_x, lax.rem(k, per_owner), r] = both

            return carry

        lax.fori_loop(0, pieces, one, 0)

    def take_all(i, carry):
        take_down(i)
        return carry

    if units > 1:
        lax.fori_loop(2, m, pass_on, 0)
        lax.fori_loop(0, n, take_all, 0)

    def mix_channels(yy, p):
        rows = normed[yy, rows_at(p)]
        g = jnp.dot(rows, weights[0], preferred_element_type=jnp.float32)
        u = jnp.dot(rows, weights[1], preferred_element_type=jnp.float32)
        hidden[yy, rows_at(p)] = (g * sigmoid(g) * u).astype(jnp.bfloat16)

    ahead = min(2, chunks)

    def pair_half(i):
        if units == 1:
            take_down(i)

        @pl.when(keeps)
        def _():
            give_half(i)

        @pl.when(jnp.logical_not(keeps))
        def _():
            sum_half(i)

    def mix_step(j, carry):
        p = lax.rem(j, pieces)
        theirs = j < pieces
        mix_channels(jnp.where(theirs, 1 - y, y), p)

        @pl.when(theirs & keeps)
        def _():
            for i in range(ahead):
                give_piece(i, p)

        @pl.when(theirs & jnp.logical_not(keeps))
        def _():
            for i in range(ahead):
                sum_piece(i, p)

        @pl.when(j == pieces - 1)
        def _():
            if units == 1:
                relay_far(1)
            if chunks > ahead:
                pair_half(ahead)

        @pl.when(j == 2 * pieces - 2)
        def _():
            if chunks > ahead + 1:
                pair_half(ahead + 1)

        return carry

    lax.fori_loop(0, 2 * pieces, mix_step, 0)

    middle = chunks // 2

    def chunk_step(i, carry):
        early = (i >= 1) & (i < middle - 1)
        late_on = (i > middle) & (i < chunks - 1)
        far = jnp.where(i < middle, i + 3, i + 1)

        if units == 1:

            @pl.when(i == min(2, chunks - 1))
            def _():
                lax.fori_loop(2, m, pass_on, 0)

        @pl.when(jnp.logical_not(keeps))
        def _():
            give_half(i)

        if units == 1:

            @pl.when(early)
            def _():
                take_down(far)

        @pl.when(keeps & early)
        def _():
            give_half(far)

        @pl.when(keeps)
        def _():
            sum_half(i)

            @pl.when(i >= 1)
            def _():
                sum_pair(i - 1)

        if units == 1:

            @pl.when(late_on)
            def _():
                take_down(far)

        @pl.when(keeps & late_on)
        def _():
            give_half(far)

        @pl.when(jnp.logical_not(keeps) & (early | late_on))
        def _():
            sum_half(far)

        return carry

    lax.fori_loop(0, chunks, chunk_step, 0)

    @pl.when(keeps)
    def _():
        sum_pair(chunks - 1)

    def finish(p, carry):
        r = rows_at(p)
        for c in range(per_owner):
            for source in range(nx):

                @pl.when((source != my_x) | jnp.logical_not(keeps))
                def _():
                    owner_copy(0, c, p, source).wait_recv()

            lanes = slice(c * width, (c + 1) * width)
            total = sums_recv[0, c, r].astype(jnp.float32)
            for source in range(1, nx):
                total = total + sums_recv[source, c, r].astype(jnp.float32)
            own = stream[y, t, r, lanes].astype(jnp.float32)
            out_ref[r, lanes] = (own + 0.5 * total).astype(jnp.bfloat16)
        return carry

    lax.fori_loop(0, pieces, finish, 0)

    def end_sums(p, carry):
        for i in range(max(chunks - 2, 0), chunks):
            give_copy(i, chunk_at(i), p).wait_send()
        for i in range(max(chunks - slots, 0), chunks):
            last = chunk_at(i)

            @pl.when(jnp.logical_not(keeps))
            def _():
                pair_copy(i, last, p).wait_send()

            @pl.when(keeps & (last // per_owner != t))
            def _():
                owner_copy(i, last, p, my_x).wait_send()

        return carry

    lax.fori_loop(0, pieces, end_sums, 0)

    @pl.when(me < n - 1)
    def _():
        rim_copy.wait_send()

    def end_state(i, carry):
        state_copy(n - 1 - 2 * i, me, stsend).wait_send()
        return carry

    @pl.when(y == 0)
    def _():
        state_copy(pair, me, stsend).wait_send()

    @pl.when(y == 1)
    def _():
        lax.fori_loop(0, m - 1 - q, end_state, 0)

        @pl.when(q > 0)
        def _():
            state_copy(pair, me, entering).wait_send()

    def end_shares(b, carry):
        for buf, yy, send, fwd, recv in (
            (mix, 0, m_send, m_fwd, m_recv),
            (stream, y, r_send, r_fwd, r_recv),
        ):
            for d in range(nx):
                share(buf, yy, t, b, me, partner, send.at[d, b], recv).wait_send()
            for d in range(1, nx):
                share(buf, yy, t, b, me, partner, fwd.at[d, b], recv).wait_send()
        for d in range(nx):
            share(stream, y, t, b, me, partner, p_send.at[d, b], p_recv).wait_send()
            share(stream, y, t, b, me, partner, p_fwd.at[d, b], p_recv).wait_send()
        return carry

    lax.fori_loop(0, nb, end_shares, 0)

    def end_weights(s, carry):
        for w in range(3):
            @pl.when((s // 2 >= q) & (q > 0))
            def _():
                along(w, s, False).wait_send()

            @pl.when((s // 2 <= q) & (q < m - 1))
            def _():
                along(w, s, True).wait_send()

        return carry

    lax.fori_loop(0, n, end_weights, 0)
    for w in range(3):
        give_pair(w).wait_send()


def layer(front, later, wg, wu, wd, heads, s1, s2):
    n, tp = lax.axis_size("sp"), lax.axis_size("tp")
    gate, wout, residual = later
    tokens = gate.shape[0]
    half = heads * HEAD
    lanes = 2 * (half + s1 + s2)
    rows8 = -(-2 * heads // 8) * 8
    cols = residual.shape[1]
    nb = tokens // BLOCK
    shard, units = wg.shape
    part = units // 2
    split = part % LANES != 0
    if split:
        wg, wu, wd = (w.reshape(shard, 2, part).swapaxes(0, 1) for w in (wg, wu, wd))
    width = max(shard, min(cols, 2 * LANES))
    chunks = tp * cols // width
    pieces = tokens // (2 * BLOCK)
    vmem = pl.BlockSpec(memory_space=pltpu.VMEM)
    hbm = pl.BlockSpec(memory_space=pl.ANY)
    dma = pltpu.SemaphoreType.DMA
    return pl.pallas_call(
        functools.partial(layer_kernel, n, tp, heads, s1, s2, split),
        out_shape=jax.ShapeDtypeStruct((tokens, cols), jnp.bfloat16),
        in_specs=[vmem] * 7
        + [pl.BlockSpec(memory_space=pltpu.SMEM)]
        + [vmem] * 5
        + [hbm] * 6,
        out_specs=vmem,
        scratch_shapes=[
            pltpu.VMEM(gate.shape, gate.dtype),
            pltpu.VMEM(wout.shape, wout.dtype),
            pltpu.VMEM(residual.shape, residual.dtype),
            dma((3,)),
            pltpu.VMEM((CONV, lanes), jnp.float32),
            pltpu.VMEM((rows8, tokens), jnp.float32),
            pltpu.VMEM((rows8, tokens), jnp.float32),
            pltpu.VMEM((RIM, lanes), jnp.bfloat16),
            pltpu.VMEM((8, lanes), jnp.float32),
            pltpu.VMEM((RIM, lanes), jnp.bfloat16),
            pltpu.VMEM((tokens, 2 * half), jnp.bfloat16),
            pltpu.VMEM((tokens, 2 * (s1 + s2)), jnp.bfloat16),
            pltpu.VMEM((tokens, BLOCK), jnp.float32),
            pltpu.VMEM((s1 + s2, half), jnp.float32),
            pltpu.VMEM((s1 + s2 + RIM, half), jnp.bfloat16),
            pltpu.VMEM((s1 + s2, half), jnp.bfloat16),
            pltpu.VMEM((n, s1 + s2 + RIM, half), jnp.bfloat16),
            pltpu.VMEM((1, tp, tokens, 2 * half), jnp.bfloat16),
            pltpu.VMEM((2, tp, tokens, cols), jnp.bfloat16),
            pltpu.VMEM((2, tokens, tp * cols), jnp.bfloat16),
            pltpu.VMEM((3, n * shard, part), jnp.bfloat16),
            pltpu.VMEM((2, tokens, part), jnp.bfloat16),
            pltpu.VMEM((2, tokens, width), jnp.bfloat16),
            pltpu.VMEM((chunks, tokens, width), jnp.bfloat16),
            pltpu.VMEM((SLOTS, tokens, width), jnp.bfloat16),
            pltpu.VMEM((chunks, tokens, width), jnp.bfloat16),
            pltpu.VMEM((SLOTS, tokens, width), jnp.bfloat16),
            pltpu.VMEM((tp // 2, cols // width, tokens, width), jnp.bfloat16),
            dma((2,)),
            dma((n,)),
            dma((n,)),
            dma((tp // 2, nb)),
            dma((tp // 2, nb)),
            dma((tp, nb)),
            dma((tp // 2, nb)),
            dma((tp // 2, nb)),
            dma((tp, nb)),
            dma((tp // 2, nb)),
            dma((tp // 2, nb)),
            dma((tp, nb)),
            dma((3,)),
            dma((3,)),
            dma((2, 3, n)),
            dma((3, n)),
            dma((2, pieces)),
            dma((chunks, pieces)),
            dma((SLOTS, pieces)),
            dma((chunks, pieces)),
            dma((SLOTS, pieces)),
            dma((tp // 2, cols // width, pieces)),
        ],
        compiler_params=pltpu.CompilerParams(
            has_side_effects=True, vmem_limit_bytes=VMEM_LIMIT
        ),
        name="layer",
    )(*front, gate, wout, residual, wg, wu, wd)


def shards(
    grouped_head_inputs,
    head_gate_inputs,
    unsmoothed_step,
    head_decay_rate,
    extra_log_decay,
    first_group_keys,
    first_group_queries,
    second_group_keys,
    second_group_queries,
    head_input_filter,
    first_group_filter,
    second_group_filter,
    head_norm_gain,
    output_weight,
    residual,
    channel_norm_gain,
    channel_gate_weight,
    channel_up_weight,
    channel_down_weight,
):
    tokens = grouped_head_inputs.shape[0]
    heads = head_decay_rate.shape[1]
    half = heads * HEAD
    s1, s2 = first_group_keys.shape[1], second_group_keys.shape[1]
    return layer(
        (
            grouped_head_inputs.reshape(tokens, 2 * half),
            first_group_keys,
            first_group_queries,
            second_group_keys.T,
            second_group_queries.T,
            unsmoothed_step.transpose(1, 2, 0),
            extra_log_decay.transpose(1, 2, 0),
            head_decay_rate,
            head_input_filter,
            first_group_filter,
            second_group_filter,
            head_norm_gain,
            channel_norm_gain.reshape(1, -1),
        ),
        (head_gate_inputs.reshape(tokens, 2 * half), output_weight, residual),
        channel_gate_weight,
        channel_up_weight,
        channel_down_weight,
        heads,
        s1,
        s2,
    )


def solution(mesh):
    return jax.shard_map(
        shards,
        mesh=mesh,
        in_specs=(
            P("sp", None, "tp"),
            P("sp", None, "tp"),
            P("sp", None, "tp"),
            P(None, "tp"),
            P("sp", None, "tp"),
            P("sp", None),
            P("sp", None),
            P("sp", None),
            P("sp", None),
            P(None, None, "tp"),
            P(),
            P(),
            P(None, "tp"),
            P(None, None, "tp"),
            P("sp", "tp"),
            P(),
            P("sp", "tp"),
            P("sp", "tp"),
            P("sp", "tp"),
        ),
        out_specs=P("sp", "tp"),
        check_vma=False,
    )
```

```python
import functools

import jax
import jax.numpy as jnp
from jax import lax
from jax.experimental import pallas as pl
from jax.experimental.pallas import tpu as pltpu
from jax.sharding import PartitionSpec as P

HEAD = 64
CONV = 4
BLOCK = 128
RIM = 16
EPSILON = 1e-06
LANES = 128
SLOTS = 4
VMEM_LIMIT = 63 << 20
MESH = pl.DeviceIdType.MESH


def rows_of(b):
    return pl.ds(pl.multiple_of(b * BLOCK, BLOCK), BLOCK)


def spread(columns, first, count):
    parts = [
        jnp.broadcast_to(columns[:, h : h + 1], (columns.shape[0], HEAD))
        for h in range(first, first + count)
    ]
    return jnp.concatenate(parts, axis=1)


def sigmoid(x):
    return 1.0 / (1.0 + jnp.exp(-x))


def layer_kernel(
    n, tp, heads, s1, s2, split,
    x_ref, keys1_ref, queries1_ref, keys2_ref, queries2_ref, unsmoothed_ref, extra_ref, rate_ref,
    head_taps_ref, taps1_ref, taps2_ref, hgain_ref, cgain_ref,
    gate_in, wout_in, res_in, wg_ref, wu_ref, wd_ref,
    out_ref,
    gate_ref, wout_ref, res_ref, in_sems, taps_ref, step_rows, log_rows, rim_out, xs, rim, vals, kq, cums, st, stsend, entering, strecv, mix, stream, normed, weights, hidden,
    give, give_recv, sums, across_recv, ready, sums_recv,
    rim_sems, st_send, st_recv, m_send, m_fwd, m_recv, r_send, r_fwd, r_recv,
    p_send, p_fwd, p_recv, w_local, w_pair, w_send, w_recv,
    g_send, g_recv, a_send, a_recv, s_send, s_recv,
):
    me = lax.axis_index("sp")
    t = lax.axis_index("tp")
    half = heads * HEAD
    wide = 2 * half
    nb = x_ref.shape[0] // BLOCK
    nx = tp // 2
    core = lax.rem(t, 2)
    my_x = t // 2
    partner = my_x * 2 + (1 - core)

    m = n // 2
    q = me // 2
    y = lax.rem(me, 2)
    pair = q * 2 + (1 - y)
    shard = wg_ref.shape[-2]
    tokens = x_ref.shape[0]
    sources = (wg_ref, wu_ref, wd_ref)
    part = weights.shape[2]

    def half_of(w, which):
        if split:
            return sources[w].at[which]
        return sources[w].at[:, pl.ds(pl.multiple_of(which * part, part), part)]

    def unit(w, s):
        return weights.at[w, pl.ds(pl.multiple_of(s * shard, shard), shard)]

    def keep_own(w):
        return pltpu.make_async_copy(half_of(w, y), unit(w, me), w_local.at[w])

    def give_pair(w):
        return pltpu.make_async_remote_copy(
            src_ref=half_of(w, 1 - y),
            dst_ref=unit(w, me),
            send_sem=w_pair.at[w],
            recv_sem=w_recv.at[w, me],
            device_id={"sp": pair},
            device_id_type=MESH,
        )

    def along(w, s, up, own=False):
        return pltpu.make_async_remote_copy(
            src_ref=half_of(w, y) if own else unit(w, s),
            dst_ref=unit(w, s),
            send_sem=w_send.at[int(up), w, s],
            recv_sem=w_recv.at[w, s],
            device_id={"sp": lax.rem(me + 2, n) if up else lax.rem(me + n - 2, n)},
            device_id_type=MESH,
        )

    def send_along(w, s, up, own=False):
        @pl.when(q < m - 1 if up else q > 0)
        def _():
            along(w, s, up, own).start()

    def take_unit(w, s):
        along(w, s, True).wait_recv()

    def start_weights():
        give_pair(0).start()

        @pl.when(y == 1)
        def _():
            give_pair(1).start()

        for w in range(2):
            send_along(w, me, False, own=True)
            send_along(w, me, True, own=True)
        for w in range(3):
            keep_own(w).start()

    def relay_down(k):
        w, d, sel = lax.rem(k, 2), k // 4, lax.rem(k // 2, 2)

        @pl.when(q + d < m)
        def _():
            s = (q + d) * 2 + lax.rem(y + sel, 2)
            take_unit(w, s)
            send_along(w, s, False)

    def relay_up(k):
        w, d, sel = lax.rem(k, 2), k // 4, lax.rem(k // 2, 2)

        @pl.when(q - d >= 0)
        def _():
            s = (q - d) * 2 + lax.rem(y + sel, 2)
            take_unit(w, s)
            send_along(w, s, True)

    early = 4 * (m - 1)
    stride = max(m - 3, 0)

    def relay_points(b):
        for j, at in ((6, 1), (7, 3)):

            @pl.when(b == at)
            def _():
                if m > 2:
                    relay_down(j)
                    relay_up(j)

        for j in range(4):

            @pl.when(b == nb - 3 + j)
            def _():
                for i in range(stride):
                    relay_down(8 + j * stride + i)
                    relay_up(8 + j * stride + i)

    later = [
        pltpu.make_async_copy(source, place, in_sems.at[i])
        for i, (source, place) in enumerate(
            ((gate_in, gate_ref), (wout_in, wout_ref), (res_in, res_ref))
        )
    ]

    def tokens_of(b):
        r = rows_of(b)
        second = jnp.concatenate([keys2_ref[:, r], queries2_ref[:, r]], axis=0)
        heads_in = x_ref[r].astype(jnp.float32)
        return jnp.concatenate(
            [
                heads_in[:, 0, :],
                heads_in[:, 1, :],
                keys1_ref[r].astype(jnp.float32),
                queries1_ref[r].astype(jnp.float32),
                second.astype(jnp.float32).T,
            ],
            axis=1,
        )

    rim_copy = pltpu.make_async_remote_copy(
        src_ref=rim_out,
        dst_ref=rim,
        send_sem=rim_sems.at[0],
        recv_sem=rim_sems.at[1],
        device_id={"sp": lax.rem(me + 1, n)},
        device_id_type=MESH,
    )

    @pl.when(me < n - 1)
    def _():
        rim_out[...] = tokens_of(nb - 1)[BLOCK - RIM :].astype(jnp.bfloat16)
        rim_copy.start()

    start_weights()

    for copy in later:
        copy.start()

    for g in range(2):
        taps_ref[:, g * half : (g + 1) * half] = head_taps_ref[:, g, :]
        taps_ref[:, wide + g * s1 : wide + (g + 1) * s1] = taps1_ref[:, g, :]
    taps_ref[:, wide + 2 * s1 :] = jnp.concatenate([taps2_ref[:, 0, :], taps2_ref[:, 1, :]], axis=1)

    unsmoothed = unsmoothed_ref[...]
    steps = jnp.maximum(unsmoothed, 0.0) + jnp.log1p(jnp.exp(-jnp.abs(unsmoothed)))
    step_rows[...] = jnp.zeros_like(step_rows)
    log_rows[...] = jnp.zeros_like(log_rows)
    for g in range(2):
        for h in range(heads):
            c = g * heads + h
            row = steps[g, h : h + 1]
            step_rows[c : c + 1] = row
            log_rows[c : c + 1] = extra_ref[g, h : h + 1] - row * rate_ref[g, h]

    @pl.when(me > 0)
    def _():
        rim_copy.wait_recv()
        xs[...] = rim[...].astype(jnp.float32)[RIM - 8 :]

    @pl.when(me == 0)
    def _():
        xs[...] = jnp.zeros_like(xs)

    st[...] = jnp.zeros_like(st)
    row_i = lax.broadcasted_iota(jnp.int32, (BLOCK, BLOCK), 0)
    col_i = lax.broadcasted_iota(jnp.int32, (BLOCK, BLOCK), 1)
    causal = row_i >= col_i
    tri = jnp.where(row_i <= col_i, 1.0, 0.0).astype(jnp.float32)
    rows8 = log_rows.shape[0]

    def state_update(b, cum):
        last = cum[BLOCK - 1 : BLOCK]
        to_end = jnp.exp(last - cum)
        decay = jnp.exp(last)
        r = rows_of(b)
        for g in range(2):
            k0, size = (wide, s1) if g == 0 else (wide + 2 * s1, s2)
            base = 0 if g == 0 else s1
            keys = kq[r, k0 - wide : k0 - wide + size]
            v = vals[r, g * half : (g + 1) * half].astype(jnp.float32)
            v = (v * spread(to_end, g * heads, heads)).astype(jnp.bfloat16)
            add = lax.dot_general(
                keys, v, (((0,), (0,)), ((), ())), preferred_element_type=jnp.float32
            )
            st[base : base + size] = (
                st[base : base + size] * spread(decay, g * heads, heads) + add
            )

    def first_pass(b, total):
        r = rows_of(b)
        current = tokens_of(b)
        taps = taps_ref[...]
        extended = jnp.concatenate([xs[...], current], axis=0)
        acc = taps[CONV - 1 : CONV] * current
        for k in range(CONV - 1):
            acc = acc + taps[k : k + 1] * pltpu.roll(extended, CONV - 1 - k, 0)[8:]
        xs[...] = current[BLOCK - 8 :]
        acc = acc * sigmoid(acc)
        cum_rows = jnp.dot(
            log_rows[:, r], tri, precision=lax.Precision.HIGHEST, preferred_element_type=jnp.float32
        )
        fill = jnp.zeros((BLOCK - 2 * rows8, BLOCK), jnp.float32)
        cum = jnp.concatenate([cum_rows, step_rows[:, r], fill], axis=0).T
        cums[r] = cum
        vals[r] = (acc[:, :wide] * spread(cum, rows8, 2 * heads)).astype(jnp.bfloat16)
        kq[r] = acc[:, wide:].astype(jnp.bfloat16)
        state_update(b, cum)

        return total + cum[BLOCK - 1 : BLOCK]

    total = lax.fori_loop(0, nb, first_pass, jnp.zeros((1, BLOCK), jnp.float32))

    states = s1 + s2

    def pack_state(total):
        stsend[0:states] = st[...].astype(jnp.bfloat16)
        which = lax.broadcasted_iota(jnp.int32, (RIM, half), 0)
        extra = jnp.zeros((RIM, half), jnp.float32)
        for g in range(2):
            logs = total[g]
            high = logs.astype(jnp.bfloat16).astype(jnp.float32)
            low = logs - high
            extra = jnp.where(which == g, high, extra)
            extra = jnp.where(which == 2 + g, low, extra)
        stsend[states : states + RIM] = extra.astype(jnp.bfloat16)

    def logs_of(got):
        return [
            got[states + g : states + g + 1] + got[states + 2 + g : states + 3 + g]
            for g in range(2)
        ]

    def state_copy(to, source, packed):
        return pltpu.make_async_remote_copy(
            src_ref=packed,
            dst_ref=strecv.at[source, pl.ds(0, packed.shape[0])],
            send_sem=st_send.at[to],
            recv_sem=st_recv.at[source],
            device_id={"sp": to},
            device_id_type=MESH,
        )

    def send_state(i, carry):
        state_copy(n - 1 - 2 * i, me, stsend).start()
        return carry

    own_logs = [spread(total, g * heads, heads) for g in range(2)]

    @pl.when(y == 0)
    def _():
        pack_state(own_logs)
        state_copy(pair, me, stsend).start()
        give_pair(1).start()
        give_pair(2).start()

    @pl.when(y == 1)
    def _():
        state_copy(me, pair, stsend).wait_recv()
        got = strecv[pair].astype(jnp.float32)
        for g in range(2):
            base, size = (0, s1) if g == 0 else (s1, s2)
            st[base : base + size] = (
                st[base : base + size] + got[base : base + size] * jnp.exp(own_logs[g])
            )
        both = [a + b for a, b in zip(logs_of(got), own_logs)]
        pack_state(both)
        lax.fori_loop(0, m - 1 - q, send_state, 0)

    def relay_pair(w):
        take_unit(w, pair)
        send_along(w, pair, False)
        send_along(w, pair, True)

    relay_pair(0)

    @pl.when(y == 0)
    def _():
        relay_pair(1)

    st[...] = jnp.zeros_like(st)

    def add_state(source):
        got = strecv[source].astype(jnp.float32)
        logs = logs_of(got)
        for g in range(2):
            base, size = (0, s1) if g == 0 else (s1, s2)
            st[base : base + size] = (
                st[base : base + size] * jnp.exp(logs[g]) + got[base : base + size]
            )

    def take_state(before, carry):
        source = before * 2 + 1
        state_copy(n - 1, source, stsend).wait_recv()
        add_state(source)
        return carry

    @pl.when(y == 1)
    def _():
        lax.fori_loop(0, q, take_state, 0)

        @pl.when(q > 0)
        def _():
            entering[...] = st[...].astype(jnp.bfloat16)
            state_copy(pair, me, entering).start()

        give_pair(2).start()
        add_state(pair)
        relay_pair(1)

    @pl.when((y == 0) & (q > 0))
    def _():
        state_copy(me, pair, entering).wait_recv()
        st[...] = strecv[pair, 0:states].astype(jnp.float32)

    def share(buf, yy, source, b, sp, to, send, recv):
        piece = buf.at[yy, source, rows_of(b)]
        return pltpu.make_async_remote_copy(
            src_ref=piece,
            dst_ref=piece,
            send_sem=send,
            recv_sem=recv.at[source, b],
            device_id={"sp": sp, "tp": to},
            device_id_type=MESH,
        )

    def across(d):
        return lax.rem(my_x + d, nx) * 2

    def send_own(buf, yy, b, send, recv):
        for d in range(1, nx):
            to = across(d) + core
            share(buf, yy, t, b, me, to, send.at[d, b], recv).start()
        share(buf, yy, t, b, me, partner, send.at[0, b], recv).start()

    def forward(buf, yy, b, fwd, recv):
        for d in range(1, nx):
            source = across(d) + core
            move = share(buf, yy, source, b, me, partner, fwd.at[d, b], recv)
            move.wait_recv()
            move.start()

    def wait_rest(buf, yy, b, send, recv):
        share(buf, yy, partner, b, me, partner, send.at[0, b], recv).wait_recv()
        for d in range(1, nx):
            source = across(d) + (1 - core)
            share(buf, yy, source, b, me, partner, send.at[0, b], recv).wait_recv()

    def send_pair(b):
        share(stream, y, t, b, pair, t, p_send.at[0, b], p_recv).start()

    def forward_pair(b):
        for d in range(nx):
            source = across(d) + core
            move = share(stream, 1 - y, source, b, me, partner, p_fwd.at[d, b], p_recv)
            move.wait_recv()
            move.start()

    def wait_pair(b):
        for d in range(nx):
            source = across(d) + (1 - core)
            share(stream, 1 - y, source, b, me, partner, p_fwd.at[d, b], p_recv).wait_recv()

    def second_pass(b):
        r = rows_of(b)
        cum = cums[r]
        cum_t = cum.T
        grown = jnp.exp(cum)
        both = gate_ref[r].astype(jnp.float32)
        gates = [both[:, g, :] for g in range(2)]
        for g in range(2):
            off, size = (0, s1) if g == 0 else (2 * s1, s2)
            base = 0 if g == 0 else s1
            keys = kq[r, off : off + size]
            queries = kq[r, off + size : off + 2 * size]
            scores = lax.dot_general(
                queries, keys, (((1,), (1,)), ((), ())), preferred_element_type=jnp.float32
            )
            carried = jnp.dot(
                queries,
                st[base : base + size].astype(jnp.bfloat16),
                preferred_element_type=jnp.float32,
            )
            carried = carried * spread(grown, g * heads, heads)
            v = vals[r, g * half : (g + 1) * half]
            outs = []
            for h in range(heads):
                c = g * heads + h
                span = jnp.where(causal, cum[:, c : c + 1] - cum_t[c : c + 1, :], -jnp.inf)
                w = (jnp.exp(span) * scores).astype(jnp.bfloat16)
                lanes = slice(h * HEAD, (h + 1) * HEAD)
                y = jnp.dot(w, v[:, lanes], preferred_element_type=jnp.float32)
                y = y + carried[:, lanes]
                z = gates[g][:, lanes]
                y = y * (z * sigmoid(z))
                y = y * lax.rsqrt(jnp.mean(y * y, axis=1, keepdims=True) + EPSILON)
                outs.append(y)
            out = jnp.concatenate(outs, axis=1) * hgain_ref[g : g + 1]
            mix[0, t, r, g * half : (g + 1) * half] = out.astype(jnp.bfloat16)
        state_update(b, cum)
        send_own(mix, 0, b, m_send, m_recv)

    def project(b):
        r = rows_of(b)
        wait_rest(mix, 0, b, m_send, m_recv)
        acc = res_ref[r].astype(jnp.float32)
        for source in range(tp):
            for g in range(2):
                acc = acc + jnp.dot(
                    mix[0, source, r, g * half : (g + 1) * half],
                    wout_ref[g, source * half : (source + 1) * half],
                    preferred_element_type=jnp.float32,
                )
        stream[y, t, r] = acc.astype(jnp.bfloat16)
        send_own(stream, y, b, r_send, r_recv)
        send_pair(b)

    cols = res_ref.shape[1]

    def normalise(yy, b):
        r = rows_of(b)
        parts = [stream[yy, source, r].astype(jnp.float32) for source in range(tp)]
        square = sum(jnp.sum(p * p, axis=1, keepdims=True) for p in parts)
        scale = lax.rsqrt(square / (tp * cols) + EPSILON)
        for source in range(tp):
            lanes = slice(source * cols, (source + 1) * cols)
            normed[yy, r, lanes] = (parts[source] * scale * cgain_ref[:, lanes]).astype(
                jnp.bfloat16
            )

    down = 2

    def stage(b, carry):
        @pl.when(b < nb)
        def _():
            second_pass(b)

        relay_points(b)

        @pl.when((b >= 1) & (b < nb + 1))
        def _():
            forward(mix, 0, b - 1, m_fwd, m_recv)

        @pl.when((b >= 2) & (b < nb + 2))
        def _():
            project(b - 2)

        for turn in range(2):

            @pl.when((b == nb + 1 + turn) & (y == turn))
            def _():
                send_along(down, me, False, own=True)
                send_along(down, me, True, own=True)

            @pl.when((b == nb + 1 + turn) & (y != turn))
            def _():
                relay_pair(down)

        @pl.when((b >= 3) & (b < nb + 3))
        def _():
            forward(stream, y, b - 3, r_fwd, r_recv)
            for d in range(1, nx):
                source = across(d) + core
                share(stream, y, source, b - 3, pair, t, p_send.at[d, b - 3], p_recv).start()

        @pl.when((b >= 4) & (b < nb + 4))
        def _():
            wait_rest(stream, y, b - 4, r_send, r_recv)
            normalise(y, b - 4)

        @pl.when((b >= 6) & (b < nb + 6))
        def _():
            forward_pair(b - 6)

        @pl.when(b >= 7)
        def _():
            wait_pair(b - 7)
            normalise(1 - y, b - 7)

        return carry

    for copy in later:
        copy.wait()
    if m > 2:
        for k in (4, 5):
            relay_down(k)
            relay_up(k)
    lax.fori_loop(0, nb + 7, stage, 0)

    units = sums.shape[2] // shard
    between = (q > 0) & (q < m - 1)

    def relay_far(d):
        for sel in range(2):

            @pl.when(between & (q + d < m))
            def _():
                s = (q + d) * 2 + sel
                take_unit(down, s)
                send_along(down, s, False)

            @pl.when(between & (q - d >= 0))
            def _():
                s = (q - d) * 2 + sel
                take_unit(down, s)
                send_along(down, s, True)

    keep_own(down).wait()
    if units > 1:
        relay_far(1)

    def late(k, carry):
        relay_down(k)
        relay_up(k)
        return carry

    lax.fori_loop(max(early, 4), 4 * m, late, 0)
    for w in range(2):
        keep_own(w).wait()

    tall = 2 * BLOCK
    pieces = tokens // tall

    def pass_on(d, carry):
        relay_far(d)
        return carry

    near = jnp.minimum(q, m - 1 - q)

    def block_at(i):
        d = (i + 1) // 2
        side = jnp.where(lax.rem(i, 2) == 1, q + d, q - d)
        beyond = jnp.where(q < m - 1 - q, i, m - 1 - i)
        return jnp.where(i <= 2 * near, side, beyond)

    width = sums.shape[2]
    chunks = tp * cols // width
    per_owner = cols // width

    def shard_at(i):
        return block_at(i // 2) * 2 + lax.rem(i, 2)

    def take_down(i):
        @pl.when((i >= 2) & jnp.logical_not(between))
        def _():
            take_unit(down, shard_at(i))

    def chunk_at(i):
        return shard_at(i) if units == 1 else i

    def product(yy, k, p, count):
        r = pl.ds(pl.multiple_of(p * tall, tall), count * tall)
        block = weights[down, pl.ds(pl.multiple_of(k * width, width), width)]
        return lax.dot_general(
            hidden[yy, r], block, (((1,), (1,)), ((), ())), preferred_element_type=jnp.float32
        )

    def rows_at(p):
        return pl.ds(pl.multiple_of(p * tall, tall), tall)

    def give_copy(i, k, p):
        return pltpu.make_async_remote_copy(
            src_ref=give.at[lax.rem(i, 2), rows_at(p)],
            dst_ref=give_recv.at[k, rows_at(p)],
            send_sem=g_send.at[lax.rem(i, 2), p],
            recv_sem=g_recv.at[k, p],
            device_id={"tp": partner},
            device_id_type=MESH,
        )

    def pair_copy(i, k, p):
        return pltpu.make_async_remote_copy(
            src_ref=sums.at[lax.rem(i, slots), rows_at(p)],
            dst_ref=across_recv.at[k, rows_at(p)],
            send_sem=a_send.at[lax.rem(i, slots), p],
            recv_sem=a_recv.at[k, p],
            device_id={"sp": pair},
            device_id_type=MESH,
        )

    def owner_copy(i, k, p, source):
        return pltpu.make_async_remote_copy(
            src_ref=ready.at[lax.rem(i, slots), rows_at(p)],
            dst_ref=sums_recv.at[source, lax.rem(k, per_owner), rows_at(p)],
            send_sem=s_send.at[lax.rem(i, slots), p],
            recv_sem=s_recv.at[source, lax.rem(k, per_owner), p],
            device_id={"tp": k // per_owner},
            device_id_type=MESH,
        )

    keeps = core == y
    slots = sums.shape[0]

    def give_piece(i, p, count=1):
        k = chunk_at(i)
        for c in range(count):

            @pl.when(i >= 2)
            def _():
                give_copy(i, k, p + c).wait_send()

        r = pl.ds(pl.multiple_of(p * tall, tall), count * tall)
        give[lax.rem(i, 2), r] = product(1 - core, k, p, count).astype(jnp.bfloat16)
        for c in range(count):
            give_copy(i, k, p + c).start()

    def sum_piece(i, p, count=1):
        k = chunk_at(i)
        for c in range(count):

            @pl.when(jnp.logical_not(keeps) & (i >= slots))
            def _():
                pair_copy(i, k, p + c).wait_send()

            give_copy(i, k, p + c).wait_recv()
        r = pl.ds(pl.multiple_of(p * tall, tall), count * tall)
        both = product(core, k, p, count) + give_recv[k, r].astype(jnp.float32)
        sums[lax.rem(i, slots), r] = both.astype(jnp.bfloat16)

        @pl.when(jnp.logical_not(keeps))
        def _():
            for c in range(count):
                pair_copy(i, k, p + c).start()

    many = 2 if pieces % 2 == 0 else 1

    def give_half(i):
        def one(p, carry):
            give_piece(i, p * many, many)
            return carry

        lax.fori_loop(0, pieces // many, one, 0)

    def sum_half(i):
        def one(p, carry):
            sum_piece(i, p * many, many)
            return carry

        lax.fori_loop(0, pieces // many, one, 0)

    def sum_pair(i):
        k = chunk_at(i)
        away = k // per_owner != t
        before = chunk_at(jnp.maximum(i - slots, 0))

        def one(p, carry):
            @pl.when((i >= slots) & (before // per_owner != t))
            def _():
                owner_copy(i, before, p, my_x).wait_send()

            pair_copy(i, k, p).wait_recv()
            r = rows_at(p)
            both = sums[lax.rem(i, slots), r].astype(jnp.float32) + across_recv[k, r].astype(
                jnp.float32
            )
            both = both.astype(jnp.bfloat16)

            @pl.when(away)
            def _():
                ready[lax.rem(i, slots), r] = both
                owner_copy(i, k, p, my_x).start()

            @pl.when(jnp.logical_not(away))
            def _():
                sums_recv[my_x, lax.rem(k, per_owner), r] = both

            return carry

        lax.fori_loop(0, pieces, one, 0)

    def take_all(i, carry):
        take_down(i)
        return carry

    if units > 1:
        lax.fori_loop(2, m, pass_on, 0)
        lax.fori_loop(0, n, take_all, 0)

    def mix_channels(yy, p):
        rows = normed[yy, rows_at(p)]
        g = jnp.dot(rows, weights[0], preferred_element_type=jnp.float32)
        u = jnp.dot(rows, weights[1], preferred_element_type=jnp.float32)
        hidden[yy, rows_at(p)] = (g * sigmoid(g) * u).astype(jnp.bfloat16)

    ahead = min(2, chunks)

    def pair_half(i):
        if units == 1:
            take_down(i)

        @pl.when(keeps)
        def _():
            give_half(i)

        @pl.when(jnp.logical_not(keeps))
        def _():
            sum_half(i)

    def mix_step(j, carry):
        p = lax.rem(j, pieces)
        theirs = j < pieces
        mix_channels(jnp.where(theirs, 1 - y, y), p)

        @pl.when(theirs & keeps)
        def _():
            for i in range(ahead):
                give_piece(i, p)

        @pl.when(theirs & jnp.logical_not(keeps))
        def _():
            for i in range(ahead):
                sum_piece(i, p)

        @pl.when(j == pieces - 1)
        def _():
            if units == 1:
                relay_far(1)
            if chunks > ahead:
                pair_half(ahead)

        @pl.when(j == 2 * pieces - 2)
        def _():
            if chunks > ahead + 1:
                pair_half(ahead + 1)

        return carry

    lax.fori_loop(0, 2 * pieces, mix_step, 0)

    middle = chunks // 2

    def chunk_step(i, carry):
        early = (i >= 1) & (i < middle - 1)
        late_on = (i > middle) & (i < chunks - 1)
        far = jnp.where(i < middle, i + 3, i + 1)

        if units == 1:

            @pl.when(i == min(2, chunks - 1))
            def _():
                lax.fori_loop(2, m, pass_on, 0)

        @pl.when(jnp.logical_not(keeps))
        def _():
            give_half(i)

        if units == 1:

            @pl.when(early)
            def _():
                take_down(far)

        @pl.when(keeps & early)
        def _():
            give_half(far)

        @pl.when(keeps & (i >= chunks - 2) & (i >= 1))
        def _():
            sum_pair(i - 1)

        @pl.when(keeps)
        def _():
            sum_half(i)

        @pl.when(keeps & (i < chunks - 2) & (i >= 1))
        def _():
            sum_pair(i - 1)

        if units == 1:

            @pl.when(late_on)
            def _():
                take_down(far)

        @pl.when(keeps & late_on)
        def _():
            give_half(far)

        @pl.when(jnp.logical_not(keeps) & (early | late_on))
        def _():
            sum_half(far)

        return carry

    lax.fori_loop(0, chunks, chunk_step, 0)

    @pl.when(keeps)
    def _():
        sum_pair(chunks - 1)

    def finish(p, carry):
        r = rows_at(p)
        for c in range(per_owner):
            for source in range(nx):

                @pl.when((source != my_x) | jnp.logical_not(keeps))
                def _():
                    owner_copy(0, c, p, source).wait_recv()

            lanes = slice(c * width, (c + 1) * width)
            total = sums_recv[0, c, r].astype(jnp.float32)
            for source in range(1, nx):
                total = total + sums_recv[source, c, r].astype(jnp.float32)
            own = stream[y, t, r, lanes].astype(jnp.float32)
            out_ref[r, lanes] = (own + 0.5 * total).astype(jnp.bfloat16)
        return carry

    lax.fori_loop(0, pieces, finish, 0)

    def end_sums(p, carry):
        for i in range(max(chunks - 2, 0), chunks):
            give_copy(i, chunk_at(i), p).wait_send()
        for i in range(max(chunks - slots, 0), chunks):
            last = chunk_at(i)

            @pl.when(jnp.logical_not(keeps))
            def _():
                pair_copy(i, last, p).wait_send()

            @pl.when(keeps & (last // per_owner != t))
            def _():
                owner_copy(i, last, p, my_x).wait_send()

        return carry

    lax.fori_loop(0, pieces, end_sums, 0)

    @pl.when(me < n - 1)
    def _():
        rim_copy.wait_send()

    def end_state(i, carry):
        state_copy(n - 1 - 2 * i, me, stsend).wait_send()
        return carry

    @pl.when(y == 0)
    def _():
        state_copy(pair, me, stsend).wait_send()

    @pl.when(y == 1)
    def _():
        lax.fori_loop(0, m - 1 - q, end_state, 0)

        @pl.when(q > 0)
        def _():
            state_copy(pair, me, entering).wait_send()

    def end_shares(b, carry):
        for buf, yy, send, fwd, recv in (
            (mix, 0, m_send, m_fwd, m_recv),
            (stream, y, r_send, r_fwd, r_recv),
        ):
            for d in range(nx):
                share(buf, yy, t, b, me, partner, send.at[d, b], recv).wait_send()
            for d in range(1, nx):
                share(buf, yy, t, b, me, partner, fwd.at[d, b], recv).wait_send()
        for d in range(nx):
            share(stream, y, t, b, me, partner, p_send.at[d, b], p_recv).wait_send()
            share(stream, y, t, b, me, partner, p_fwd.at[d, b], p_recv).wait_send()
        return carry

    lax.fori_loop(0, nb, end_shares, 0)

    def end_weights(s, carry):
        for w in range(3):
            @pl.when((s // 2 >= q) & (q > 0))
            def _():
                along(w, s, False).wait_send()

            @pl.when((s // 2 <= q) & (q < m - 1))
            def _():
                along(w, s, True).wait_send()

        return carry

    lax.fori_loop(0, n, end_weights, 0)
    for w in range(3):
        give_pair(w).wait_send()


def layer(front, later, wg, wu, wd, heads, s1, s2):
    n, tp = lax.axis_size("sp"), lax.axis_size("tp")
    gate, wout, residual = later
    tokens = gate.shape[0]
    half = heads * HEAD
    lanes = 2 * (half + s1 + s2)
    rows8 = -(-2 * heads // 8) * 8
    cols = residual.shape[1]
    nb = tokens // BLOCK
    shard, units = wg.shape
    part = units // 2
    split = part % LANES != 0
    if split:
        wg, wu, wd = (w.reshape(shard, 2, part).swapaxes(0, 1) for w in (wg, wu, wd))
    width = max(shard, min(cols, 2 * LANES))
    chunks = tp * cols // width
    pieces = tokens // (2 * BLOCK)
    vmem = pl.BlockSpec(memory_space=pltpu.VMEM)
    hbm = pl.BlockSpec(memory_space=pl.ANY)
    dma = pltpu.SemaphoreType.DMA
    return pl.pallas_call(
        functools.partial(layer_kernel, n, tp, heads, s1, s2, split),
        out_shape=jax.ShapeDtypeStruct((tokens, cols), jnp.bfloat16),
        in_specs=[vmem] * 7
        + [pl.BlockSpec(memory_space=pltpu.SMEM)]
        + [vmem] * 5
        + [hbm] * 6,
        out_specs=vmem,
        scratch_shapes=[
            pltpu.VMEM(gate.shape, gate.dtype),
            pltpu.VMEM(wout.shape, wout.dtype),
            pltpu.VMEM(residual.shape, residual.dtype),
            dma((3,)),
            pltpu.VMEM((CONV, lanes), jnp.float32),
            pltpu.VMEM((rows8, tokens), jnp.float32),
            pltpu.VMEM((rows8, tokens), jnp.float32),
            pltpu.VMEM((RIM, lanes), jnp.bfloat16),
            pltpu.VMEM((8, lanes), jnp.float32),
            pltpu.VMEM((RIM, lanes), jnp.bfloat16),
            pltpu.VMEM((tokens, 2 * half), jnp.bfloat16),
            pltpu.VMEM((tokens, 2 * (s1 + s2)), jnp.bfloat16),
            pltpu.VMEM((tokens, BLOCK), jnp.float32),
            pltpu.VMEM((s1 + s2, half), jnp.float32),
            pltpu.VMEM((s1 + s2 + RIM, half), jnp.bfloat16),
            pltpu.VMEM((s1 + s2, half), jnp.bfloat16),
            pltpu.VMEM((n, s1 + s2 + RIM, half), jnp.bfloat16),
            pltpu.VMEM((1, tp, tokens, 2 * half), jnp.bfloat16),
            pltpu.VMEM((2, tp, tokens, cols), jnp.bfloat16),
            pltpu.VMEM((2, tokens, tp * cols), jnp.bfloat16),
            pltpu.VMEM((3, n * shard, part), jnp.bfloat16),
            pltpu.VMEM((2, tokens, part), jnp.bfloat16),
            pltpu.VMEM((2, tokens, width), jnp.bfloat16),
            pltpu.VMEM((chunks, tokens, width), jnp.bfloat16),
            pltpu.VMEM((SLOTS, tokens, width), jnp.bfloat16),
            pltpu.VMEM((chunks, tokens, width), jnp.bfloat16),
            pltpu.VMEM((SLOTS, tokens, width), jnp.bfloat16),
            pltpu.VMEM((tp // 2, cols // width, tokens, width), jnp.bfloat16),
            dma((2,)),
            dma((n,)),
            dma((n,)),
            dma((tp // 2, nb)),
            dma((tp // 2, nb)),
            dma((tp, nb)),
            dma((tp // 2, nb)),
            dma((tp // 2, nb)),
            dma((tp, nb)),
            dma((tp // 2, nb)),
            dma((tp // 2, nb)),
            dma((tp, nb)),
            dma((3,)),
            dma((3,)),
            dma((2, 3, n)),
            dma((3, n)),
            dma((2, pieces)),
            dma((chunks, pieces)),
            dma((SLOTS, pieces)),
            dma((chunks, pieces)),
            dma((SLOTS, pieces)),
            dma((tp // 2, cols // width, pieces)),
        ],
        compiler_params=pltpu.CompilerParams(
            has_side_effects=True, vmem_limit_bytes=VMEM_LIMIT
        ),
        name="layer",
    )(*front, gate, wout, residual, wg, wu, wd)


def shards(
    grouped_head_inputs,
    head_gate_inputs,
    unsmoothed_step,
    head_decay_rate,
    extra_log_decay,
    first_group_keys,
    first_group_queries,
    second_group_keys,
    second_group_queries,
    head_input_filter,
    first_group_filter,
    second_group_filter,
    head_norm_gain,
    output_weight,
    residual,
    channel_norm_gain,
    channel_gate_weight,
    channel_up_weight,
    channel_down_weight,
):
    heads = head_decay_rate.shape[1]
    s1, s2 = first_group_keys.shape[1], second_group_keys.shape[1]
    return layer(
        (
            grouped_head_inputs,
            first_group_keys,
            first_group_queries,
            second_group_keys.T,
            second_group_queries.T,
            unsmoothed_step.transpose(1, 2, 0),
            extra_log_decay.transpose(1, 2, 0),
            head_decay_rate,
            head_input_filter,
            first_group_filter,
            second_group_filter,
            head_norm_gain,
            channel_norm_gain.reshape(1, -1),
        ),
        (head_gate_inputs, output_weight, residual),
        channel_gate_weight,
        channel_up_weight,
        channel_down_weight,
        heads,
        s1,
        s2,
    )


def solution(mesh):
    return jax.shard_map(
        shards,
        mesh=mesh,
        in_specs=(
            P("sp", None, "tp"),
            P("sp", None, "tp"),
            P("sp", None, "tp"),
            P(None, "tp"),
            P("sp", None, "tp"),
            P("sp", None),
            P("sp", None),
            P("sp", None),
            P("sp", None),
            P(None, None, "tp"),
            P(),
            P(),
            P(None, "tp"),
            P(None, None, "tp"),
            P("sp", "tp"),
            P(),
            P("sp", "tp"),
            P("sp", "tp"),
            P("sp", "tp"),
        ),
        out_specs=P("sp", "tp"),
        check_vma=False,
    )
```

```python
import functools

import jax
import jax.numpy as jnp
from jax import lax
from jax.experimental import pallas as pl
from jax.experimental.pallas import tpu as pltpu
from jax.sharding import PartitionSpec as P

HEAD = 64
CONV = 4
BLOCK = 128
RIM = 16
EPSILON = 1e-06
LANES = 128
SLOTS = 4
VMEM_LIMIT = 63 << 20
MESH = pl.DeviceIdType.MESH


def rows_of(b):
    return pl.ds(pl.multiple_of(b * BLOCK, BLOCK), BLOCK)


def spread(columns, first, count):
    parts = [
        jnp.broadcast_to(columns[:, h : h + 1], (columns.shape[0], HEAD))
        for h in range(first, first + count)
    ]
    return jnp.concatenate(parts, axis=1)


def sigmoid(x):
    return 1.0 / (1.0 + jnp.exp(-x))


def layer_kernel(
    n, tp, heads, s1, s2, split,
    x_ref, keys1_ref, queries1_ref, keys2_ref, queries2_ref, unsmoothed_ref, extra_ref, rate_ref,
    head_taps_ref, taps1_ref, taps2_ref, hgain_ref, cgain_ref,
    gate_in, wout_in, res_in, wg_ref, wu_ref, wd_ref,
    out_ref,
    gate_ref, wout_ref, res_ref, in_sems, taps_ref, step_rows, log_rows, rim_out, xs, rim, vals, kq, cums, st, stsend, entering, strecv, mix, stream, normed, weights, hidden,
    give, give_recv, sums, across_recv, ready, sums_recv,
    rim_sems, st_send, st_recv, m_send, m_fwd, m_recv, r_send, r_fwd, r_recv,
    p_send, p_fwd, p_recv, w_local, w_pair, w_send, w_recv,
    g_send, g_recv, a_send, a_recv, s_send, s_recv,
):
    me = lax.axis_index("sp")
    t = lax.axis_index("tp")
    half = heads * HEAD
    wide = 2 * half
    nb = x_ref.shape[0] // BLOCK
    nx = tp // 2
    core = lax.rem(t, 2)
    my_x = t // 2
    partner = my_x * 2 + (1 - core)

    m = n // 2
    q = me // 2
    y = lax.rem(me, 2)
    pair = q * 2 + (1 - y)
    shard = wg_ref.shape[-2]
    tokens = x_ref.shape[0]
    sources = (wg_ref, wu_ref, wd_ref)
    part = weights.shape[2]

    def half_of(w, which):
        if split:
            return sources[w].at[which]
        return sources[w].at[:, pl.ds(pl.multiple_of(which * part, part), part)]

    def unit(w, s):
        return weights.at[w, pl.ds(pl.multiple_of(s * shard, shard), shard)]

    def keep_own(w):
        return pltpu.make_async_copy(half_of(w, y), unit(w, me), w_local.at[w])

    def give_pair(w):
        return pltpu.make_async_remote_copy(
            src_ref=half_of(w, 1 - y),
            dst_ref=unit(w, me),
            send_sem=w_pair.at[w],
            recv_sem=w_recv.at[w, me],
            device_id={"sp": pair},
            device_id_type=MESH,
        )

    def along(w, s, up, own=False):
        return pltpu.make_async_remote_copy(
            src_ref=half_of(w, y) if own else unit(w, s),
            dst_ref=unit(w, s),
            send_sem=w_send.at[int(up), w, s],
            recv_sem=w_recv.at[w, s],
            device_id={"sp": lax.rem(me + 2, n) if up else lax.rem(me + n - 2, n)},
            device_id_type=MESH,
        )

    def send_along(w, s, up, own=False):
        @pl.when(q < m - 1 if up else q > 0)
        def _():
            along(w, s, up, own).start()

    def take_unit(w, s):
        along(w, s, True).wait_recv()

    def start_weights():
        give_pair(0).start()

        @pl.when(y == 1)
        def _():
            give_pair(1).start()

        @pl.when(y == 1)
        def _():
            for w in range(2):
                send_along(w, me, True, own=True)

        for w in range(3):
            keep_own(w).start()

    def relay_down(k):
        w, d, sel = lax.rem(k, 2), k // 4, lax.rem(k // 2, 2)

        @pl.when(q + d < m)
        def _():
            s = (q + d) * 2 + lax.rem(y + sel, 2)
            take_unit(w, s)
            send_along(w, s, False)

    def relay_up(k):
        w, d, sel = lax.rem(k, 2), k // 4, lax.rem(k // 2, 2)

        @pl.when(q - d >= 0)
        def _():
            s = (q - d) * 2 + lax.rem(y + sel, 2)
            take_unit(w, s)
            send_along(w, s, True)

    early = 4 * (m - 1)
    stride = max(m - 3, 0)

    def relay_points(b):
        for j, at in ((6, 1), (7, 3)):

            @pl.when(b == at)
            def _():
                if m > 2:
                    relay_down(j)
                    relay_up(j)

        for j in range(4):

            @pl.when(b == nb - 3 + j)
            def _():
                for i in range(stride):
                    relay_down(8 + j * stride + i)
                    relay_up(8 + j * stride + i)

    later = [
        pltpu.make_async_copy(source, place, in_sems.at[i])
        for i, (source, place) in enumerate(
            ((gate_in, gate_ref), (wout_in, wout_ref), (res_in, res_ref))
        )
    ]

    def tokens_of(b):
        r = rows_of(b)
        second = jnp.concatenate([keys2_ref[:, r], queries2_ref[:, r]], axis=0)
        heads_in = x_ref[r].astype(jnp.float32)
        return jnp.concatenate(
            [
                heads_in[:, 0, :],
                heads_in[:, 1, :],
                keys1_ref[r].astype(jnp.float32),
                queries1_ref[r].astype(jnp.float32),
                second.astype(jnp.float32).T,
            ],
            axis=1,
        )

    rim_copy = pltpu.make_async_remote_copy(
        src_ref=rim_out,
        dst_ref=rim,
        send_sem=rim_sems.at[0],
        recv_sem=rim_sems.at[1],
        device_id={"sp": lax.rem(me + 1, n)},
        device_id_type=MESH,
    )

    for w in range(2):
        send_along(w, me, False, own=True)

    @pl.when(y == 0)
    def _():
        for w in range(2):
            send_along(w, me, True, own=True)

    @pl.when(me < n - 1)
    def _():
        rim_out[...] = tokens_of(nb - 1)[BLOCK - RIM :].astype(jnp.bfloat16)
        rim_copy.start()

    start_weights()

    for copy in later:
        copy.start()

    for g in range(2):
        taps_ref[:, g * half : (g + 1) * half] = head_taps_ref[:, g, :]
        taps_ref[:, wide + g * s1 : wide + (g + 1) * s1] = taps1_ref[:, g, :]
    taps_ref[:, wide + 2 * s1 :] = jnp.concatenate([taps2_ref[:, 0, :], taps2_ref[:, 1, :]], axis=1)

    unsmoothed = unsmoothed_ref[...]
    steps = jnp.maximum(unsmoothed, 0.0) + jnp.log1p(jnp.exp(-jnp.abs(unsmoothed)))
    step_rows[...] = jnp.zeros_like(step_rows)
    log_rows[...] = jnp.zeros_like(log_rows)
    for g in range(2):
        for h in range(heads):
            c = g * heads + h
            row = steps[g, h : h + 1]
            step_rows[c : c + 1] = row
            log_rows[c : c + 1] = extra_ref[g, h : h + 1] - row * rate_ref[g, h]

    @pl.when(me > 0)
    def _():
        rim_copy.wait_recv()
        xs[...] = rim[...].astype(jnp.float32)[RIM - 8 :]

    @pl.when(me == 0)
    def _():
        xs[...] = jnp.zeros_like(xs)

    st[...] = jnp.zeros_like(st)
    row_i = lax.broadcasted_iota(jnp.int32, (BLOCK, BLOCK), 0)
    col_i = lax.broadcasted_iota(jnp.int32, (BLOCK, BLOCK), 1)
    causal = row_i >= col_i
    tri = jnp.where(row_i <= col_i, 1.0, 0.0).astype(jnp.float32)
    rows8 = log_rows.shape[0]

    def state_update(b, cum):
        last = cum[BLOCK - 1 : BLOCK]
        to_end = jnp.exp(last - cum)
        decay = jnp.exp(last)
        r = rows_of(b)
        for g in range(2):
            k0, size = (wide, s1) if g == 0 else (wide + 2 * s1, s2)
            base = 0 if g == 0 else s1
            keys = kq[r, k0 - wide : k0 - wide + size]
            v = vals[r, g * half : (g + 1) * half].astype(jnp.float32)
            v = (v * spread(to_end, g * heads, heads)).astype(jnp.bfloat16)
            add = lax.dot_general(
                keys, v, (((0,), (0,)), ((), ())), preferred_element_type=jnp.float32
            )
            st[base : base + size] = (
                st[base : base + size] * spread(decay, g * heads, heads) + add
            )

    def first_pass(b, total):
        r = rows_of(b)
        current = tokens_of(b)
        taps = taps_ref[...]
        extended = jnp.concatenate([xs[...], current], axis=0)
        acc = taps[CONV - 1 : CONV] * current
        for k in range(CONV - 1):
            acc = acc + taps[k : k + 1] * pltpu.roll(extended, CONV - 1 - k, 0)[8:]
        xs[...] = current[BLOCK - 8 :]
        acc = acc * sigmoid(acc)
        cum_rows = jnp.dot(
            log_rows[:, r], tri, precision=lax.Precision.HIGHEST, preferred_element_type=jnp.float32
        )
        fill = jnp.zeros((BLOCK - 2 * rows8, BLOCK), jnp.float32)
        cum = jnp.concatenate([cum_rows, step_rows[:, r], fill], axis=0).T
        cums[r] = cum
        vals[r] = (acc[:, :wide] * spread(cum, rows8, 2 * heads)).astype(jnp.bfloat16)
        kq[r] = acc[:, wide:].astype(jnp.bfloat16)
        state_update(b, cum)

        return total + cum[BLOCK - 1 : BLOCK]

    total = lax.fori_loop(0, nb, first_pass, jnp.zeros((1, BLOCK), jnp.float32))

    states = s1 + s2

    def pack_state(total):
        stsend[0:states] = st[...].astype(jnp.bfloat16)
        which = lax.broadcasted_iota(jnp.int32, (RIM, half), 0)
        extra = jnp.zeros((RIM, half), jnp.float32)
        for g in range(2):
            logs = total[g]
            high = logs.astype(jnp.bfloat16).astype(jnp.float32)
            low = logs - high
            extra = jnp.where(which == g, high, extra)
            extra = jnp.where(which == 2 + g, low, extra)
        stsend[states : states + RIM] = extra.astype(jnp.bfloat16)

    def logs_of(got):
        return [
            got[states + g : states + g + 1] + got[states + 2 + g : states + 3 + g]
            for g in range(2)
        ]

    def state_copy(to, source, packed):
        return pltpu.make_async_remote_copy(
            src_ref=packed,
            dst_ref=strecv.at[source, pl.ds(0, packed.shape[0])],
            send_sem=st_send.at[to],
            recv_sem=st_recv.at[source],
            device_id={"sp": to},
            device_id_type=MESH,
        )

    def send_state(i, carry):
        state_copy(n - 1 - 2 * i, me, stsend).start()
        return carry

    own_logs = [spread(total, g * heads, heads) for g in range(2)]

    @pl.when(y == 0)
    def _():
        pack_state(own_logs)
        state_copy(pair, me, stsend).start()
        give_pair(1).start()
        give_pair(2).start()

    @pl.when(y == 1)
    def _():
        state_copy(me, pair, stsend).wait_recv()
        got = strecv[pair].astype(jnp.float32)
        for g in range(2):
            base, size = (0, s1) if g == 0 else (s1, s2)
            st[base : base + size] = (
                st[base : base + size] + got[base : base + size] * jnp.exp(own_logs[g])
            )
        both = [a + b for a, b in zip(logs_of(got), own_logs)]
        pack_state(both)
        lax.fori_loop(0, m - 1 - q, send_state, 0)

    def relay_pair(w):
        take_unit(w, pair)
        send_along(w, pair, False)
        send_along(w, pair, True)

    relay_pair(0)

    @pl.when(y == 0)
    def _():
        relay_pair(1)

    st[...] = jnp.zeros_like(st)

    def add_state(source):
        got = strecv[source].astype(jnp.float32)
        logs = logs_of(got)
        for g in range(2):
            base, size = (0, s1) if g == 0 else (s1, s2)
            st[base : base + size] = (
                st[base : base + size] * jnp.exp(logs[g]) + got[base : base + size]
            )

    def take_state(before, carry):
        source = before * 2 + 1
        state_copy(n - 1, source, stsend).wait_recv()
        add_state(source)
        return carry

    @pl.when(y == 1)
    def _():
        lax.fori_loop(0, q, take_state, 0)

        @pl.when(q > 0)
        def _():
            entering[...] = st[...].astype(jnp.bfloat16)
            state_copy(pair, me, entering).start()

        give_pair(2).start()
        add_state(pair)
        relay_pair(1)

    @pl.when((y == 0) & (q > 0))
    def _():
        state_copy(me, pair, entering).wait_recv()
        st[...] = strecv[pair, 0:states].astype(jnp.float32)

    def share(buf, yy, source, b, sp, to, send, recv):
        piece = buf.at[yy, source, rows_of(b)]
        return pltpu.make_async_remote_copy(
            src_ref=piece,
            dst_ref=piece,
            send_sem=send,
            recv_sem=recv.at[source, b],
            device_id={"sp": sp, "tp": to},
            device_id_type=MESH,
        )

    def across(d):
        return lax.rem(my_x + d, nx) * 2

    def send_own(buf, yy, b, send, recv):
        for d in range(1, nx):
            to = across(d) + core
            share(buf, yy, t, b, me, to, send.at[d, b], recv).start()
        share(buf, yy, t, b, me, partner, send.at[0, b], recv).start()

    def forward(buf, yy, b, fwd, recv):
        for d in range(1, nx):
            source = across(d) + core
            move = share(buf, yy, source, b, me, partner, fwd.at[d - 1, b], recv)
            move.wait_recv()
            move.start()

    def wait_rest(buf, yy, b, send, recv):
        share(buf, yy, partner, b, me, partner, send.at[0, b], recv).wait_recv()
        for d in range(1, nx):
            source = across(d) + (1 - core)
            share(buf, yy, source, b, me, partner, send.at[0, b], recv).wait_recv()

    def send_pair(b):
        share(stream, y, t, b, pair, t, p_send.at[0, b], p_recv).start()

    def forward_pair(b):
        for d in range(nx):
            source = across(d) + core
            move = share(stream, 1 - y, source, b, me, partner, p_fwd.at[d, b], p_recv)
            move.wait_recv()
            move.start()

    def wait_pair(b):
        for d in range(nx):
            source = across(d) + (1 - core)
            share(stream, 1 - y, source, b, me, partner, p_fwd.at[d, b], p_recv).wait_recv()

    def second_pass(b):
        r = rows_of(b)
        cum = cums[r]
        cum_t = cum.T
        grown = jnp.exp(cum)
        both = gate_ref[r].astype(jnp.float32)
        gates = [both[:, g, :] for g in range(2)]
        for g in range(2):
            off, size = (0, s1) if g == 0 else (2 * s1, s2)
            base = 0 if g == 0 else s1
            keys = kq[r, off : off + size]
            queries = kq[r, off + size : off + 2 * size]
            scores = lax.dot_general(
                queries, keys, (((1,), (1,)), ((), ())), preferred_element_type=jnp.float32
            )
            carried = jnp.dot(
                queries,
                st[base : base + size].astype(jnp.bfloat16),
                preferred_element_type=jnp.float32,
            )
            carried = carried * spread(grown, g * heads, heads)
            v = vals[r, g * half : (g + 1) * half]
            outs = []
            for h in range(heads):
                c = g * heads + h
                span = jnp.where(causal, cum[:, c : c + 1] - cum_t[c : c + 1, :], -jnp.inf)
                w = (jnp.exp(span) * scores).astype(jnp.bfloat16)
                lanes = slice(h * HEAD, (h + 1) * HEAD)
                y = jnp.dot(w, v[:, lanes], preferred_element_type=jnp.float32)
                y = y + carried[:, lanes]
                z = gates[g][:, lanes]
                y = y * (z * sigmoid(z))
                y = y * lax.rsqrt(jnp.mean(y * y, axis=1, keepdims=True) + EPSILON)
                outs.append(y)
            out = jnp.concatenate(outs, axis=1) * hgain_ref[g : g + 1]
            mix[0, t, r, g * half : (g + 1) * half] = out.astype(jnp.bfloat16)
        state_update(b, cum)
        send_own(mix, 0, b, m_send, m_recv)

    def project(b):
        r = rows_of(b)
        wait_rest(mix, 0, b, m_send, m_recv)
        acc = res_ref[r].astype(jnp.float32)
        for source in range(tp):
            for g in range(2):
                acc = acc + jnp.dot(
                    mix[0, source, r, g * half : (g + 1) * half],
                    wout_ref[g, source * half : (source + 1) * half],
                    preferred_element_type=jnp.float32,
                )
        stream[y, t, r] = acc.astype(jnp.bfloat16)
        send_own(stream, y, b, r_send, r_recv)
        send_pair(b)

    cols = res_ref.shape[1]

    def normalise(yy, b):
        r = rows_of(b)
        parts = [stream[yy, source, r].astype(jnp.float32) for source in range(tp)]
        square = sum(jnp.sum(p * p, axis=1, keepdims=True) for p in parts)
        scale = lax.rsqrt(square / (tp * cols) + EPSILON)
        for source in range(tp):
            lanes = slice(source * cols, (source + 1) * cols)
            normed[yy, r, lanes] = (parts[source] * scale * cgain_ref[:, lanes]).astype(
                jnp.bfloat16
            )

    down = 2

    def stage(b, carry):
        @pl.when(b < nb)
        def _():
            second_pass(b)

        relay_points(b)

        @pl.when((b >= 1) & (b < nb + 1))
        def _():
            forward(mix, 0, b - 1, m_fwd, m_recv)

        @pl.when((b >= 2) & (b < nb + 2))
        def _():
            project(b - 2)

        for turn in range(2):

            @pl.when((b == nb + 1 + turn) & (y == turn))
            def _():
                send_along(down, me, False, own=True)
                send_along(down, me, True, own=True)

            @pl.when((b == nb + 1 + turn) & (y != turn))
            def _():
                relay_pair(down)

        @pl.when((b >= 3) & (b < nb + 3))
        def _():
            forward(stream, y, b - 3, r_fwd, r_recv)
            for d in range(1, nx):
                source = across(d) + core
                share(stream, y, source, b - 3, pair, t, p_send.at[d, b - 3], p_recv).start()

        @pl.when((b >= 4) & (b < nb + 4))
        def _():
            wait_rest(stream, y, b - 4, r_send, r_recv)
            normalise(y, b - 4)

        @pl.when((b >= 6) & (b < nb + 6))
        def _():
            forward_pair(b - 6)

        @pl.when(b >= 7)
        def _():
            wait_pair(b - 7)
            normalise(1 - y, b - 7)

        return carry

    for copy in later:
        copy.wait()
    if m > 2:
        for k in (4, 5):
            relay_down(k)
            relay_up(k)
    lax.fori_loop(0, nb + 7, stage, 0)

    units = sums.shape[2] // shard
    between = (q > 0) & (q < m - 1)

    def relay_far(d):
        for sel in range(2):

            @pl.when(between & (q + d < m))
            def _():
                s = (q + d) * 2 + sel
                take_unit(down, s)
                send_along(down, s, False)

            @pl.when(between & (q - d >= 0))
            def _():
                s = (q - d) * 2 + sel
                take_unit(down, s)
                send_along(down, s, True)

    keep_own(down).wait()
    if units > 1:
        relay_far(1)

    def late(k, carry):
        relay_down(k)
        relay_up(k)
        return carry

    lax.fori_loop(max(early, 4), 4 * m, late, 0)
    for w in range(2):
        keep_own(w).wait()

    tall = 2 * BLOCK
    pieces = tokens // tall

    def pass_on(d, carry):
        relay_far(d)
        return carry

    near = jnp.minimum(q, m - 1 - q)

    def block_at(i):
        d = (i + 1) // 2
        side = jnp.where(lax.rem(i, 2) == 1, q + d, q - d)
        beyond = jnp.where(q < m - 1 - q, i, m - 1 - i)
        return jnp.where(i <= 2 * near, side, beyond)

    width = sums.shape[2]
    chunks = tp * cols // width
    per_owner = cols // width

    def shard_at(i):
        return block_at(i // 2) * 2 + lax.rem(i, 2)

    def take_down(i):
        @pl.when((i >= 2) & jnp.logical_not(between))
        def _():
            take_unit(down, shard_at(i))

    def chunk_at(i):
        return shard_at(i) if units == 1 else i

    def product(yy, k, p, count):
        r = pl.ds(pl.multiple_of(p * tall, tall), count * tall)
        block = weights[down, pl.ds(pl.multiple_of(k * width, width), width)]
        return lax.dot_general(
            hidden[yy, r], block, (((1,), (1,)), ((), ())), preferred_element_type=jnp.float32
        )

    def rows_at(p):
        return pl.ds(pl.multiple_of(p * tall, tall), tall)

    def give_copy(i, k, p):
        return pltpu.make_async_remote_copy(
            src_ref=give.at[lax.rem(i, 2), rows_at(p)],
            dst_ref=give_recv.at[k, rows_at(p)],
            send_sem=g_send.at[lax.rem(i, 2), p],
            recv_sem=g_recv.at[k, p],
            device_id={"tp": partner},
            device_id_type=MESH,
        )

    def pair_copy(i, k, p):
        return pltpu.make_async_remote_copy(
            src_ref=sums.at[lax.rem(i, slots), rows_at(p)],
            dst_ref=across_recv.at[k, rows_at(p)],
            send_sem=a_send.at[lax.rem(i, slots), p],
            recv_sem=a_recv.at[k, p],
            device_id={"sp": pair},
            device_id_type=MESH,
        )

    def owner_copy(i, k, p, source):
        return pltpu.make_async_remote_copy(
            src_ref=ready.at[lax.rem(i, slots), rows_at(p)],
            dst_ref=sums_recv.at[source, lax.rem(k, per_owner), rows_at(p)],
            send_sem=s_send.at[lax.rem(i, slots), p],
            recv_sem=s_recv.at[source, lax.rem(k, per_owner), p],
            device_id={"tp": k // per_owner},
            device_id_type=MESH,
        )

    keeps = core == y
    slots = sums.shape[0]

    def give_piece(i, p, count=1):
        k = chunk_at(i)
        for c in range(count):

            @pl.when(i >= 2)
            def _():
                give_copy(i, k, p + c).wait_send()

        r = pl.ds(pl.multiple_of(p * tall, tall), count * tall)
        give[lax.rem(i, 2), r] = product(1 - core, k, p, count).astype(jnp.bfloat16)
        for c in range(count):
            give_copy(i, k, p + c).start()

    def sum_piece(i, p, count=1):
        k = chunk_at(i)
        for c in range(count):

            @pl.when(jnp.logical_not(keeps) & (i >= slots))
            def _():
                pair_copy(i, k, p + c).wait_send()

            give_copy(i, k, p + c).wait_recv()
        r = pl.ds(pl.multiple_of(p * tall, tall), count * tall)
        both = product(core, k, p, count) + give_recv[k, r].astype(jnp.float32)
        sums[lax.rem(i, slots), r] = both.astype(jnp.bfloat16)

        @pl.when(jnp.logical_not(keeps))
        def _():
            for c in range(count):
                pair_copy(i, k, p + c).start()

    many = 2 if pieces % 2 == 0 else 1

    def give_half(i):
        def one(p, carry):
            give_piece(i, p * many, many)
            return carry

        lax.fori_loop(0, pieces // many, one, 0)

    def sum_half(i):
        def one(p, carry):
            sum_piece(i, p * many, many)
            return carry

        lax.fori_loop(0, pieces // many, one, 0)

    def sum_pair(i):
        k = chunk_at(i)
        away = k // per_owner != t
        before = chunk_at(jnp.maximum(i - slots, 0))

        def one(p, carry):
            @pl.when((i >= slots) & (before // per_owner != t))
            def _():
                owner_copy(i, before, p, my_x).wait_send()

            pair_copy(i, k, p).wait_recv()
            r = rows_at(p)
            both = sums[lax.rem(i, slots), r].astype(jnp.float32) + across_recv[k, r].astype(
                jnp.float32
            )
            both = both.astype(jnp.bfloat16)

            @pl.when(away)
            def _():
                ready[lax.rem(i, slots), r] = both
                owner_copy(i, k, p, my_x).start()

            @pl.when(jnp.logical_not(away))
            def _():
                sums_recv[my_x, lax.rem(k, per_owner), r] = both

            return carry

        lax.fori_loop(0, pieces, one, 0)

    def take_all(i, carry):
        take_down(i)
        return carry

    if units > 1:
        lax.fori_loop(2, m, pass_on, 0)
        lax.fori_loop(0, n, take_all, 0)

    def mix_channels(yy, p):
        rows = normed[yy, rows_at(p)]
        g = jnp.dot(rows, weights[0], preferred_element_type=jnp.float32)
        u = jnp.dot(rows, weights[1], preferred_element_type=jnp.float32)
        hidden[yy, rows_at(p)] = (g * sigmoid(g) * u).astype(jnp.bfloat16)

    ahead = min(2, chunks)

    def pair_half(i):
        if units == 1:
            take_down(i)

        @pl.when(keeps)
        def _():
            give_half(i)

        @pl.when(jnp.logical_not(keeps))
        def _():
            sum_half(i)

    def mix_step(j, carry):
        p = lax.rem(j, pieces)
        theirs = j < pieces
        mix_channels(jnp.where(theirs, 1 - y, y), p)

        @pl.when(theirs & keeps)
        def _():
            for i in range(ahead):
                give_piece(i, p)

        @pl.when(theirs & jnp.logical_not(keeps))
        def _():
            for i in range(ahead):
                sum_piece(i, p)

        @pl.when(j == pieces - 1)
        def _():
            if units == 1:
                relay_far(1)
            if chunks > ahead:
                pair_half(ahead)

        @pl.when(j == 2 * pieces - 2)
        def _():
            if chunks > ahead + 1:
                pair_half(ahead + 1)

        return carry

    lax.fori_loop(0, 2 * pieces, mix_step, 0)

    middle = chunks // 2

    def chunk_step(i, carry):
        early = (i >= 1) & (i < middle - 1)
        late_on = (i > middle) & (i < chunks - 1)
        far = jnp.where(i < middle, i + 3, i + 1)

        if units == 1:

            @pl.when(i == min(2, chunks - 1))
            def _():
                lax.fori_loop(2, m, pass_on, 0)

        @pl.when(jnp.logical_not(keeps))
        def _():
            give_half(i)

        if units == 1:

            @pl.when(early)
            def _():
                take_down(far)

        @pl.when(keeps & early)
        def _():
            give_half(far)

        @pl.when(keeps & (i >= chunks - 2) & (i >= 1))
        def _():
            sum_pair(i - 1)

        @pl.when(keeps)
        def _():
            sum_half(i)

        @pl.when(keeps & (i < chunks - 2) & (i >= 1))
        def _():
            sum_pair(i - 1)

        if units == 1:

            @pl.when(late_on)
            def _():
                take_down(far)

        @pl.when(keeps & late_on)
        def _():
            give_half(far)

        @pl.when(jnp.logical_not(keeps) & (early | late_on))
        def _():
            sum_half(far)

        return carry

    lax.fori_loop(0, chunks, chunk_step, 0)

    @pl.when(keeps)
    def _():
        sum_pair(chunks - 1)

    def finish(p, carry):
        r = rows_at(p)
        for c in range(per_owner):
            for source in range(nx):

                @pl.when((source != my_x) | jnp.logical_not(keeps))
                def _():
                    owner_copy(0, c, p, source).wait_recv()

            lanes = slice(c * width, (c + 1) * width)
            total = sums_recv[0, c, r].astype(jnp.float32)
            for source in range(1, nx):
                total = total + sums_recv[source, c, r].astype(jnp.float32)
            own = stream[y, t, r, lanes].astype(jnp.float32)
            out_ref[r, lanes] = (own + 0.5 * total).astype(jnp.bfloat16)
        return carry

    lax.fori_loop(0, pieces, finish, 0)

    def end_sums(p, carry):
        for i in range(max(chunks - 2, 0), chunks):
            give_copy(i, chunk_at(i), p).wait_send()
        for i in range(max(chunks - slots, 0), chunks):
            last = chunk_at(i)

            @pl.when(jnp.logical_not(keeps))
            def _():
                pair_copy(i, last, p).wait_send()

            @pl.when(keeps & (last // per_owner != t))
            def _():
                owner_copy(i, last, p, my_x).wait_send()

        return carry

    lax.fori_loop(0, pieces, end_sums, 0)

    @pl.when(me < n - 1)
    def _():
        rim_copy.wait_send()

    def end_state(i, carry):
        state_copy(n - 1 - 2 * i, me, stsend).wait_send()
        return carry

    @pl.when(y == 0)
    def _():
        state_copy(pair, me, stsend).wait_send()

    @pl.when(y == 1)
    def _():
        lax.fori_loop(0, m - 1 - q, end_state, 0)

        @pl.when(q > 0)
        def _():
            state_copy(pair, me, entering).wait_send()

    def end_shares(b, carry):
        for buf, yy, send, fwd, recv in (
            (mix, 0, m_send, m_fwd, m_recv),
            (stream, y, r_send, r_fwd, r_recv),
        ):
            for d in range(nx):
                share(buf, yy, t, b, me, partner, send.at[d, b], recv).wait_send()
            for d in range(1, nx):
                share(buf, yy, t, b, me, partner, fwd.at[d - 1, b], recv).wait_send()
        for d in range(nx):
            share(stream, y, t, b, me, partner, p_send.at[d, b], p_recv).wait_send()
            share(stream, y, t, b, me, partner, p_fwd.at[d, b], p_recv).wait_send()
        return carry

    lax.fori_loop(0, nb, end_shares, 0)

    def end_weights(s, carry):
        for w in range(3):
            @pl.when((s // 2 >= q) & (q > 0))
            def _():
                along(w, s, False).wait_send()

            @pl.when((s // 2 <= q) & (q < m - 1))
            def _():
                along(w, s, True).wait_send()

        return carry

    lax.fori_loop(0, n, end_weights, 0)
    for w in range(3):
        give_pair(w).wait_send()


def layer(front, later, wg, wu, wd, heads, s1, s2):
    n, tp = lax.axis_size("sp"), lax.axis_size("tp")
    gate, wout, residual = later
    tokens = gate.shape[0]
    half = heads * HEAD
    lanes = 2 * (half + s1 + s2)
    rows8 = -(-2 * heads // 8) * 8
    cols = residual.shape[1]
    nb = tokens // BLOCK
    shard, units = wg.shape
    part = units // 2
    split = part % LANES != 0
    if split:
        wg, wu, wd = (w.reshape(shard, 2, part).swapaxes(0, 1) for w in (wg, wu, wd))
    width = max(shard, min(cols, 2 * LANES))
    chunks = tp * cols // width
    pieces = tokens // (2 * BLOCK)
    vmem = pl.BlockSpec(memory_space=pltpu.VMEM)
    hbm = pl.BlockSpec(memory_space=pl.ANY)
    dma = pltpu.SemaphoreType.DMA
    return pl.pallas_call(
        functools.partial(layer_kernel, n, tp, heads, s1, s2, split),
        out_shape=jax.ShapeDtypeStruct((tokens, cols), jnp.bfloat16),
        in_specs=[vmem] * 7
        + [pl.BlockSpec(memory_space=pltpu.SMEM)]
        + [vmem] * 5
        + [hbm] * 6,
        out_specs=vmem,
        scratch_shapes=[
            pltpu.VMEM(gate.shape, gate.dtype),
            pltpu.VMEM(wout.shape, wout.dtype),
            pltpu.VMEM(residual.shape, residual.dtype),
            dma((3,)),
            pltpu.VMEM((CONV, lanes), jnp.float32),
            pltpu.VMEM((rows8, tokens), jnp.float32),
            pltpu.VMEM((rows8, tokens), jnp.float32),
            pltpu.VMEM((RIM, lanes), jnp.bfloat16),
            pltpu.VMEM((8, lanes), jnp.float32),
            pltpu.VMEM((RIM, lanes), jnp.bfloat16),
            pltpu.VMEM((tokens, 2 * half), jnp.bfloat16),
            pltpu.VMEM((tokens, 2 * (s1 + s2)), jnp.bfloat16),
            pltpu.VMEM((tokens, BLOCK), jnp.float32),
            pltpu.VMEM((s1 + s2, half), jnp.float32),
            pltpu.VMEM((s1 + s2 + RIM, half), jnp.bfloat16),
            pltpu.VMEM((s1 + s2, half), jnp.bfloat16),
            pltpu.VMEM((n, s1 + s2 + RIM, half), jnp.bfloat16),
            pltpu.VMEM((1, tp, tokens, 2 * half), jnp.bfloat16),
            pltpu.VMEM((2, tp, tokens, cols), jnp.bfloat16),
            pltpu.VMEM((2, tokens, tp * cols), jnp.bfloat16),
            pltpu.VMEM((3, n * shard, part), jnp.bfloat16),
            pltpu.VMEM((2, tokens, part), jnp.bfloat16),
            pltpu.VMEM((2, tokens, width), jnp.bfloat16),
            pltpu.VMEM((chunks, tokens, width), jnp.bfloat16),
            pltpu.VMEM((SLOTS, tokens, width), jnp.bfloat16),
            pltpu.VMEM((chunks, tokens, width), jnp.bfloat16),
            pltpu.VMEM((SLOTS, tokens, width), jnp.bfloat16),
            pltpu.VMEM((tp // 2, cols // width, tokens, width), jnp.bfloat16),
            dma((2,)),
            dma((n,)),
            dma((n,)),
            dma((tp // 2, nb)),
            dma((max(tp // 2 - 1, 1), nb)),
            dma((tp, nb)),
            dma((tp // 2, nb)),
            dma((max(tp // 2 - 1, 1), nb)),
            dma((tp, nb)),
            dma((tp // 2, nb)),
            dma((tp // 2, nb)),
            dma((tp, nb)),
            dma((3,)),
            dma((3,)),
            dma((2, 3, n)),
            dma((3, n)),
            dma((2, pieces)),
            dma((chunks, pieces)),
            dma((SLOTS, pieces)),
            dma((chunks, pieces)),
            dma((SLOTS, pieces)),
            dma((tp // 2, cols // width, pieces)),
        ],
        compiler_params=pltpu.CompilerParams(
            has_side_effects=True, vmem_limit_bytes=VMEM_LIMIT
        ),
        name="layer",
    )(*front, gate, wout, residual, wg, wu, wd)


def shards(
    grouped_head_inputs,
    head_gate_inputs,
    unsmoothed_step,
    head_decay_rate,
    extra_log_decay,
    first_group_keys,
    first_group_queries,
    second_group_keys,
    second_group_queries,
    head_input_filter,
    first_group_filter,
    second_group_filter,
    head_norm_gain,
    output_weight,
    residual,
    channel_norm_gain,
    channel_gate_weight,
    channel_up_weight,
    channel_down_weight,
):
    heads = head_decay_rate.shape[1]
    s1, s2 = first_group_keys.shape[1], second_group_keys.shape[1]
    return layer(
        (
            grouped_head_inputs,
            first_group_keys,
            first_group_queries,
            second_group_keys.T,
            second_group_queries.T,
            unsmoothed_step.transpose(1, 2, 0),
            extra_log_decay.transpose(1, 2, 0),
            head_decay_rate,
            head_input_filter,
            first_group_filter,
            second_group_filter,
            head_norm_gain,
            channel_norm_gain.reshape(1, -1),
        ),
        (head_gate_inputs, output_weight, residual),
        channel_gate_weight,
        channel_up_weight,
        channel_down_weight,
        heads,
        s1,
        s2,
    )


def solution(mesh):
    return jax.shard_map(
        shards,
        mesh=mesh,
        in_specs=(
            P("sp", None, "tp"),
            P("sp", None, "tp"),
            P("sp", None, "tp"),
            P(None, "tp"),
            P("sp", None, "tp"),
            P("sp", None),
            P("sp", None),
            P("sp", None),
            P("sp", None),
            P(None, None, "tp"),
            P(),
            P(),
            P(None, "tp"),
            P(None, None, "tp"),
            P("sp", "tp"),
            P(),
            P("sp", "tp"),
            P("sp", "tp"),
            P("sp", "tp"),
        ),
        out_specs=P("sp", "tp"),
        check_vma=False,
    )
```
